128 devices in a mesh: sp: 32 (over z, y, core), tp: 4 (over x).
Axes of the slice: x: 4, y: 4, z: 4, core: 2. Of those that a mesh axis runs over, the one named last changes fastest.
Arguments:
- queries_nope: bfloat16 [12288, 8, 128], P('sp', 'tp'), may hold values from -9 to 9
- queries_rope: bfloat16 [12288, 8, 64], P('sp', 'tp'), may hold values from -6 to 6
- latent: bfloat16 [12288, 512], P('sp'), may hold values from -8 to 8, as said below
- rope_key: bfloat16 [12288, 64], P('sp'), may hold values from -6 to 6
- latent_gain: float32 [512], replicated, may hold values from 0.1 to 1.9
- key_up: bfloat16 [512, 1024], P(None, 'tp'), may hold values from -0.25 to 0.25
- value_up: bfloat16 [512, 1024], P(None, 'tp'), may hold values from -0.25 to 0.25
- out_proj: bfloat16 [1024, 2048], P('tp'), may hold values from -0.75 to 0.75
- stream: bfloat16 [12288, 2048], P(('sp', 'tp')), may hold values from -6 to 6
- mix_gain: float32 [2048], replicated, may hold values from 0.1 to 1.9
- w_gate: bfloat16 [2048, 3072], P('sp', 'tp'), may hold values from -0.125 to 0.125
- w_up: bfloat16 [2048, 3072], P('sp', 'tp'), may hold values from -0.125 to 0.125
- w_down: bfloat16 [3072, 2048], P('tp', 'sp'), may hold values from -0.4375 to 0.4375
- mlp_gain: float32 [2048], replicated, may hold values from 0.1 to 1.9
Outputs:
- result: bfloat16 [12288, 2048], P(('sp', 'tp'))
The draws below stay inside these ranges and needn't reach their ends.
Inputs may be any that keep to these rules, and one draw needn't show every extreme that they name: latent rows carry a mean vector that changes from one eighth of the sequence to the next.
All inputs are finite; a program needn't handle non-finite values.
Results may differ from the reference program's by a relative error of at most 0.017.
Values may be sent and summed in bfloat16 or wider, within the bound.
A program may use at most 192 MiB of HBM per device.

```python
import math
import jax
import jax.numpy as jnp
from jax import lax

D = 2048
HEADS = 8
HEAD = 128
ROPE = 64
LATENT = 512
FF = 3072
SEQ = 12288


def draw_latent(key, part):
    base = jax.random.fold_in(key, 11)
    noise_key, centre_key, factor_key = jax.random.split(base, 3)
    places = jnp.arange(SEQ, dtype=jnp.int32)
    segment = places * 8 // SEQ
    centres = jax.random.normal(centre_key, (8, LATENT), jnp.float32) * 1.5
    noise = jax.random.normal(noise_key, (SEQ, LATENT), jnp.float32)
    return jnp.clip(noise + centres[segment], -8.0, 8.0).astype(jnp.bfloat16)


def rope_pair(key):
    base = jax.random.fold_in(key, 23)
    first_key, second_key, third_key = jax.random.split(base, 3)
    key_part = jnp.clip(jax.random.normal(first_key, (SEQ, ROPE), jnp.float32), -6.0, 6.0)
    query_part = jnp.clip(jax.random.normal(second_key, (SEQ, HEADS, ROPE), jnp.float32), -6.0, 6.0)
    return (query_part.astype(jnp.bfloat16), key_part.astype(jnp.bfloat16))


def draw_queries_rope(key, part):
    return rope_pair(key)[0]


def draw_rope_key(key, part):
    return rope_pair(key)[1]


def levels(own_key, dims, cuts, least, high):
    def one(dim, shards_of):
        heights = jax.random.uniform(jax.random.fold_in(jax.random.fold_in(own_key, 6), dim), (shards_of,), jnp.float32, least / len(cuts), high / len(cuts))
        return jnp.repeat(jnp.exp(heights), dims[dim] // shards_of).reshape((-1,) + (1,) * (len(dims) - dim - 1))

    factor_of = one(*cuts[0])
    for cut in cuts[1:]:
        factor_of = factor_of * one(*cut)
    return factor_of


def normal_values(own_key, dims, scale, reach, shards=(), held_as=jnp.bfloat16):
    loudness = levels(own_key, dims, shards, -0.22, 0.18) if shards else 1.0
    drawn = jax.random.normal(own_key, dims, jnp.float32) * scale * loudness
    return jnp.minimum(jnp.maximum(drawn, -reach), reach).astype(held_as)


def setup_inputs(seed: int = 0) -> dict:
    seeds = jax.random.split(jax.random.key(seed), 15)
    queries_nope = normal_values(seeds[0], (SEQ, HEADS, HEAD), 3.0, 9.0, ((0, 32), (1, 4)))
    queries_rope = draw_queries_rope(jax.random.fold_in(seeds[14], 71), 0)
    latent = draw_latent(jax.random.fold_in(seeds[14], 71), 0)
    rope_key = draw_rope_key(jax.random.fold_in(seeds[14], 71), 0)
    latent_gain = jnp.clip(1.0 + 0.18 * jax.random.normal(seeds[4], (LATENT,), jnp.float32), 0.1, 1.9)
    key_up = normal_values(seeds[5], (LATENT, HEADS * HEAD), LATENT ** -0.5, 0.25, ((1, 4),))
    value_up = normal_values(seeds[6], (LATENT, HEADS * HEAD), LATENT ** -0.5, 0.25, ((1, 4),))
    out_proj = normal_values(seeds[7], (HEADS * HEAD, D), (HEADS * HEAD // 16) ** -0.5, 0.75, ((0, 4),))
    stream = normal_values(seeds[8], (SEQ, D), 1.0, 6.0, ((0, 128),))
    mix_gain = jnp.clip(1.0 + 0.18 * jax.random.normal(seeds[9], (D,), jnp.float32), 0.1, 1.9)
    w_gate = normal_values(seeds[10], (D, FF), D ** -0.5, 0.125, ((0, 32), (1, 4)))
    w_up = normal_values(seeds[11], (D, FF), D ** -0.5, 0.125, ((0, 32), (1, 4)))
    w_down = normal_values(seeds[12], (FF, D), (FF // 16) ** -0.5, 0.4375, ((0, 4), (1, 32)))
    mlp_gain = jnp.clip(1.0 + 0.18 * jax.random.normal(seeds[13], (D,), jnp.float32), 0.1, 1.9)
    return dict(queries_nope=queries_nope, queries_rope=queries_rope, latent=latent, rope_key=rope_key, latent_gain=latent_gain, key_up=key_up, value_up=value_up, out_proj=out_proj, stream=stream, mix_gain=mix_gain, w_gate=w_gate, w_up=w_up, w_down=w_down, mlp_gain=mlp_gain)


theta_base = 10000.0
residual_weight = 8.0 ** 0.25
norm_floor = 1.0
big_negative = -1e+30

def rotate(vector, first_row):
    half = vector.shape[-1] // 2
    rates = theta_base ** (-2.0 * jnp.arange(half, dtype=jnp.float32) / vector.shape[-1])
    places = (first_row + jnp.arange(vector.shape[0], dtype=jnp.int32)).astype(jnp.float32)
    angle = places[:, None] * rates[None, :]
    angle = angle.reshape((vector.shape[0],) + (1,) * (vector.ndim - 2) + (half,))
    cosine = jnp.cos(angle)
    sine = jnp.sin(angle)
    left = vector[..., :half]
    right = vector[..., half:]
    return jnp.concatenate([left * cosine - right * sine, left * sine + right * cosine], axis=-1)

def latent_norm(latent, latent_gain):
    wide = latent.astype(jnp.float32)
    factor = lax.rsqrt(lax.optimization_barrier(jnp.mean(wide * wide, axis=-1, keepdims=True)) + norm_floor)
    return (wide * factor * latent_gain).astype(jnp.bfloat16)

def layer_norm(values, gain):
    centre = lax.optimization_barrier(jnp.mean(values, axis=-1, keepdims=True))
    centred = values - centre
    spread = lax.optimization_barrier(jnp.mean(centred * centred, axis=-1, keepdims=True))
    return centred * lax.rsqrt(spread + norm_floor) * gain

def widen(array):
    return lax.optimization_barrier(array).astype(jnp.float32)

def reference(queries_nope, queries_rope, latent, rope_key, latent_gain, key_up, value_up, out_proj, stream, mix_gain, w_gate, w_up, w_down, mlp_gain):
    seq_len, head_count, head_dim = queries_nope.shape
    rope_dim = queries_rope.shape[2]
    query_turned = rotate(queries_rope.astype(jnp.float32), 0).astype(jnp.bfloat16)
    key_turned = rotate(rope_key.astype(jnp.float32), 0).astype(jnp.bfloat16)
    normed = latent_norm(latent, latent_gain)
    keys = jnp.dot(normed, key_up, preferred_element_type=jnp.float32).astype(jnp.bfloat16)
    keys = widen(keys).reshape(seq_len, head_count, head_dim)
    values_all = jnp.dot(normed, value_up, preferred_element_type=jnp.float32).astype(jnp.bfloat16)
    values_all = widen(values_all).reshape(seq_len, head_count, head_dim)
    key_wide = key_turned.astype(jnp.float32)
    scale = (head_dim + rope_dim) ** (-0.5)
    block = math.gcd(seq_len, 512)
    key_places = jnp.arange(seq_len, dtype=jnp.int32)

    def one_block(index):
        begin = (index * block).astype(jnp.int32)
        query_block = lax.dynamic_slice_in_dim(queries_nope, begin, block, 0).astype(jnp.float32)
        turned_block = lax.dynamic_slice_in_dim(query_turned, begin, block, 0).astype(jnp.float32)
        score = jnp.einsum('thd,shd->hts', query_block, keys) + jnp.einsum('thr,sr->hts', turned_block, key_wide)
        score = score * scale
        allowed = key_places[None, :] <= (begin + jnp.arange(block, dtype=jnp.int32))[:, None]
        score = jnp.where(allowed[None], score, big_negative)
        top = lax.optimization_barrier(jnp.max(score, axis=2, keepdims=True))
        powers = jnp.exp(score - top) * allowed[None]
        denominators = lax.optimization_barrier(jnp.sum(powers, axis=2))
        summed = jnp.einsum('hts,shd->thd', widen(powers.astype(jnp.bfloat16)), values_all)
        return (summed / denominators.T[:, :, None]).astype(jnp.bfloat16)
    blocks = lax.map(one_block, jnp.arange(seq_len // block, dtype=jnp.int32))
    attended = blocks.reshape(seq_len, head_count * head_dim)
    projected = jnp.dot(attended, out_proj, preferred_element_type=jnp.float32)
    mixed = layer_norm(residual_weight * stream.astype(jnp.float32) + projected, mix_gain).astype(jnp.bfloat16)
    gate_sum = jnp.dot(mixed, w_gate, preferred_element_type=jnp.float32)
    up_sum = jnp.dot(mixed, w_up, preferred_element_type=jnp.float32)
    hidden = (jax.nn.silu(gate_sum) * up_sum).astype(jnp.bfloat16)
    lowered = jnp.dot(hidden, w_down, preferred_element_type=jnp.float32)
    return layer_norm(residual_weight * mixed.astype(jnp.float32) + 0.5 * lowered, mlp_gain).astype(jnp.bfloat16)
```

```python
import functools
import math

import jax
import jax.numpy as jnp
from jax import lax
from jax.experimental import pallas as pl
from jax.experimental.pallas import tpu as pltpu
from jax.sharding import PartitionSpec as P

theta_base = 10000.0
residual_weight = 8.0**0.25
norm_floor = 1.0
big_negative = -1e30
F32 = jnp.float32
BF16 = jnp.bfloat16


def rows_first(arrays, axis, dims):
    turned = [jnp.moveaxis(a, dim, 0) for a, dim in zip(arrays, dims)]
    both = jnp.concatenate([t.reshape(len(t), -1) for t in turned], axis=1)
    filled, at, gathered = (lax.all_gather(both, axis, axis=0, tiled=True), 0, [])
    for t, dim in zip(turned, dims):
        share = filled[:, at : at + t[0].size].reshape(-1, *t.shape[1:])
        gathered.append(jnp.moveaxis(share, 0, dim))
        at += t[0].size
    return tuple(gathered)


def in_order(pieces, dim):
    dims = list(pieces.shape[1:])
    dims[dim] *= pieces.shape[0]
    return jnp.moveaxis(pieces, 0, dim).reshape(dims)


def copy_for_each(x, axis):
    copies = jnp.broadcast_to(x, (lax.axis_size(axis), *x.shape))
    return lax.all_to_all(copies, axis, split_axis=0, concat_axis=0, tiled=True)


def collect(x, axis, dim):
    return in_order(copy_for_each(x, axis), dim)


def cut_along(x, dim, devices):
    before, after = (x.shape[:dim], x.shape[dim + 1 :])
    return jnp.moveaxis(x.reshape(*before, devices, -1, *after), dim, 0)


def sent_and_summed(x, axis, dim):
    devices = lax.axis_size(axis)
    pieces = lax.all_to_all(cut_along(x, dim, devices), axis, 0, 0, tiled=True)
    return jnp.sum(pieces.astype(jnp.float32), axis=0)


def rotate(vector, first_row):
    half = vector.shape[-1] // 2
    rates = theta_base ** (-2.0 * jnp.arange(half, dtype=jnp.float32) / vector.shape[-1])
    places = (first_row + jnp.arange(vector.shape[0], dtype=jnp.int32)).astype(jnp.float32)
    angle = places[:, None] * rates[None, :]
    angle = angle.reshape((vector.shape[0],) + (1,) * (vector.ndim - 2) + (half,))
    cosine = jnp.cos(angle)
    sine = jnp.sin(angle)
    left = vector[..., :half]
    right = vector[..., half:]
    return jnp.concatenate([left * cosine - right * sine, left * sine + right * cosine], axis=-1)


def latent_norm(latent, latent_gain):
    wide = latent.astype(jnp.float32)
    factor = lax.rsqrt(jnp.mean(wide * wide, axis=-1, keepdims=True) + norm_floor)
    return (wide * factor * latent_gain).astype(jnp.bfloat16)


def layer_norm(values, gain):
    centre = jnp.mean(values, axis=-1, keepdims=True)
    centred = values - centre
    spread = jnp.mean(centred * centred, axis=-1, keepdims=True)
    return centred * lax.rsqrt(spread + norm_floor) * gain


def attend_chunk(kv, q_ref, m_ref, l_ref, acc_ref, rows, const, diag):
    half = rows // 2
    blocks = rows // 128
    r = kv[4 * rows : 4 * rows + half, :]
    for h in range(2):
        top = jnp.concatenate([kv[h * rows : h * rows + half, :], r], axis=1)
        low = jnp.concatenate([kv[h * rows + half : (h + 1) * rows, :], r], axis=1)
        s = jnp.concatenate(
            [
                jnp.dot(top, q_ref[2 * h], preferred_element_type=F32),
                jnp.dot(low, q_ref[2 * h + 1], preferred_element_type=F32),
            ],
            axis=0,
        )
        s = s * const
        if diag:
            key = lax.broadcasted_iota(jnp.int32, s.shape, 0)
            query = lax.broadcasted_iota(jnp.int32, s.shape, 1)
            s = jnp.where(key <= query, s, big_negative)
        m_old = m_ref[h]
        m_new = jnp.maximum(m_old, jnp.max(s, axis=0, keepdims=True))
        p = jnp.exp2(s - m_new)
        alpha = jnp.exp2(m_old - m_new)
        l_ref[h] = l_ref[h] * alpha + jnp.sum(p, axis=0, keepdims=True)
        m_ref[h] = m_new
        at = 2 * rows + h * rows
        vt = jnp.concatenate([kv[at + 128 * i : at + 128 * (i + 1), :] for i in range(blocks)], axis=1)
        acc_ref[h] = acc_ref[h] * alpha + jnp.dot(vt, p.astype(BF16), preferred_element_type=F32)


def attention_kernel(rows, const, kv_ref, q_ref, out_ref, m_ref, l_ref, acc_ref):
    me = lax.axis_index("sp")
    m_ref[...] = jnp.full_like(m_ref, big_negative)
    l_ref[...] = jnp.zeros_like(l_ref)
    acc_ref[...] = jnp.zeros_like(acc_ref)
    attend_chunk(kv_ref.at[me], q_ref, m_ref, l_ref, acc_ref, rows, const, True)

    def step(j, _):
        attend_chunk(kv_ref.at[j], q_ref, m_ref, l_ref, acc_ref, rows, const, False)
        return _

    lax.fori_loop(0, me, step, 0)
    for h in range(2):
        out_ref[:, 128 * h : 128 * (h + 1)] = (acc_ref[h] / l_ref[h]).T.astype(BF16)


def per_device(
    queries_nope,
    queries_rope,
    latent,
    rope_key,
    latent_gain,
    key_up,
    value_up,
    out_proj,
    stream,
    mix_gain,
    w_gate,
    w_up,
    w_down,
    mlp_gain,
):
    rows, heads, head_dim = queries_nope.shape
    rope_dim = queries_rope.shape[2]
    first_row = lax.axis_index("sp") * rows
    query_turned = rotate(queries_rope.astype(F32), first_row).astype(BF16)
    key_turned = rotate(rope_key.astype(F32), first_row).astype(BF16)
    normed = latent_norm(latent, latent_gain)
    keys = jnp.dot(normed, key_up, preferred_element_type=F32).astype(BF16)
    values_t = lax.dot_general(
        value_up, normed, (((0,), (1,)), ((), ())), preferred_element_type=F32
    ).astype(BF16)
    half = rows // 2
    slab = jnp.concatenate(
        [keys[:, :128], keys[:, 128:]]
        + [values_t[128 * h : 128 * (h + 1), 128 * i : 128 * (i + 1)] for h in range(2) for i in range(rows // 128)]
        + [jnp.concatenate([key_turned[:half], key_turned[half:]], axis=1)],
        axis=0,
    )
    pieces = lax.all_gather(slab, "sp", axis=0, tiled=False)
    gate_full, up_full, down_full = rows_first((w_gate, w_up, w_down), "sp", (0, 0, 1))
    qn = jnp.transpose(queries_nope, (1, 2, 0))
    qr = jnp.transpose(query_turned, (1, 2, 0))
    zero = jnp.zeros_like(qr)
    q_all = jnp.stack(
        [jnp.concatenate([qn, qr, zero], axis=1), jnp.concatenate([qn, zero, qr], axis=1)], axis=1
    ).reshape(2 * heads, 2 * head_dim, rows)
    const = (head_dim + rope_dim) ** (-0.5) * math.log2(math.e)
    attended = pl.pallas_call(
        functools.partial(attention_kernel, rows, const),
        out_shape=jax.ShapeDtypeStruct((rows, heads * head_dim), BF16),
        in_specs=[pl.BlockSpec(memory_space=pltpu.VMEM)] * 2,
        out_specs=pl.BlockSpec(memory_space=pltpu.VMEM),
        scratch_shapes=[
            pltpu.VMEM((2, 1, rows), F32),
            pltpu.VMEM((2, 1, rows), F32),
            pltpu.VMEM((2, 128, rows), F32),
        ],
        compiler_params=pltpu.CompilerParams(vmem_limit_bytes=48 * 1024 * 1024),
        cost_estimate=pl.CostEstimate(flops=10**10, bytes_accessed=15 * 10**6, transcendentals=10**7),
        name="attend",
    )(pieces, q_all)
    row_heads = lax.all_to_all(attended, "tp", split_axis=0, concat_axis=1, tiled=True)
    whole_proj = collect(out_proj, "tp", 0)
    projected = jnp.dot(row_heads, whole_proj, preferred_element_type=F32)
    mixed = layer_norm(residual_weight * stream.astype(F32) + projected, mix_gain).astype(BF16)
    expand_piece = collect(mixed, "tp", 0)
    gate_sum = jnp.dot(expand_piece, gate_full, preferred_element_type=F32)
    up_sum = jnp.dot(expand_piece, up_full, preferred_element_type=F32)
    hidden = (jax.nn.silu(gate_sum) * up_sum).astype(BF16)
    lowered = sent_and_summed(
        jnp.dot(hidden, down_full, preferred_element_type=F32).astype(BF16), "tp", 0
    )
    return layer_norm(residual_weight * mixed.astype(F32) + 0.5 * lowered, mlp_gain).astype(BF16)


def solution(mesh):
    return jax.shard_map(
        per_device,
        mesh=mesh,
        in_specs=(
            P("sp", "tp", None),
            P("sp", "tp", None),
            P("sp", None),
            P("sp", None),
            P(),
            P(None, "tp"),
            P(None, "tp"),
            P("tp", None),
            P(("sp", "tp"), None),
            P(),
            P("sp", "tp"),
            P("sp", "tp"),
            P("tp", "sp"),
            P(),
        ),
        out_specs=P(("sp", "tp"), None),
        check_vma=False,
    )
```

```python
import functools
import math

import jax
import jax.numpy as jnp
from jax import lax
from jax.experimental import pallas as pl
from jax.experimental.pallas import tpu as pltpu
from jax.sharding import PartitionSpec as P

theta_base = 10000.0
residual_weight = 8.0**0.25
norm_floor = 1.0
big_negative = -1e30
F32 = jnp.float32
BF16 = jnp.bfloat16


def rotate(vector, first_row):
    half = vector.shape[-1] // 2
    rates = theta_base ** (-2.0 * jnp.arange(half, dtype=jnp.float32) / vector.shape[-1])
    places = (first_row + jnp.arange(vector.shape[0], dtype=jnp.int32)).astype(jnp.float32)
    angle = places[:, None] * rates[None, :]
    angle = angle.reshape((vector.shape[0],) + (1,) * (vector.ndim - 2) + (half,))
    cosine = jnp.cos(angle)
    sine = jnp.sin(angle)
    left = vector[..., :half]
    right = vector[..., half:]
    return jnp.concatenate([left * cosine - right * sine, left * sine + right * cosine], axis=-1)


def latent_norm(latent, latent_gain):
    wide = latent.astype(jnp.float32)
    factor = lax.rsqrt(jnp.mean(wide * wide, axis=-1, keepdims=True) + norm_floor)
    return (wide * factor * latent_gain).astype(jnp.bfloat16)


def layer_norm(values, gain):
    centre = jnp.mean(values, axis=-1, keepdims=True)
    centred = values - centre
    spread = jnp.mean(centred * centred, axis=-1, keepdims=True)
    return centred * lax.rsqrt(spread + norm_floor) * gain


def attend_chunk(kv, q_ref, m_ref, l_ref, acc_ref, rows, const, diag):
    half = rows // 2
    blocks = rows // 128
    r = kv[4 * rows : 4 * rows + half, :]
    for h in range(2):
        top = jnp.concatenate([kv[h * rows : h * rows + half, :], r], axis=1)
        low = jnp.concatenate([kv[h * rows + half : (h + 1) * rows, :], r], axis=1)
        s = jnp.concatenate(
            [
                jnp.dot(top, q_ref[2 * h], preferred_element_type=F32),
                jnp.dot(low, q_ref[2 * h + 1], preferred_element_type=F32),
            ],
            axis=0,
        )
        s = s * const
        if diag:
            key = lax.broadcasted_iota(jnp.int32, s.shape, 0)
            query = lax.broadcasted_iota(jnp.int32, s.shape, 1)
            s = jnp.where(key <= query, s, big_negative)
        m_old = m_ref[h]
        m_new = jnp.maximum(m_old, jnp.max(s, axis=0, keepdims=True))
        p = jnp.exp2(s - m_new)
        alpha = jnp.exp2(m_old - m_new)
        l_ref[h] = l_ref[h] * alpha + jnp.sum(p, axis=0, keepdims=True)
        m_ref[h] = m_new
        at = 2 * rows + h * rows
        vt = jnp.concatenate([kv[at + 128 * i : at + 128 * (i + 1), :] for i in range(blocks)], axis=1)
        acc_ref[h] = acc_ref[h] * alpha + jnp.dot(vt, p.astype(BF16), preferred_element_type=F32)


MESH = pl.DeviceIdType.MESH
ITEMS = (
    (0, 0), (-1, 0), (1, 0), (0, -1), (0, 1), (2, 0), (-1, -1), (-1, 1),
    (1, -1), (1, 1), (0, 2), (2, -1), (2, 1), (-1, 2), (1, 2), (2, 2),
)
PLACE = {item: k for k, item in enumerate(ITEMS)}
STEPS = 2 * len(ITEMS)


def remote(src, dst, send_sem, recv_sem, device):
    return pltpu.make_async_remote_copy(
        src_ref=src, dst_ref=dst, send_sem=send_sem, recv_sem=recv_sem, device_id=device, device_id_type=MESH
    )


class Torus:
    def __init__(self):
        self.me = lax.axis_index("sp")
        self.x = lax.axis_index("tp")
        self.c = lax.rem(self.me, 2)
        chip = self.me // 2
        z, y = chip // 4, lax.rem(chip, 4)
        self.a = z + self.c * (y - z)
        self.b = y + self.c * (z - y)
        self.step_a = 8 - 6 * self.c
        self.step_b = 2 + 6 * self.c

    def index(self, da, db):
        at_a = lax.rem(self.a + da + 4, 4)
        at_b = lax.rem(self.b + db + 4, 4)
        return at_a * self.step_a + at_b * self.step_b + self.c

    def twin_index(self, da, db):
        at_b = lax.rem(self.b + da + 4, 4)
        at_a = lax.rem(self.a + db + 4, 4)
        return at_a * self.step_a + at_b * self.step_b + 1 - self.c

    def at(self, da, db):
        return (self.index(da, db), self.x)

    def twin(self):
        return (self.me + 1 - 2 * self.c, self.x)

    def along_x(self, d):
        return (self.me, lax.rem(self.x + d + 4, 4))


class Gather:
    def __init__(self, torus, buf, send_sems, recv_sems, twin_sems):
        self.torus, self.buf = torus, buf
        self.send_sems, self.recv_sems, self.twin_sems = send_sems, recv_sems, twin_sems
        self.half = buf.shape[1] // 2

    def part(self, slot, which):
        if which is None:
            return self.buf.at[slot]
        return self.buf.at[slot, pl.ds(which * self.half, self.half)]

    def copies(self, k):
        t = self.torus
        da, db = ITEMS[k]
        slot = t.index(da, db)
        plan = []
        if db == 0:
            if da == 0:
                plan += [(2, (1, 0), (-1, 0), None), (3, (-1, 0), (1, 0), None)]
            plan += [(0, (0, 1), (da, -1), None), (1, (0, -1), (da, 1), None)]
            if da == -1:
                plan += [(2, (1, 0), (2, 0), 0)]
            if da == 1:
                plan += [(2, (-1, 0), (2, 0), 1)]
        if db == -1:
            plan += [(0, (0, 1), (da, 2), 0)]
        if db == 1:
            plan += [(1, (0, -1), (da, 2), 1)]
        out = []
        for sem, to, name, which in plan:
            ref = self.part(slot, which)
            recv = self.recv_sems.at[PLACE[name], which or 0]
            out.append(remote(ref, ref, self.send_sems.at[k, sem], recv, t.at(*to)))
        ref = self.part(slot, None)
        out.append(remote(ref, ref, self.send_sems.at[k, 4], self.twin_sems.at[k], t.twin()))
        return out

    def send(self, k):
        for copy in self.copies(k):
            copy.start()

    def sent(self):
        for k in range(len(ITEMS)):
            for copy in self.copies(k):
                copy.wait_send()

    def arrived(self, k):
        t = self.torus
        da, db = ITEMS[k]
        slot = t.index(da, db)
        for which in (0, 1) if 2 in (da, db) and not (da == 2 and db in (-1, 1)) else (None,):
            ref = self.part(slot, which)
            remote(ref, ref, self.send_sems.at[k, 0], self.recv_sems.at[k, which or 0], t.twin()).wait_recv()

    def twin_arrived(self, k, slot):
        ref = self.part(slot, None)
        remote(ref, ref, self.send_sems.at[0, 0], self.twin_sems.at[k], self.torus.twin()).wait_recv()


def whole_kernel(
    rows,
    const,
    slab_hbm,
    weights_hbm,
    proj_hbm,
    q_ref,
    stream_ref,
    mix_gain_ref,
    mlp_gain_ref,
    out_ref,
    kv,
    weights,
    proj,
    m_ref,
    l_ref,
    acc_ref,
    attended,
    row_heads,
    sums,
    mixed,
    hidden,
    far_out,
    plus_out,
    minus_out,
    far_plus,
    far_minus,
    from_plus,
    from_minus,
    load_sems,
    kv_send,
    kv_recv,
    kv_twin,
    w_send,
    w_recv,
    w_twin,
    proj_send,
    proj_recv,
    x_send,
    x_recv,
):
    t = Torus()
    me, x = t.me, t.x
    loads = [
        pltpu.make_async_copy(slab_hbm, kv.at[me], load_sems.at[0]),
        pltpu.make_async_copy(proj_hbm, proj.at[x], load_sems.at[1]),
        pltpu.make_async_copy(weights_hbm, weights.at[me], load_sems.at[2]),
    ]
    for load in loads:
        load.start()

    plus, minus, across = t.along_x(1), t.along_x(-1), t.along_x(2)
    peers = (t.at(1, 0), t.at(-1, 0), t.at(0, 1), t.at(0, -1), t.twin(), plus, minus, across)
    barrier = pltpu.get_barrier_semaphore()
    for peer in peers:
        pl.semaphore_signal(barrier, inc=1, device_id=peer, device_id_type=MESH)
    pl.semaphore_wait(barrier, len(peers))

    pieces = Gather(t, kv, kv_send, kv_recv, kv_twin)
    halves = Gather(t, weights, w_send, w_recv, w_twin)

    share = proj.shape[1] // 2

    def proj_part(d, which):
        slot = lax.rem(x + d + 4, 4)
        size = share if which is None else share // 2
        first = t.c * share + (0 if which is None else which * size)
        return proj.at[slot, pl.ds(pl.multiple_of(first, size), size)]

    def proj_copy(d, which, sem, recv, to):
        ref = proj_part(d, which)
        return remote(ref, ref, proj_send.at[sem], proj_recv.at[recv], to)

    proj_first = [proj_copy(0, None, 0, 0, plus), proj_copy(0, None, 1, 1, minus)]
    proj_second = [
        proj_copy(-1, 0, 2, 2, plus),
        proj_copy(1, 1, 3, 3, minus),
        proj_copy(-1, None, 4, 4, t.twin()),
        proj_copy(1, None, 5, 5, t.twin()),
    ]
    proj_third = [proj_copy(2, None, 6, 6, t.twin())]

    def twin_proj(d, recv):
        slot = lax.rem(x + d + 4, 4)
        first = (1 - t.c) * share
        ref = proj.at[slot, pl.ds(pl.multiple_of(first, share), share)]
        return remote(ref, ref, proj_send.at[0], proj_recv.at[recv], t.twin())

    loads[0].wait()
    pieces.send(0)
    loads[1].wait()
    for copy in proj_first:
        copy.start()

    m_ref[...] = jnp.full_like(m_ref, big_negative)
    l_ref[...] = jnp.zeros_like(l_ref)
    acc_ref[...] = jnp.zeros_like(acc_ref)
    attend_chunk(kv.at[me], q_ref, m_ref, l_ref, acc_ref, rows, const, True)
    loads[2].wait()

    def step(i, carry):
        item = i // 2
        odd = lax.rem(i, 2)
        for k in range(1, len(ITEMS)):

            @pl.when(i == 2 * (k - 1))
            def _():
                pieces.arrived(k)
                pieces.send(k)

        @pl.when(i == PROJ_SECOND)
        def _():
            proj_copy(-1, None, 0, 0, minus).wait_recv()
            proj_copy(1, None, 0, 1, minus).wait_recv()
            for copy in proj_second:
                copy.start()

        @pl.when(i == PROJ_THIRD)
        def _():
            proj_copy(2, 0, 0, 2, minus).wait_recv()
            proj_copy(2, 1, 0, 3, minus).wait_recv()
            for copy in proj_third:
                copy.start()

        @pl.when(i == WEIGHTS_FIRST)
        def _():
            halves.send(0)

        da, db = jnp.int32(0), jnp.int32(0)
        number = item + 1 - odd
        for k, (ka, kb) in enumerate(ITEMS):
            da = jnp.where(number == k, ka, da)
            db = jnp.where(number == k, kb, db)
        off_a = jnp.where(odd == 1, db, da)
        off_b = jnp.where(odd == 1, da, db)
        at_a = lax.rem(t.a + off_a + 4, 4)
        at_b = lax.rem(t.b + off_b + 4, 4)
        slot = at_a * t.step_a + at_b * t.step_b + jnp.where(odd == 1, 1 - t.c, t.c)

        @pl.when(odd == 1)
        def _():
            pieces.twin_arrived(item, slot)

        @pl.when(jnp.logical_and(slot < me, i != STEPS - 2))
        def _():
            attend_chunk(kv.at[slot], q_ref, m_ref, l_ref, acc_ref, rows, const, False)

        return carry

    lax.fori_loop(0, STEPS, step, 0)

    for h in range(2):
        attended[:, 128 * h : 128 * (h + 1)] = (acc_ref[h] / l_ref[h]).T.astype(BF16)
    own = rows // 4

    def own_rows(d):
        first = lax.rem(x + d + 4, 4) * own
        return attended.at[pl.ds(pl.multiple_of(first, own), own)]

    heads_out = [
        remote(own_rows(2), row_heads.at[x], x_send.at[0], x_recv.at[0], across),
        remote(own_rows(1), row_heads.at[x], x_send.at[1], x_recv.at[1], plus),
        remote(own_rows(-1), row_heads.at[x], x_send.at[2], x_recv.at[2], minus),
    ]
    for copy in heads_out:
        copy.start()
    row_heads[x] = attended[pl.ds(pl.multiple_of(x * own, own), own), :]

    def weights_step(first, last):
        for k in range(first, last):
            halves.arrived(k)
            halves.send(k)

    weights_step(1, 3)
    for d, sem in ((1, 4), (-1, 5), (2, 6)):
        twin_proj(d, sem).wait_recv()
    for d, sem in ((2, 0), (-1, 1), (1, 2)):
        ref = row_heads.at[lax.rem(x + d + 4, 4)]
        remote(ref, ref, x_send.at[0], x_recv.at[sem], plus).wait_recv()

    lhs = jnp.concatenate([row_heads[p] for p in range(4)], axis=1)
    width = sums.shape[1]

    def project(n, carry):
        cols = pl.ds(pl.multiple_of(n * 256, 256), 256)
        rhs = proj[:, :, cols].reshape(4 * proj.shape[1], 256)
        sums[pl.ds(0, own), cols] = jnp.dot(lhs, rhs, preferred_element_type=F32)
        return carry

    lax.fori_loop(0, width // 256, project, 0)
    mixed[x] = layer_norm(
        residual_weight * stream_ref[...].astype(F32) + sums[pl.ds(0, own), :], mix_gain_ref[...]
    ).astype(BF16)

    half = own // 2

    def mixed_copy(d, which, sem, recv, to):
        slot = lax.rem(x + d + 4, 4)
        ref = mixed.at[slot] if which is None else mixed.at[slot, pl.ds(which * half, half)]
        return remote(ref, ref, x_send.at[sem], x_recv.at[recv], to)

    mixed_first = [mixed_copy(0, None, 3, 3, plus), mixed_copy(0, None, 4, 4, minus)]
    mixed_second = [mixed_copy(-1, 0, 5, 5, plus), mixed_copy(1, 1, 6, 6, minus)]
    for copy in mixed_first:
        copy.start()
    weights_step(3, 10)
    mixed_copy(-1, None, 3, 3, plus).wait_recv()
    mixed_copy(1, None, 3, 4, plus).wait_recv()
    for copy in mixed_second:
        copy.start()
    weights_step(10, 13)
    mixed_copy(2, 0, 3, 5, plus).wait_recv()
    mixed_copy(2, 1, 3, 6, plus).wait_recv()
    weights_step(13, 16)
    for k, item in enumerate(ITEMS):
        halves.twin_arrived(k, t.twin_index(*item))

    count = weights.shape[0]
    depth = weights.shape[1] // 3
    units = weights.shape[2]

    def feed(first, second):
        into = jnp.concatenate(
            [mixed[lax.rem(x + first + 4, 4)], mixed[lax.rem(x + second + 4, 4)]], axis=0
        )

        def expand(n, carry):
            cols = pl.ds(pl.multiple_of(n * 256, 256), 256)
            gate = jnp.dot(
                into, weights[:, 0:depth, cols].reshape(count * depth, 256), preferred_element_type=F32
            )
            up = jnp.dot(
                into, weights[:, depth : 2 * depth, cols].reshape(count * depth, 256), preferred_element_type=F32
            )
            hidden[:, cols] = (gate / (1.0 + jnp.exp(-gate)) * up).astype(BF16)
            return carry

        lax.fori_loop(0, units // 256, expand, 0)
        group = 256 // depth

        def lower(n, carry):
            rhs = weights[pl.ds(n * group, group), 2 * depth : 3 * depth, :].reshape(256, units)
            sums[:, pl.ds(pl.multiple_of(n * 256, 256), 256)] = lax.dot_general(
                hidden[...], rhs, (((1,), (1,)), ((), ())), preferred_element_type=F32
            )
            return carry

        lax.fori_loop(0, count // group, lower, 0)

    top, low = pl.ds(0, half), pl.ds(half, half)

    def result_copy(src, src_rows, dst, dst_rows, sem, to):
        s = src.at[src_rows]
        d = dst if dst_rows is None else dst.at[dst_rows]
        return remote(s, d, x_send.at[sem], x_recv.at[sem], to)

    feed(2, 1)
    far_out[...] = sums[0:own, :].astype(BF16)
    plus_out[...] = sums[own : 2 * own, :].astype(BF16)
    back = [
        result_copy(far_out, top, far_minus, None, 7, plus),
        result_copy(far_out, low, far_plus, None, 8, minus),
        result_copy(plus_out, low, from_minus, low, 9, plus),
        result_copy(minus_out, top, from_plus, top, 10, minus),
        result_copy(plus_out, top, from_minus, top, 11, plus),
        result_copy(minus_out, low, from_plus, low, 12, minus),
    ]
    for copy in back[:3]:
        copy.start()
    feed(-1, 0)
    minus_out[...] = sums[0:own, :].astype(BF16)
    back[3].start()
    back[0].wait_recv()
    plus_out[top, :] = (plus_out[top, :].astype(F32) + far_minus[...].astype(F32)).astype(BF16)
    back[4].start()
    back[1].wait_recv()
    minus_out[low, :] = (minus_out[low, :].astype(F32) + far_plus[...].astype(F32)).astype(BF16)
    back[5].start()
    for copy in back[2:]:
        copy.wait_recv()
    lowered = sums[own : 2 * own, :] + from_plus[...].astype(F32) + from_minus[...].astype(F32)
    out_ref[...] = layer_norm(
        residual_weight * mixed[x].astype(F32) + 0.5 * lowered, mlp_gain_ref[...]
    ).astype(BF16)

    pieces.sent()
    halves.sent()
    for copy in proj_first + proj_second + proj_third + heads_out + mixed_first + mixed_second + back:
        copy.wait_send()


PROJ_SECOND = 11
PROJ_THIRD = 19
WEIGHTS_FIRST = 23


def per_device(
    queries_nope,
    queries_rope,
    latent,
    rope_key,
    latent_gain,
    key_up,
    value_up,
    out_proj,
    stream,
    mix_gain,
    w_gate,
    w_up,
    w_down,
    mlp_gain,
):
    rows, heads, head_dim = queries_nope.shape
    rope_dim = queries_rope.shape[2]
    count = lax.axis_size("sp")
    tp = lax.axis_size("tp")
    own, width = stream.shape
    units = w_gate.shape[1]
    first_row = lax.axis_index("sp") * rows
    query_turned = rotate(queries_rope.astype(F32), first_row).astype(BF16)
    key_turned = rotate(rope_key.astype(F32), first_row).astype(BF16)
    normed = latent_norm(latent, latent_gain)
    keys = jnp.dot(normed, key_up, preferred_element_type=F32).astype(BF16)
    values_t = lax.dot_general(
        value_up, normed, (((0,), (1,)), ((), ())), preferred_element_type=F32
    ).astype(BF16)
    half = rows // 2
    slab = jnp.concatenate(
        [keys[:, :128], keys[:, 128:]]
        + [values_t[128 * h : 128 * (h + 1), 128 * i : 128 * (i + 1)] for h in range(2) for i in range(rows // 128)]
        + [jnp.concatenate([key_turned[:half], key_turned[half:]], axis=1)],
        axis=0,
    )
    weights = jnp.concatenate([w_gate, w_up, w_down.T], axis=0)
    qn = jnp.transpose(queries_nope, (1, 2, 0))
    qr = jnp.transpose(query_turned, (1, 2, 0))
    zero = jnp.zeros_like(qr)
    q_all = jnp.stack(
        [jnp.concatenate([qn, qr, zero], axis=1), jnp.concatenate([qn, zero, qr], axis=1)], axis=1
    ).reshape(2 * heads, 2 * head_dim, rows)
    const = (head_dim + rope_dim) ** (-0.5) * math.log2(math.e)
    vmem = pl.BlockSpec(memory_space=pltpu.VMEM)
    hbm = pl.BlockSpec(memory_space=pl.ANY)
    dma = pltpu.SemaphoreType.DMA
    return pl.pallas_call(
        functools.partial(whole_kernel, rows, const),
        out_shape=jax.ShapeDtypeStruct((own, width), BF16),
        in_specs=[hbm, hbm, hbm, vmem, vmem, vmem, vmem],
        out_specs=vmem,
        scratch_shapes=[
            pltpu.VMEM((count, *slab.shape), BF16),
            pltpu.VMEM((count, *weights.shape), BF16),
            pltpu.VMEM((tp, *out_proj.shape), BF16),
            pltpu.VMEM((2, 1, rows), F32),
            pltpu.VMEM((2, 1, rows), F32),
            pltpu.VMEM((2, 128, rows), F32),
            pltpu.VMEM((rows, heads * head_dim), BF16),
            pltpu.VMEM((tp, own, heads * head_dim), BF16),
            pltpu.VMEM((2 * own, width), F32),
            pltpu.VMEM((tp, own, width), BF16),
            pltpu.VMEM((2 * own, units), BF16),
            pltpu.VMEM((own, width), BF16),
            pltpu.VMEM((own, width), BF16),
            pltpu.VMEM((own, width), BF16),
            pltpu.VMEM((own // 2, width), BF16),
            pltpu.VMEM((own // 2, width), BF16),
            pltpu.VMEM((own, width), BF16),
            pltpu.VMEM((own, width), BF16),
            dma((3,)),
            dma((16, 5)),
            dma((16, 2)),
            dma((16,)),
            dma((16, 5)),
            dma((16, 2)),
            dma((16,)),
            dma((7,)),
            dma((7,)),
            dma((13,)),
            dma((13,)),
        ],
        compiler_params=pltpu.CompilerParams(
            collective_id=0, has_side_effects=True, vmem_limit_bytes=60 * 1024 * 1024
        ),
        name="layer",
    )(slab, weights, out_proj, q_all, stream, mix_gain.reshape(1, -1), mlp_gain.reshape(1, -1))


def solution(mesh):
    return jax.shard_map(
        per_device,
        mesh=mesh,
        in_specs=(
            P("sp", "tp", None),
            P("sp", "tp", None),
            P("sp", None),
            P("sp", None),
            P(),
            P(None, "tp"),
            P(None, "tp"),
            P("tp", None),
            P(("sp", "tp"), None),
            P(),
            P("sp", "tp"),
            P("sp", "tp"),
            P("tp", "sp"),
            P(),
        ),
        out_specs=P(("sp", "tp"), None),
        check_vma=False,
    )
```

```python
import functools
import math

import jax
import jax.numpy as jnp
import numpy as np
from jax import lax
from jax.experimental import pallas as pl
from jax.experimental.pallas import tpu as pltpu
from jax.sharding import PartitionSpec as P

theta_base = 10000.0
residual_weight = 8.0**0.25
norm_floor = 1.0
big_negative = -1e30
F32 = jnp.float32
BF16 = jnp.bfloat16


def turn_tables(rows, count, rope_dim):
    rates = theta_base ** (-2.0 * np.arange(rope_dim // 2) / rope_dim)[:, None]
    inner = rates * np.arange(rows)
    outer = (rates * (np.arange(count) * rows)).T[:, :, None] + np.zeros((1, 1, 128))
    pair = lambda angle: jnp.asarray(np.stack([np.cos(angle), np.sin(angle)]), F32)
    return pair(inner), jnp.moveaxis(pair(outer), 0, 1)


def turn(v, cosine, sine):
    half = v.shape[0] // 2
    a, b = v[:half], v[half:]
    return jnp.concatenate([a * cosine - b * sine, a * sine + b * cosine], axis=0)


def layer_norm(values, gain):
    centre = jnp.mean(values, axis=-1, keepdims=True)
    centred = values - centre
    spread = jnp.mean(centred * centred, axis=-1, keepdims=True)
    return centred * lax.rsqrt(spread + norm_floor) * gain


def scores(kv, h, q_ref, rows, const):
    half = rows // 2
    r = kv[4 * rows : 4 * rows + half, :]
    top = jnp.concatenate([kv[h * rows : h * rows + half, :], r], axis=1)
    low = jnp.concatenate([kv[h * rows + half : (h + 1) * rows, :], r], axis=1)
    both = [
        jnp.dot(top, q_ref[2 * h], preferred_element_type=F32),
        jnp.dot(low, q_ref[2 * h + 1], preferred_element_type=F32),
    ]
    return jnp.concatenate(both, axis=0) * const


def values_of(kv, h, rows):
    at = 2 * rows + h * rows
    return [kv[at + 128 * i : at + 128 * (i + 1), :] for i in range(rows // 128)]


def attend(pieces, q_ref, m_ref, l_ref, acc_ref, rows, const, diag=False):
    for h in range(2):
        s = jnp.concatenate([scores(kv, h, q_ref, rows, const) for kv in pieces], axis=0)
        if diag:
            key = lax.broadcasted_iota(jnp.int32, s.shape, 0)
            query = lax.broadcasted_iota(jnp.int32, s.shape, 1)
            s = jnp.where(key <= query, s, big_negative)
        m_old = m_ref[h]
        m_new = jnp.maximum(m_old, jnp.max(s, axis=0, keepdims=True))
        p = jnp.exp2(s - m_new)
        alpha = jnp.exp2(m_old - m_new)
        l_ref[h] = l_ref[h] * alpha + jnp.sum(p, axis=0, keepdims=True)
        m_ref[h] = m_new
        vt = jnp.concatenate([block for kv in pieces for block in values_of(kv, h, rows)], axis=1)
        acc_ref[h] = acc_ref[h] * alpha + jnp.dot(vt, p.astype(BF16), preferred_element_type=F32)


MESH = pl.DeviceIdType.MESH
ITEMS = (
    (0, 0), (-1, 0), (1, 0), (0, -1), (0, 1), (2, 0), (-1, -1), (-1, 1),
    (1, -1), (1, 1), (0, 2), (2, -1), (2, 1), (-1, 2), (1, 2), (2, 2),
)
PLACE = {item: k for k, item in enumerate(ITEMS)}


def remote(src, dst, send_sem, recv_sem, device):
    return pltpu.make_async_remote_copy(
        src_ref=src, dst_ref=dst, send_sem=send_sem, recv_sem=recv_sem, device_id=device, device_id_type=MESH
    )


class Torus:
    def __init__(self):
        self.me = lax.axis_index("sp")
        self.x = lax.axis_index("tp")
        self.c = lax.rem(self.me, 2)
        chip = self.me // 2
        z, y = chip // 4, lax.rem(chip, 4)
        self.a = z + self.c * (y - z)
        self.b = y + self.c * (z - y)
        self.step_a = 8 - 6 * self.c
        self.step_b = 2 + 6 * self.c

    def index(self, da, db):
        at_a = lax.rem(self.a + da + 4, 4)
        at_b = lax.rem(self.b + db + 4, 4)
        return at_a * self.step_a + at_b * self.step_b + self.c

    def twin_index(self, da, db):
        at_b = lax.rem(self.b + da + 4, 4)
        at_a = lax.rem(self.a + db + 4, 4)
        return at_a * self.step_a + at_b * self.step_b + 1 - self.c

    def at(self, da, db):
        return (self.index(da, db), self.x)

    def twin(self):
        return (self.me + 1 - 2 * self.c, self.x)

    def along_x(self, d):
        return (self.me, lax.rem(self.x + d + 4, 4))


class Gather:
    def __init__(self, torus, buf, send_sems, recv_sems, twin_sems):
        self.torus, self.buf = torus, buf
        self.send_sems, self.recv_sems, self.twin_sems = send_sems, recv_sems, twin_sems
        self.half = buf.shape[1] // 2

    def part(self, slot, which):
        if which is None:
            return self.buf.at[slot]
        return self.buf.at[slot, pl.ds(which * self.half, self.half)]

    def copies(self, k):
        t = self.torus
        da, db = ITEMS[k]
        slot = t.index(da, db)
        plan = []
        if db == 0:
            if da == 0:
                plan += [(2, (1, 0), (-1, 0), None), (3, (-1, 0), (1, 0), None)]
            plan += [(0, (0, 1), (da, -1), None), (1, (0, -1), (da, 1), None)]
            if da == -1:
                plan += [(2, (1, 0), (2, 0), 0)]
            if da == 1:
                plan += [(2, (-1, 0), (2, 0), 1)]
        if db == -1:
            plan += [(0, (0, 1), (da, 2), 0)]
        if db == 1:
            plan += [(1, (0, -1), (da, 2), 1)]
        out = []
        for sem, to, name, which in plan:
            ref = self.part(slot, which)
            recv = self.recv_sems.at[PLACE[name], which or 0]
            out.append(remote(ref, ref, self.send_sems.at[k, sem], recv, t.at(*to)))
        ref = self.part(slot, None)
        out.append(remote(ref, ref, self.send_sems.at[k, 4], self.twin_sems.at[k], t.twin()))
        return out

    def send(self, k):
        for copy in self.copies(k):
            copy.start()

    def sent(self):
        for k in range(len(ITEMS)):
            for copy in self.copies(k):
                copy.wait_send()

    def arrived(self, k):
        t = self.torus
        da, db = ITEMS[k]
        slot = t.index(da, db)
        for which in (0, 1) if 2 in (da, db) and not (da == 2 and db in (-1, 1)) else (None,):
            ref = self.part(slot, which)
            remote(ref, ref, self.send_sems.at[k, 0], self.recv_sems.at[k, which or 0], t.twin()).wait_recv()

    def twin_arrived(self, k, slot):
        ref = self.part(slot, None)
        remote(ref, ref, self.send_sems.at[0, 0], self.twin_sems.at[k], self.torus.twin()).wait_recv()


def whole_kernel(
    rows,
    const,
    latent_hbm,
    rope_key_hbm,
    key_up_hbm,
    value_up_hbm,
    inner_hbm,
    qn_hbm,
    qr_hbm,
    proj_hbm,
    gate_hbm,
    up_hbm,
    down_hbm,
    stream_hbm,
    outer_hbm,
    latent_gain_ref,
    mix_gain_ref,
    mlp_gain_ref,
    out_ref,
    latent_v,
    rope_key_v,
    key_up_v,
    value_up_v,
    inner_v,
    outer_v,
    qn_v,
    qr_v,
    stream_v,
    q_ref,
    kv,
    weights,
    proj,
    m_ref,
    l_ref,
    acc_ref,
    attended,
    row_heads,
    sums,
    mixed,
    hidden,
    far_out,
    plus_out,
    minus_out,
    far_plus,
    far_minus,
    from_plus,
    from_minus,
    load_sems,
    kv_send,
    kv_recv,
    kv_twin,
    w_send,
    w_recv,
    w_twin,
    proj_send,
    proj_recv,
    x_send,
    x_recv,
):
    t = Torus()
    me, x = t.me, t.x
    depth = weights.shape[1] // 3
    loads = [
        pltpu.make_async_copy(src, dst, load_sems.at[n])
        for n, (src, dst) in enumerate(
            (
                (latent_hbm, latent_v),
                (key_up_hbm, key_up_v),
                (value_up_hbm, value_up_v),
                (rope_key_hbm, rope_key_v),
                (inner_hbm, inner_v),
                (outer_hbm.at[me], outer_v),
                (proj_hbm, proj.at[x]),
                (qn_hbm, qn_v),
                (qr_hbm, qr_v),
                (down_hbm, weights.at[me, pl.ds(2 * depth, depth)]),
                (gate_hbm, weights.at[me, pl.ds(0, depth)]),
                (up_hbm, weights.at[me, pl.ds(depth, depth)]),
                (stream_hbm, stream_v),
            )
        )
    ]
    for load in loads:
        load.start()

    plus, minus, across = t.along_x(1), t.along_x(-1), t.along_x(2)
    peers = (t.at(1, 0), t.at(-1, 0), t.at(0, 1), t.at(0, -1), t.twin(), plus, minus, across)
    barrier = pltpu.get_barrier_semaphore()
    for peer in peers:
        pl.semaphore_signal(barrier, inc=1, device_id=peer, device_id_type=MESH)

    pieces = Gather(t, kv, kv_send, kv_recv, kv_twin)
    halves = Gather(t, weights, w_send, w_recv, w_twin)

    share = proj.shape[1] // 2

    def proj_part(d, which):
        slot = lax.rem(x + d + 4, 4)
        size = share if which is None else share // 2
        first = t.c * share + (0 if which is None else which * size)
        return proj.at[slot, pl.ds(pl.multiple_of(first, size), size)]

    def proj_copy(d, which, sem, recv, to):
        ref = proj_part(d, which)
        return remote(ref, ref, proj_send.at[sem], proj_recv.at[recv], to)

    proj_first = [proj_copy(0, None, 0, 0, plus), proj_copy(0, None, 1, 1, minus)]
    proj_second = [
        proj_copy(-1, 0, 2, 2, plus),
        proj_copy(1, 1, 3, 3, minus),
        proj_copy(-1, None, 4, 4, t.twin()),
        proj_copy(1, None, 5, 5, t.twin()),
    ]
    proj_third = [proj_copy(2, None, 6, 6, t.twin())]

    def twin_proj(d, recv):
        slot = lax.rem(x + d + 4, 4)
        first = (1 - t.c) * share
        ref = proj.at[slot, pl.ds(pl.multiple_of(first, share), share)]
        return remote(ref, ref, proj_send.at[0], proj_recv.at[recv], t.twin())

    for load in loads[:6]:
        load.wait()
    wide = latent_v[...].astype(F32)
    factor = lax.rsqrt(jnp.mean(wide * wide, axis=-1, keepdims=True) + norm_floor)
    normed = (wide * factor * latent_gain_ref[...]).astype(BF16)
    slab = kv.at[me]
    keys = jnp.dot(normed, key_up_v[...], preferred_element_type=F32).astype(BF16)
    values = jnp.dot(normed, value_up_v[...], preferred_element_type=F32)
    for h in range(2):
        slab[h * rows : (h + 1) * rows, :] = keys[:, 128 * h : 128 * (h + 1)]
        turned = values[:, 128 * h : 128 * (h + 1)].T.astype(BF16)
        for i in range(rows // 128):
            at = 2 * rows + h * rows + 128 * i
            slab[at : at + 128, :] = turned[:, 128 * i : 128 * (i + 1)]
    outer_cos, outer_sin = outer_v[0, :, 0:1], outer_v[1, :, 0:1]
    inner_cos, inner_sin = inner_v[0], inner_v[1]
    cosine = outer_cos * inner_cos - outer_sin * inner_sin
    sine = outer_sin * inner_cos + outer_cos * inner_sin
    mid = rows // 2
    key_turned = turn(rope_key_v[...].astype(F32), cosine, sine).T
    slab[4 * rows : 4 * rows + mid, :] = jnp.concatenate([key_turned[:mid], key_turned[mid:]], axis=1).astype(BF16)

    pl.semaphore_wait(barrier, len(peers))
    pieces.send(0)
    loads[6].wait()
    for copy in proj_first:
        copy.start()

    for load in loads[7:]:
        load.wait()
    zeros = jnp.zeros((64, rows), BF16)
    for h in range(2):
        nope = qn_v[:, h, :].astype(F32).T.astype(BF16)
        rotary = turn(qr_v[64 * h : 64 * (h + 1), :].astype(F32), cosine, sine).astype(BF16)
        for odd in range(2):
            q_ref[2 * h + odd, 0:128, :] = nope
            q_ref[2 * h + odd, 128:192, :] = zeros if odd else rotary
            q_ref[2 * h + odd, 192:256, :] = rotary if odd else zeros

    m_ref[...] = jnp.full_like(m_ref, big_negative)
    l_ref[...] = jnp.zeros_like(l_ref)
    acc_ref[...] = jnp.zeros_like(acc_ref)
    attend([kv.at[me]], q_ref, m_ref, l_ref, acc_ref, rows, const, diag=True)

    last = len(ITEMS)

    def step(i, carry):
        for group in range(0, last, 4):

            @pl.when(i // 4 == group // 4)
            def _():
                for k in range(max(group, 1), group + 4):

                    @pl.when(i == k)
                    def _():
                        pieces.arrived(k)
                        pieces.send(k)
                        if k == PROJ_SECOND:
                            proj_copy(-1, None, 0, 0, minus).wait_recv()
                            proj_copy(1, None, 0, 1, minus).wait_recv()
                            for copy in proj_second:
                                copy.start()
                        if k == PROJ_THIRD:
                            proj_copy(2, 0, 0, 2, minus).wait_recv()
                            proj_copy(2, 1, 0, 3, minus).wait_recv()
                            for copy in proj_third:
                                copy.start()
                        if k == WEIGHTS_FIRST:
                            halves.send(0)

        da, db, ea, eb = (jnp.int32(0) for _ in range(4))
        for k, (ka, kb) in enumerate(ITEMS):
            da = jnp.where(i == k, ka, da)
            db = jnp.where(i == k, kb, db)
            ea = jnp.where(i == k + 1, ka, ea)
            eb = jnp.where(i == k + 1, kb, eb)
        own_slot = t.index(da, db)
        twin_slot = t.twin_index(ea, eb)
        pieces.twin_arrived(i - 1, twin_slot)
        own_here = jnp.logical_and(own_slot < me, i < last)
        twin_here = twin_slot < me

        @pl.when(jnp.logical_and(own_here, twin_here))
        def _():
            attend([kv.at[own_slot], kv.at[twin_slot]], q_ref, m_ref, l_ref, acc_ref, rows, const)

        @pl.when(own_here != twin_here)
        def _():
            slot = jnp.where(own_here, own_slot, twin_slot)
            attend([kv.at[slot]], q_ref, m_ref, l_ref, acc_ref, rows, const)

        return carry

    lax.fori_loop(1, last + 1, step, 0)

    for h in range(2):
        attended[:, 128 * h : 128 * (h + 1)] = (acc_ref[h] / l_ref[h]).T.astype(BF16)
    own = rows // 4

    def own_rows(d):
        first = lax.rem(x + d + 4, 4) * own
        return attended.at[pl.ds(pl.multiple_of(first, own), own)]

    heads_out = [
        remote(own_rows(2), row_heads.at[x], x_send.at[0], x_recv.at[0], across),
        remote(own_rows(1), row_heads.at[x], x_send.at[1], x_recv.at[1], plus),
        remote(own_rows(-1), row_heads.at[x], x_send.at[2], x_recv.at[2], minus),
    ]
    for copy in heads_out:
        copy.start()
    row_heads[x] = attended[pl.ds(pl.multiple_of(x * own, own), own), :]

    def weights_step(first, last):
        for k in range(first, last):
            halves.arrived(k)
            halves.send(k)

    weights_step(1, 3)
    for d, sem in ((1, 4), (-1, 5), (2, 6)):
        twin_proj(d, sem).wait_recv()
    for d, sem in ((2, 0), (-1, 1), (1, 2)):
        ref = row_heads.at[lax.rem(x + d + 4, 4)]
        remote(ref, ref, x_send.at[0], x_recv.at[sem], plus).wait_recv()

    lhs = jnp.concatenate([row_heads[p] for p in range(4)], axis=1)
    width = sums.shape[1]

    def project(n, carry):
        cols = pl.ds(pl.multiple_of(n * 256, 256), 256)
        rhs = proj[:, :, cols].reshape(4 * proj.shape[1], 256)
        sums[pl.ds(0, own), cols] = jnp.dot(lhs, rhs, preferred_element_type=F32)
        return carry

    lax.fori_loop(0, width // 256, project, 0)
    mixed[x] = layer_norm(
        residual_weight * stream_v[...].astype(F32) + sums[pl.ds(0, own), :], mix_gain_ref[...]
    ).astype(BF16)

    half = own // 2

    def mixed_copy(d, which, sem, recv, to):
        slot = lax.rem(x + d + 4, 4)
        ref = mixed.at[slot] if which is None else mixed.at[slot, pl.ds(which * half, half)]
        return remote(ref, ref, x_send.at[sem], x_recv.at[recv], to)

    mixed_first = [mixed_copy(0, None, 3, 3, plus), mixed_copy(0, None, 4, 4, minus)]
    mixed_second = [mixed_copy(-1, 0, 5, 5, plus), mixed_copy(1, 1, 6, 6, minus)]
    for copy in mixed_first:
        copy.start()
    weights_step(3, 10)
    mixed_copy(-1, None, 3, 3, plus).wait_recv()
    mixed_copy(1, None, 3, 4, plus).wait_recv()
    for copy in mixed_second:
        copy.start()
    weights_step(10, 13)
    mixed_copy(2, 0, 3, 5, plus).wait_recv()
    mixed_copy(2, 1, 3, 6, plus).wait_recv()
    weights_step(13, 16)
    for k, item in enumerate(ITEMS):
        halves.twin_arrived(k, t.twin_index(*item))

    count = weights.shape[0]
    units = weights.shape[2]

    def feed(first, second):
        into = jnp.concatenate(
            [mixed[lax.rem(x + first + 4, 4)], mixed[lax.rem(x + second + 4, 4)]], axis=0
        )

        gate = jnp.dot(
            into, weights[:, 0:depth, :].reshape(count * depth, units), preferred_element_type=F32
        )
        up = jnp.dot(
            into, weights[:, depth : 2 * depth, :].reshape(count * depth, units), preferred_element_type=F32
        )
        hidden[...] = (gate / (1.0 + jnp.exp(-gate)) * up).astype(BF16)
        sums[...] = lax.dot_general(
            hidden[...],
            weights[:, 2 * depth : 3 * depth, :].reshape(count * depth, units),
            (((1,), (1,)), ((), ())),
            preferred_element_type=F32,
        )

    top, low = pl.ds(0, half), pl.ds(half, half)

    def result_copy(src, src_rows, dst, dst_rows, sem, to):
        s = src.at[src_rows]
        d = dst if dst_rows is None else dst.at[dst_rows]
        return remote(s, d, x_send.at[sem], x_recv.at[sem], to)

    feed(2, 1)
    far_out[...] = sums[0:own, :].astype(BF16)
    plus_out[...] = sums[own : 2 * own, :].astype(BF16)
    back = [
        result_copy(far_out, top, far_minus, None, 7, plus),
        result_copy(far_out, low, far_plus, None, 8, minus),
        result_copy(plus_out, low, from_minus, low, 9, plus),
        result_copy(minus_out, top, from_plus, top, 10, minus),
        result_copy(plus_out, top, from_minus, top, 11, plus),
        result_copy(minus_out, low, from_plus, low, 12, minus),
    ]
    for copy in back[:3]:
        copy.start()
    feed(-1, 0)
    minus_out[...] = sums[0:own, :].astype(BF16)
    back[3].start()
    back[0].wait_recv()
    plus_out[top, :] = (plus_out[top, :].astype(F32) + far_minus[...].astype(F32)).astype(BF16)
    back[4].start()
    back[1].wait_recv()
    minus_out[low, :] = (minus_out[low, :].astype(F32) + far_plus[...].astype(F32)).astype(BF16)
    back[5].start()
    for copy in back[2:]:
        copy.wait_recv()
    lowered = sums[own : 2 * own, :] + from_plus[...].astype(F32) + from_minus[...].astype(F32)
    out_ref[...] = layer_norm(
        residual_weight * mixed[x].astype(F32) + 0.5 * lowered, mlp_gain_ref[...]
    ).astype(BF16)

    pieces.sent()
    halves.sent()
    for copy in proj_first + proj_second + proj_third + heads_out + mixed_first + mixed_second + back:
        copy.wait_send()


PROJ_SECOND = 5
PROJ_THIRD = 9
WEIGHTS_FIRST = 12


def per_device(
    queries_nope,
    queries_rope,
    latent,
    rope_key,
    latent_gain,
    key_up,
    value_up,
    out_proj,
    stream,
    mix_gain,
    w_gate,
    w_up,
    w_down,
    mlp_gain,
):
    rows, heads, head_dim = queries_nope.shape
    rope_dim = queries_rope.shape[2]
    count = lax.axis_size("sp")
    tp = lax.axis_size("tp")
    own, width = stream.shape
    units = w_gate.shape[1]
    const = (head_dim + rope_dim) ** (-0.5) * math.log2(math.e)
    lanes = heads * rope_dim
    inner, outer = turn_tables(rows, count, rope_dim)
    slab = 4 * rows + rows // 2
    vmem = pl.BlockSpec(memory_space=pltpu.VMEM)
    hbm = pl.BlockSpec(memory_space=pl.ANY)
    dma = pltpu.SemaphoreType.DMA
    return pl.pallas_call(
        functools.partial(whole_kernel, rows, const),
        out_shape=jax.ShapeDtypeStruct((own, width), BF16),
        in_specs=[hbm] * 13 + [vmem] * 3,
        out_specs=vmem,
        scratch_shapes=[
            pltpu.VMEM(latent.shape, BF16),
            pltpu.VMEM((rope_dim, rows), BF16),
            pltpu.VMEM(key_up.shape, BF16),
            pltpu.VMEM(value_up.shape, BF16),
            pltpu.VMEM(inner.shape, F32),
            pltpu.VMEM(outer.shape[1:], F32),
            pltpu.VMEM(queries_nope.shape, BF16),
            pltpu.VMEM((lanes, rows), BF16),
            pltpu.VMEM((own, width), BF16),
            pltpu.VMEM((2 * heads, 2 * head_dim, rows), BF16),
            pltpu.VMEM((count, slab, 128), BF16),
            pltpu.VMEM((count, 3 * w_gate.shape[0], units), BF16),
            pltpu.VMEM((tp, *out_proj.shape), BF16),
            pltpu.VMEM((2, 1, rows), F32),
            pltpu.VMEM((2, 1, rows), F32),
            pltpu.VMEM((2, 128, rows), F32),
            pltpu.VMEM((rows, heads * head_dim), BF16),
            pltpu.VMEM((tp, own, heads * head_dim), BF16),
            pltpu.VMEM((2 * own, width), F32),
            pltpu.VMEM((tp, own, width), BF16),
            pltpu.VMEM((2 * own, units), BF16),
            pltpu.VMEM((own, width), BF16),
            pltpu.VMEM((own, width), BF16),
            pltpu.VMEM((own, width), BF16),
            pltpu.VMEM((own // 2, width), BF16),
            pltpu.VMEM((own // 2, width), BF16),
            pltpu.VMEM((own, width), BF16),
            pltpu.VMEM((own, width), BF16),
            dma((13,)),
            dma((16, 5)),
            dma((16, 2)),
            dma((16,)),
            dma((16, 5)),
            dma((16, 2)),
            dma((16,)),
            dma((7,)),
            dma((7,)),
            dma((13,)),
            dma((13,)),
        ],
        compiler_params=pltpu.CompilerParams(
            collective_id=0, has_side_effects=True, vmem_limit_bytes=60 * 1024 * 1024
        ),
        name="layer",
    )(
        latent,
        rope_key.T,
        key_up,
        value_up,
        inner,
        queries_nope,
        jnp.transpose(queries_rope, (1, 2, 0)).reshape(lanes, rows),
        out_proj,
        w_gate,
        w_up,
        w_down.T,
        stream,
        outer,
        latent_gain.reshape(1, -1),
        mix_gain.reshape(1, -1),
        mlp_gain.reshape(1, -1),
    )


def solution(mesh):
    return jax.shard_map(
        per_device,
        mesh=mesh,
        in_specs=(
            P("sp", "tp", None),
            P("sp", "tp", None),
            P("sp", None),
            P("sp", None),
            P(),
            P(None, "tp"),
            P(None, "tp"),
            P("tp", None),
            P(("sp", "tp"), None),
            P(),
            P("sp", "tp"),
            P("sp", "tp"),
            P("tp", "sp"),
            P(),
        ),
        out_specs=P(("sp", "tp"), None),
        check_vma=False,
    )
```

```python
import functools
import math

import jax
import jax.numpy as jnp
import numpy as np
from jax import lax
from jax.experimental import pallas as pl
from jax.experimental.pallas import tpu as pltpu
from jax.sharding import PartitionSpec as P

theta_base = 10000.0
residual_weight = 8.0**0.25
norm_floor = 1.0
big_negative = -1e30
F32 = jnp.float32
BF16 = jnp.bfloat16


def turn_tables(rows, count, rope_dim):
    rates = theta_base ** (-2.0 * np.arange(rope_dim // 2) / rope_dim)[:, None]
    inner = rates * np.arange(rows)
    outer = (rates * (np.arange(count) * rows)).T[:, :, None] + np.zeros((1, 1, 128))
    pair = lambda angle: jnp.asarray(np.stack([np.cos(angle), np.sin(angle)]), F32)
    return pair(inner), jnp.moveaxis(pair(outer), 0, 1)


def turn(v, cosine, sine):
    half = v.shape[0] // 2
    a, b = v[:half], v[half:]
    return jnp.concatenate([a * cosine - b * sine, a * sine + b * cosine], axis=0)


def layer_norm(values, gain):
    centre = jnp.mean(values, axis=-1, keepdims=True)
    centred = values - centre
    spread = jnp.mean(centred * centred, axis=-1, keepdims=True)
    return centred * lax.rsqrt(spread + norm_floor) * gain


def scores(kv, h, q_ref, rows, const):
    half = rows // 2
    r = kv[4 * rows : 4 * rows + half, :]
    top = jnp.concatenate([kv[h * rows : h * rows + half, :], r], axis=1)
    low = jnp.concatenate([kv[h * rows + half : (h + 1) * rows, :], r], axis=1)
    both = [
        jnp.dot(top, q_ref[2 * h], preferred_element_type=F32),
        jnp.dot(low, q_ref[2 * h + 1], preferred_element_type=F32),
    ]
    return jnp.concatenate(both, axis=0) * const


def values_of(kv, h, rows):
    at = 2 * rows + h * rows
    return [kv[at + 128 * i : at + 128 * (i + 1), :] for i in range(rows // 128)]


def attend(pieces, q_ref, m_ref, l_ref, acc_ref, rows, const, diag=False):
    for h in range(2):
        s = jnp.concatenate([scores(kv, h, q_ref, rows, const) for kv in pieces], axis=0)
        if diag:
            key = lax.broadcasted_iota(jnp.int32, s.shape, 0)
            query = lax.broadcasted_iota(jnp.int32, s.shape, 1)
            s = jnp.where(key <= query, s, big_negative)
        m_old = m_ref[h]
        m_new = jnp.maximum(m_old, jnp.max(s, axis=0, keepdims=True))
        p = jnp.exp2(s - m_new)
        alpha = jnp.exp2(m_old - m_new)
        l_ref[h] = l_ref[h] * alpha + jnp.sum(p, axis=0, keepdims=True)
        m_ref[h] = m_new
        vt = jnp.concatenate([block for kv in pieces for block in values_of(kv, h, rows)], axis=1)
        acc_ref[h] = acc_ref[h] * alpha + jnp.dot(vt, p.astype(BF16), preferred_element_type=F32)


MESH = pl.DeviceIdType.MESH
ITEMS = (
    (0, 0), (-1, 0), (1, 0), (0, -1), (0, 1), (2, 0), (-1, -1), (-1, 1),
    (1, -1), (1, 1), (0, 2), (2, -1), (2, 1), (-1, 2), (1, 2), (2, 2),
)
PLACE = {item: k for k, item in enumerate(ITEMS)}


def remote(src, dst, send_sem, recv_sem, device):
    return pltpu.make_async_remote_copy(
        src_ref=src, dst_ref=dst, send_sem=send_sem, recv_sem=recv_sem, device_id=device, device_id_type=MESH
    )


class Torus:
    def __init__(self):
        self.me = lax.axis_index("sp")
        self.x = lax.axis_index("tp")
        self.c = lax.rem(self.me, 2)
        chip = self.me // 2
        z, y = chip // 4, lax.rem(chip, 4)
        self.a = z + self.c * (y - z)
        self.b = y + self.c * (z - y)
        self.step_a = 8 - 6 * self.c
        self.step_b = 2 + 6 * self.c

    def index(self, da, db):
        at_a = lax.rem(self.a + da + 4, 4)
        at_b = lax.rem(self.b + db + 4, 4)
        return at_a * self.step_a + at_b * self.step_b + self.c

    def twin_index(self, da, db):
        at_b = lax.rem(self.b + da + 4, 4)
        at_a = lax.rem(self.a + db + 4, 4)
        return at_a * self.step_a + at_b * self.step_b + 1 - self.c

    def at(self, da, db):
        return (self.index(da, db), self.x)

    def twin(self):
        return (self.me + 1 - 2 * self.c, self.x)

    def along_x(self, d):
        return (self.me, lax.rem(self.x + d + 4, 4))


class Gather:
    def __init__(self, torus, buf, parts, send_sem, recv_sems, twin_sems, twin_of):
        self.torus, self.buf, self.parts = torus, buf, parts
        self.send_sem, self.recv_sems, self.twin_sems, self.twin_of = send_sem, recv_sems, twin_sems, twin_of

    def ref(self, slot, part, which=None):
        begin, size = self.parts[part]
        if which is not None:
            size //= 2
            begin += which * size
        return self.buf.at[slot, pl.ds(begin, size)]

    def copies(self, k, part):
        t = self.torus
        da, db = ITEMS[k]
        slot = t.index(da, db)
        plan = []
        if db == 0:
            if da == 0:
                plan += [((1, 0), (-1, 0), None), ((-1, 0), (1, 0), None)]
            plan += [((0, 1), (da, -1), None), ((0, -1), (da, 1), None)]
            if da == -1:
                plan += [((1, 0), (2, 0), 0)]
            if da == 1:
                plan += [((-1, 0), (2, 0), 1)]
        if db == -1:
            plan += [((0, 1), (da, 2), 0)]
        if db == 1:
            plan += [((0, -1), (da, 2), 1)]
        out = []
        for to, name, which in plan:
            ref = self.ref(slot, part, which)
            out.append(remote(ref, ref, self.send_sem, self.recv_sems.at[PLACE[name], part], t.at(*to)))
        ref = self.ref(slot, part)
        out.append(remote(ref, ref, self.send_sem, self.twin_sems.at[self.twin_of(k)], t.twin()))
        return out

    def send(self, k, part):
        for copy in self.copies(k, part):
            copy.start()

    def sent(self):
        ref = self.buf.at[pl.ds(0, 31)]
        remote(ref, ref, self.send_sem, self.recv_sems.at[0, 0], self.torus.twin()).wait_send()

    def arrived(self, k, part):
        ref = self.ref(self.torus.index(*ITEMS[k]), part)
        remote(ref, ref, self.send_sem, self.recv_sems.at[k, part], self.torus.twin()).wait_recv()

    def pass_on(self, k, part):
        self.arrived(k, part)
        self.send(k, part)

    def twin_arrived(self, sem, first, count):
        ref = self.buf.at[pl.ds(first, count)]
        remote(ref, ref, self.send_sem, self.twin_sems.at[sem], self.torus.twin()).wait_recv()


def whole_kernel(
    rows,
    const,
    latent_hbm,
    rope_key_hbm,
    key_up_hbm,
    value_up_hbm,
    inner_hbm,
    qn_hbm,
    qr_hbm,
    proj_hbm,
    gate_hbm,
    up_hbm,
    down_hbm,
    stream_hbm,
    outer_hbm,
    latent_gain_ref,
    mix_gain_ref,
    mlp_gain_ref,
    out_ref,
    latent_v,
    rope_key_v,
    key_up_v,
    value_up_v,
    inner_v,
    outer_v,
    qn_v,
    qr_v,
    q_ref,
    kv,
    weights,
    proj,
    m_ref,
    l_ref,
    acc_ref,
    heads_all,
    stream_all,
    sums,
    mixed,
    hidden,
    gate_sum,
    up_sum,
    far_out,
    plus_out,
    minus_out,
    far_plus,
    far_minus,
    from_plus,
    from_minus,
    load_sems,
    kv_send,
    kv_recv,
    kv_twin,
    w_send,
    w_recv,
    w_twin,
    proj_send,
    proj_recv,
    ring_send,
    ring_recv,
    x_send,
    x_recv,
):
    t = Torus()
    me, x = t.me, t.x
    depth = weights.shape[1] // 3
    loads = [
        pltpu.make_async_copy(src, dst, load_sems.at[n])
        for n, (src, dst) in enumerate(
            (
                (latent_hbm, latent_v),
                (key_up_hbm, key_up_v),
                (value_up_hbm, value_up_v),
                (rope_key_hbm, rope_key_v),
                (inner_hbm, inner_v),
                (outer_hbm.at[me], outer_v),
                (proj_hbm, proj.at[x]),
                (qn_hbm, qn_v),
                (qr_hbm, qr_v),
                (down_hbm, weights.at[me, pl.ds(2 * depth, depth)]),
                (gate_hbm, weights.at[me, pl.ds(0, depth)]),
                (up_hbm, weights.at[me, pl.ds(depth, depth)]),
                (stream_hbm, stream_all.at[x]),
            )
        )
    ]
    for load in loads:
        load.start()

    plus, minus, across = t.along_x(1), t.along_x(-1), t.along_x(2)
    peers = (t.at(1, 0), t.at(-1, 0), t.at(0, 1), t.at(0, -1), t.twin(), plus, minus, across)
    barrier = pltpu.get_barrier_semaphore()
    for peer in peers:
        pl.semaphore_signal(barrier, inc=1, device_id=peer, device_id_type=MESH)

    slab_rows = kv.shape[1]
    pieces = Gather(t, kv, [(0, slab_rows // 2), (slab_rows // 2, slab_rows // 2)], kv_send.at[0], kv_recv, kv_twin, lambda k: k)
    halves = Gather(t, weights, [(0, 3 * depth)], w_send.at[0], w_recv, w_twin, lambda k: k // EARLY)

    class Ring:
        def __init__(self, buf, send_sem, first_sem):
            self.buf, self.send_sem, self.first_sem, self.half = buf, send_sem, first_sem, buf.shape[1] // 2

        def copy(self, d, which, sem, to):
            ref = self.buf.at[lax.rem(x + d + 4, 4), pl.ds(which * self.half, self.half)]
            n = self.first_sem + sem
            return remote(ref, ref, self.send_sem, ring_recv.at[n], to)

        def first(self):
            return [
                self.copy(0, 0, 0, plus),
                self.copy(0, 1, 1, minus),
                self.copy(0, 1, 2, plus),
                self.copy(0, 0, 3, minus),
            ]

        def second(self, which):
            return self.copy(1, 1, 5, minus) if which else self.copy(-1, 0, 4, plus)

        def forward(self):
            for d, which in ((-1, 0), (1, 1)):
                self.copy(d, which, which, plus).wait_recv()
                self.second(which).start()

        def near_arrived(self):
            self.copy(-1, 1, 2, plus).wait_recv()
            self.copy(1, 0, 3, plus).wait_recv()

        def far_arrived(self):
            self.copy(2, 0, 4, plus).wait_recv()
            self.copy(2, 1, 5, plus).wait_recv()

    stream_ring = Ring(stream_all, ring_send.at[0], 0)
    heads_ring = Ring(heads_all, ring_send.at[1], 6)

    share = proj.shape[1] // 2

    def proj_part(d, which):
        slot = lax.rem(x + d + 4, 4)
        size = share if which is None else share // 2
        first = t.c * share + (0 if which is None else which * size)
        return proj.at[slot, pl.ds(pl.multiple_of(first, size), size)]

    def proj_copy(d, which, sem, recv, to):
        ref = proj_part(d, which)
        return remote(ref, ref, proj_send.at[0], proj_recv.at[recv], to)

    proj_first = [proj_copy(0, None, 0, 0, plus), proj_copy(0, None, 1, 1, minus)]
    proj_second = [
        proj_copy(-1, 0, 2, 2, plus),
        proj_copy(1, 1, 3, 3, minus),
        proj_copy(-1, None, 4, 4, t.twin()),
        proj_copy(1, None, 5, 5, t.twin()),
    ]
    proj_third = [proj_copy(2, None, 6, 6, t.twin())]

    def twin_proj(d, recv):
        slot = lax.rem(x + d + 4, 4)
        first = (1 - t.c) * share
        ref = proj.at[slot, pl.ds(pl.multiple_of(first, share), share)]
        return remote(ref, ref, proj_send.at[0], proj_recv.at[recv], t.twin())

    for load in loads[:6]:
        load.wait()
    wide = latent_v[...].astype(F32)
    factor = lax.rsqrt(jnp.mean(wide * wide, axis=-1, keepdims=True) + norm_floor)
    normed = (wide * factor * latent_gain_ref[...]).astype(BF16)
    slab = kv.at[me]
    keys = jnp.dot(normed, key_up_v[...], preferred_element_type=F32).astype(BF16)
    values = jnp.dot(normed, value_up_v[...], preferred_element_type=F32)
    for h in range(2):
        slab[h * rows : (h + 1) * rows, :] = keys[:, 128 * h : 128 * (h + 1)]
        turned = values[:, 128 * h : 128 * (h + 1)].T.astype(BF16)
        for i in range(rows // 128):
            at = 2 * rows + h * rows + 128 * i
            slab[at : at + 128, :] = turned[:, 128 * i : 128 * (i + 1)]
    outer_cos, outer_sin = outer_v[0, :, 0:1], outer_v[1, :, 0:1]
    inner_cos, inner_sin = inner_v[0], inner_v[1]
    cosine = outer_cos * inner_cos - outer_sin * inner_sin
    sine = outer_sin * inner_cos + outer_cos * inner_sin
    mid = rows // 2
    key_turned = turn(rope_key_v[...].astype(F32), cosine, sine).T
    slab[4 * rows : 4 * rows + mid, :] = jnp.concatenate([key_turned[:mid], key_turned[mid:]], axis=1).astype(BF16)

    pl.semaphore_wait(barrier, len(peers))
    for part in range(2):
        pieces.send(0, part)
    loads[6].wait()
    for copy in proj_first:
        copy.start()

    for load in loads[7:]:
        load.wait()
    for copy in stream_ring.first():
        copy.start()
    zeros = jnp.zeros((64, rows), BF16)
    for h in range(2):
        nope = qn_v[:, h, :].astype(F32).T.astype(BF16)
        rotary = turn(qr_v[64 * h : 64 * (h + 1), :].astype(F32), cosine, sine).astype(BF16)
        for odd in range(2):
            q_ref[2 * h + odd, 0:128, :] = nope
            q_ref[2 * h + odd, 128:192, :] = zeros if odd else rotary
            q_ref[2 * h + odd, 192:256, :] = rotary if odd else zeros

    m_ref[...] = jnp.full_like(m_ref, big_negative)
    l_ref[...] = jnp.zeros_like(l_ref)
    acc_ref[...] = jnp.zeros_like(acc_ref)
    attend([kv.at[me]], q_ref, m_ref, l_ref, acc_ref, rows, const, diag=True)

    last = len(ITEMS)

    def step(i, carry):
        for group in range(0, last, 4):

            @pl.when(i // 4 == group // 4)
            def _():
                for k in range(max(group, 1), group + 4):

                    @pl.when(i == k)
                    def _():
                        for begin, end in GROUPS:
                            if k == begin:
                                for other in range(begin, end):
                                    pieces.pass_on(other, 0)
                        pieces.pass_on(k, 1)
                        if k == PROJ_SECOND:
                            proj_copy(-1, None, 0, 0, minus).wait_recv()
                            proj_copy(1, None, 0, 1, minus).wait_recv()
                            for copy in proj_second:
                                copy.start()
                        if k == PROJ_THIRD:
                            proj_copy(2, 0, 0, 2, minus).wait_recv()
                            proj_copy(2, 1, 0, 3, minus).wait_recv()
                            for copy in proj_third:
                                copy.start()
                            stream_ring.forward()
                        if k == WEIGHTS_FIRST:
                            halves.send(0, 0)

        da, db, ea, eb = (jnp.int32(0) for _ in range(4))
        for k, (ka, kb) in enumerate(ITEMS):
            da = jnp.where(i == k, ka, da)
            db = jnp.where(i == k, kb, db)
            ea = jnp.where(i == k + 1, ka, ea)
            eb = jnp.where(i == k + 1, kb, eb)
        own_slot = t.index(da, db)
        twin_slot = t.twin_index(ea, eb)
        pieces.twin_arrived(i - 1, twin_slot, 1)
        own_here = jnp.logical_and(own_slot < me, i < last)
        twin_here = twin_slot < me

        @pl.when(jnp.logical_and(own_here, twin_here))
        def _():
            attend([kv.at[own_slot], kv.at[twin_slot]], q_ref, m_ref, l_ref, acc_ref, rows, const)

        @pl.when(own_here != twin_here)
        def _():
            slot = jnp.where(own_here, own_slot, twin_slot)
            attend([kv.at[slot]], q_ref, m_ref, l_ref, acc_ref, rows, const)

        return carry

    lax.fori_loop(1, last + 1, step, 0)

    own = rows // 4
    for h in range(2):
        heads_all[x, :, 128 * h : 128 * (h + 1)] = (acc_ref[h] / l_ref[h]).T.astype(BF16)
    for copy in heads_ring.first():
        copy.start()
    for k in range(1, 5):
        halves.pass_on(k, 0)
    stream_ring.near_arrived()
    stream_ring.far_arrived()
    for d, sem in ((1, 4), (-1, 5), (2, 6)):
        twin_proj(d, sem).wait_recv()
    heads_ring.forward()
    heads_ring.near_arrived()

    def slots(ref, offsets, axis):
        return jnp.concatenate([ref[lax.rem(x + d + 4, 4)] for d in offsets], axis=axis)

    halves.pass_on(5, 0)
    near = (0, 1, -1)
    sums[...] = jnp.dot(slots(heads_all, near, 1), slots(proj, near, 0), preferred_element_type=F32)
    for k in range(6, 10):
        halves.pass_on(k, 0)
    heads_ring.far_arrived()
    sums[...] += jnp.dot(slots(heads_all, (2,), 1), slots(proj, (2,), 0), preferred_element_type=F32)

    def norm_rows(n, carry):
        total = sums[pl.ds(pl.multiple_of(n * own, own), own), :]
        mixed[n] = layer_norm(residual_weight * stream_all[n].astype(F32) + total, mix_gain_ref[...]).astype(BF16)
        return carry

    lax.fori_loop(0, 4, norm_rows, 0)
    count, units = weights.shape[0], weights.shape[2]
    halves.pass_on(10, 0)
    halves.twin_arrived(0, 0, EARLY)

    def expand(items):
        chips = [t.index(*item) // 2 for item in items]
        into = jnp.concatenate(
            [mixed[:, :, pl.ds(pl.multiple_of(chip * 2 * depth, 2 * depth), 2 * depth)].reshape(rows, 2 * depth) for chip in chips],
            axis=1,
        )

        def rhs(begin):
            blocks = [weights[pl.ds(chip * 2, 2), begin : begin + depth, :].reshape(2 * depth, units) for chip in chips]
            return jnp.concatenate(blocks, axis=0)

        return [jnp.dot(into, rhs(begin), preferred_element_type=F32) for begin in (0, depth)]

    gate_sum[...], up_sum[...] = expand(ITEMS[:EARLY])
    for k in range(EARLY, 16):
        halves.pass_on(k, 0)
    halves.twin_arrived(1, 0, 16 - EARLY)
    gate, up = expand(ITEMS[EARLY:])
    gate = gate_sum[...] + gate
    hidden[...] = (gate / (1.0 + jnp.exp(-gate)) * (up_sum[...] + up)).astype(BF16)

    def lower(first, second):
        rows_of = [hidden[pl.ds(pl.multiple_of(lax.rem(x + d + 4, 4) * own, own), own), :] for d in (first, second)]
        sums[0 : 2 * own, :] = lax.dot_general(
            jnp.concatenate(rows_of, axis=0),
            weights[:, 2 * depth : 3 * depth, :].reshape(count * depth, units),
            (((1,), (1,)), ((), ())),
            preferred_element_type=F32,
        )

    half = own // 2
    top, low = pl.ds(0, half), pl.ds(half, half)

    def result_copy(src, src_rows, dst, dst_rows, sem, to):
        s = src.at[src_rows]
        d = dst if dst_rows is None else dst.at[dst_rows]
        return remote(s, d, x_send.at[0], x_recv.at[sem - 7], to)

    lower(2, 1)
    far_out[...] = sums[0:own, :].astype(BF16)
    plus_out[...] = sums[own : 2 * own, :].astype(BF16)
    back = [
        result_copy(far_out, top, far_minus, None, 7, plus),
        result_copy(far_out, low, far_plus, None, 8, minus),
        result_copy(plus_out, low, from_minus, low, 9, plus),
        result_copy(minus_out, top, from_plus, top, 10, minus),
        result_copy(plus_out, top, from_minus, top, 11, plus),
        result_copy(minus_out, low, from_plus, low, 12, minus),
    ]
    for copy in back[:3]:
        copy.start()
    lower(-1, 0)
    minus_out[...] = sums[0:own, :].astype(BF16)
    back[3].start()
    back[0].wait_recv()
    plus_out[top, :] = (plus_out[top, :].astype(F32) + far_minus[...].astype(F32)).astype(BF16)
    back[4].start()
    back[1].wait_recv()
    minus_out[low, :] = (minus_out[low, :].astype(F32) + far_plus[...].astype(F32)).astype(BF16)
    back[5].start()
    for copy in back[2:]:
        copy.wait_recv()
    lowered = sums[own : 2 * own, :] + from_plus[...].astype(F32) + from_minus[...].astype(F32)
    out_ref[...] = layer_norm(
        residual_weight * mixed[x].astype(F32) + 0.5 * lowered, mlp_gain_ref[...]
    ).astype(BF16)

    pieces.sent()
    halves.sent()
    for ref, sem in (
        (proj.at[pl.ds(0, 3)], proj_send.at[0]),
        (stream_all.at[pl.ds(0, 3)], ring_send.at[0]),
        (heads_all.at[pl.ds(0, 3)], ring_send.at[1]),
        (mixed.at[pl.ds(0, 3)], x_send.at[0]),
    ):
        remote(ref, ref, sem, x_recv.at[0], t.twin()).wait_send()


GROUPS = ((1, 5), (5, 11), (11, 15), (15, 16))
EARLY = 11
PROJ_SECOND = 5
PROJ_THIRD = 9
WEIGHTS_FIRST = 12


def per_device(
    queries_nope,
    queries_rope,
    latent,
    rope_key,
    latent_gain,
    key_up,
    value_up,
    out_proj,
    stream,
    mix_gain,
    w_gate,
    w_up,
    w_down,
    mlp_gain,
):
    rows, heads, head_dim = queries_nope.shape
    rope_dim = queries_rope.shape[2]
    count = lax.axis_size("sp")
    tp = lax.axis_size("tp")
    own, width = stream.shape
    units = w_gate.shape[1]
    const = (head_dim + rope_dim) ** (-0.5) * math.log2(math.e)
    lanes = heads * rope_dim
    inner, outer = turn_tables(rows, count, rope_dim)
    slab = 4 * rows + rows // 2
    vmem = pl.BlockSpec(memory_space=pltpu.VMEM)
    hbm = pl.BlockSpec(memory_space=pl.ANY)
    dma = pltpu.SemaphoreType.DMA
    return pl.pallas_call(
        functools.partial(whole_kernel, rows, const),
        out_shape=jax.ShapeDtypeStruct((own, width), BF16),
        in_specs=[hbm] * 13 + [vmem] * 3,
        out_specs=vmem,
        scratch_shapes=[
            pltpu.VMEM(latent.shape, BF16),
            pltpu.VMEM((rope_dim, rows), BF16),
            pltpu.VMEM(key_up.shape, BF16),
            pltpu.VMEM(value_up.shape, BF16),
            pltpu.VMEM(inner.shape, F32),
            pltpu.VMEM(outer.shape[1:], F32),
            pltpu.VMEM(queries_nope.shape, BF16),
            pltpu.VMEM((lanes, rows), BF16),
            pltpu.VMEM((2 * heads, 2 * head_dim, rows), BF16),
            pltpu.VMEM((count, slab, 128), BF16),
            pltpu.VMEM((count, 3 * w_gate.shape[0], units), BF16),
            pltpu.VMEM((tp, *out_proj.shape), BF16),
            pltpu.VMEM((2, 1, rows), F32),
            pltpu.VMEM((2, 1, rows), F32),
            pltpu.VMEM((2, 128, rows), F32),
            pltpu.VMEM((tp, rows, heads * head_dim), BF16),
            pltpu.VMEM((tp, own, width), BF16),
            pltpu.VMEM((rows, width), F32),
            pltpu.VMEM((tp, own, width), BF16),
            pltpu.VMEM((rows, units), BF16),
            pltpu.VMEM((rows, units), F32),
            pltpu.VMEM((rows, units), F32),
            pltpu.VMEM((own, width), BF16),
            pltpu.VMEM((own, width), BF16),
            pltpu.VMEM((own, width), BF16),
            pltpu.VMEM((own // 2, width), BF16),
            pltpu.VMEM((own // 2, width), BF16),
            pltpu.VMEM((own, width), BF16),
            pltpu.VMEM((own, width), BF16),
            dma((13,)),
            dma((1,)),
            dma((16, 2)),
            dma((16,)),
            dma((1,)),
            dma((16, 1)),
            dma((2,)),
            dma((1,)),
            dma((7,)),
            dma((2,)),
            dma((12,)),
            dma((1,)),
            dma((6,)),
        ],
        compiler_params=pltpu.CompilerParams(
            collective_id=0, has_side_effects=True, vmem_limit_bytes=60 * 1024 * 1024
        ),
        name="layer",
    )(
        latent,
        rope_key.T,
        key_up,
        value_up,
        inner,
        queries_nope,
        jnp.transpose(queries_rope, (1, 2, 0)).reshape(lanes, rows),
        out_proj,
        w_gate,
        w_up,
        w_down.T,
        stream,
        outer,
        latent_gain.reshape(1, -1),
        mix_gain.reshape(1, -1),
        mlp_gain.reshape(1, -1),
    )


def solution(mesh):
    return jax.shard_map(
        per_device,
        mesh=mesh,
        in_specs=(
            P("sp", "tp", None),
            P("sp", "tp", None),
            P("sp", None),
            P("sp", None),
            P(),
            P(None, "tp"),
            P(None, "tp"),
            P("tp", None),
            P(("sp", "tp"), None),
            P(),
            P("sp", "tp"),
            P("sp", "tp"),
            P("tp", "sp"),
            P(),
        ),
        out_specs=P(("sp", "tp"), None),
        check_vma=False,
    )
```

```python
import functools
import math

import jax
import jax.numpy as jnp
import numpy as np
from jax import lax
from jax.experimental import pallas as pl
from jax.experimental.pallas import tpu as pltpu
from jax.sharding import PartitionSpec as P

theta_base = 10000.0
residual_weight = 8.0**0.25
norm_floor = 1.0
big_negative = -1e30
F32 = jnp.float32
BF16 = jnp.bfloat16


def turn_tables(rows, count, rope_dim):
    rates = theta_base ** (-2.0 * np.arange(rope_dim // 2) / rope_dim)[:, None]
    inner = rates * np.arange(rows)
    outer = (rates * (np.arange(count) * rows)).T[:, :, None] + np.zeros((1, 1, 128))
    pair = lambda angle: jnp.asarray(np.stack([np.cos(angle), np.sin(angle)]), F32)
    return pair(inner), jnp.moveaxis(pair(outer), 0, 1)


def turn(v, cosine, sine):
    half = v.shape[0] // 2
    a, b = v[:half], v[half:]
    return jnp.concatenate([a * cosine - b * sine, a * sine + b * cosine], axis=0)


def layer_norm(values, gain):
    centre = jnp.mean(values, axis=-1, keepdims=True)
    centred = values - centre
    spread = jnp.mean(centred * centred, axis=-1, keepdims=True)
    return centred * lax.rsqrt(spread + norm_floor) * gain


def scores(kv, h, q_ref, rows, const):
    half = rows // 2
    r = kv[4 * rows : 4 * rows + half, :]
    top = jnp.concatenate([kv[h * rows : h * rows + half, :], r], axis=1)
    low = jnp.concatenate([kv[h * rows + half : (h + 1) * rows, :], r], axis=1)
    both = [
        jnp.dot(top, q_ref[2 * h], preferred_element_type=F32),
        jnp.dot(low, q_ref[2 * h + 1], preferred_element_type=F32),
    ]
    return jnp.concatenate(both, axis=0) * const


def values_of(kv, h, rows):
    at = 2 * rows + h * rows
    return [kv[at + 128 * i : at + 128 * (i + 1), :] for i in range(rows // 128)]


def attend(pieces, q_ref, m_ref, l_ref, acc_ref, rows, const, diag=False):
    for h in range(2):
        s = jnp.concatenate([scores(kv, h, q_ref, rows, const) for kv in pieces], axis=0)
        if diag:
            key = lax.broadcasted_iota(jnp.int32, s.shape, 0)
            query = lax.broadcasted_iota(jnp.int32, s.shape, 1)
            s = jnp.where(key <= query, s, big_negative)
        m_old = m_ref[h]
        m_new = jnp.maximum(m_old, jnp.max(s, axis=0, keepdims=True))
        p = jnp.exp2(s - m_new)
        alpha = jnp.exp2(m_old - m_new)
        l_ref[h] = l_ref[h] * alpha + jnp.sum(p, axis=0, keepdims=True)
        m_ref[h] = m_new
        vt = jnp.concatenate([block for kv in pieces for block in values_of(kv, h, rows)], axis=1)
        acc_ref[h] = acc_ref[h] * alpha + jnp.dot(vt, p.astype(BF16), preferred_element_type=F32)


MESH = pl.DeviceIdType.MESH
ITEMS = (
    (0, 0), (-1, 0), (1, 0), (0, -1), (0, 1), (2, 0), (-1, -1), (-1, 1),
    (1, -1), (1, 1), (0, 2), (2, -1), (2, 1), (-1, 2), (1, 2), (2, 2),
)
PLACE = {item: k for k, item in enumerate(ITEMS)}


def remote(src, dst, send_sem, recv_sem, device):
    return pltpu.make_async_remote_copy(
        src_ref=src, dst_ref=dst, send_sem=send_sem, recv_sem=recv_sem, device_id=device, device_id_type=MESH
    )


class Torus:
    def __init__(self):
        self.me = lax.axis_index("sp")
        self.x = lax.axis_index("tp")
        self.c = lax.rem(self.me, 2)
        chip = self.me // 2
        z, y = chip // 4, lax.rem(chip, 4)
        self.a = z + self.c * (y - z)
        self.b = y + self.c * (z - y)
        self.step_a = 8 - 6 * self.c
        self.step_b = 2 + 6 * self.c

    def index(self, da, db):
        at_a = lax.rem(self.a + da + 4, 4)
        at_b = lax.rem(self.b + db + 4, 4)
        return at_a * self.step_a + at_b * self.step_b + self.c

    def twin_index(self, da, db):
        at_b = lax.rem(self.b + da + 4, 4)
        at_a = lax.rem(self.a + db + 4, 4)
        return at_a * self.step_a + at_b * self.step_b + 1 - self.c

    def at(self, da, db):
        return (self.index(da, db), self.x)

    def twin(self):
        return (self.me + 1 - 2 * self.c, self.x)

    def along_x(self, d):
        return (self.me, lax.rem(self.x + d + 4, 4))


class Gather:
    def __init__(self, torus, buf, parts, send_sem, recv_sems, twin_sems, twin_of):
        self.torus, self.buf, self.parts = torus, buf, parts
        self.send_sem, self.recv_sems, self.twin_sems, self.twin_of = send_sem, recv_sems, twin_sems, twin_of

    def ref(self, slot, part, which=None):
        begin, size = self.parts[part]
        if which is not None:
            size //= 2
            begin += which * size
        return self.buf.at[slot, pl.ds(begin, size)]

    def copies(self, k, part):
        t = self.torus
        da, db = ITEMS[k]
        slot = t.index(da, db)
        plan = []
        if db == 0:
            if da == 0:
                plan += [((1, 0), (-1, 0), None), ((-1, 0), (1, 0), None)]
            plan += [((0, 1), (da, -1), None), ((0, -1), (da, 1), None)]
            if da == -1:
                plan += [((1, 0), (2, 0), 0)]
            if da == 1:
                plan += [((-1, 0), (2, 0), 1)]
        if db == -1:
            plan += [((0, 1), (da, 2), 0)]
        if db == 1:
            plan += [((0, -1), (da, 2), 1)]
        out = []
        for to, name, which in plan:
            ref = self.ref(slot, part, which)
            out.append(remote(ref, ref, self.send_sem, self.recv_sems.at[PLACE[name], part], t.at(*to)))
        ref = self.ref(slot, part)
        out.append(remote(ref, ref, self.send_sem, self.twin_sems.at[self.twin_of(k, part)], t.twin()))
        return out

    def send(self, k, part):
        for copy in self.copies(k, part):
            copy.start()

    def sent(self):
        ref = self.buf.at[pl.ds(0, 31)]
        remote(ref, ref, self.send_sem, self.recv_sems.at[0, 0], self.torus.twin()).wait_send()

    def arrived(self, k, part):
        ref = self.ref(self.torus.index(*ITEMS[k]), part)
        remote(ref, ref, self.send_sem, self.recv_sems.at[k, part], self.torus.twin()).wait_recv()

    def pass_on(self, k, part):
        self.arrived(k, part)
        self.send(k, part)

    def twin_arrived(self, sem, first, count, part=None):
        ref = self.buf.at[pl.ds(first, count)]
        if part is not None:
            ref = self.buf.at[pl.ds(first, count), pl.ds(*self.parts[part])]
        remote(ref, ref, self.send_sem, self.twin_sems.at[sem], self.torus.twin()).wait_recv()


def whole_kernel(
    rows,
    const,
    latent_hbm,
    rope_key_hbm,
    key_up_hbm,
    value_up_hbm,
    inner_hbm,
    qn_hbm,
    qr_hbm,
    proj_hbm,
    gate_hbm,
    up_hbm,
    down_hbm,
    stream_hbm,
    outer_hbm,
    latent_gain_ref,
    mix_gain_ref,
    mlp_gain_ref,
    out_ref,
    latent_v,
    rope_key_v,
    key_up_v,
    value_up_v,
    inner_v,
    outer_v,
    qn_v,
    qr_v,
    q_ref,
    kv,
    weights,
    proj,
    m_ref,
    l_ref,
    acc_ref,
    heads_all,
    stream_all,
    sums,
    mixed,
    hidden,
    gate_sum,
    up_sum,
    far_out,
    plus_out,
    minus_out,
    far_plus,
    far_minus,
    from_plus,
    from_minus,
    load_sems,
    kv_send,
    kv_recv,
    kv_twin,
    w_send,
    w_recv,
    w_twin,
    proj_send,
    proj_recv,
    ring_send,
    ring_recv,
    x_send,
    x_recv,
):
    t = Torus()
    me, x = t.me, t.x
    depth = weights.shape[1] // 3
    loads = [
        pltpu.make_async_copy(src, dst, load_sems.at[n])
        for n, (src, dst) in enumerate(
            (
                (latent_hbm, latent_v),
                (key_up_hbm, key_up_v),
                (value_up_hbm, value_up_v),
                (rope_key_hbm, rope_key_v),
                (inner_hbm, inner_v),
                (outer_hbm.at[me], outer_v),
                (proj_hbm, proj.at[x]),
                (qn_hbm, qn_v),
                (qr_hbm, qr_v),
                (down_hbm, weights.at[me, pl.ds(2 * depth, depth)]),
                (gate_hbm, weights.at[me, pl.ds(0, depth)]),
                (up_hbm, weights.at[me, pl.ds(depth, depth)]),
                (stream_hbm, stream_all.at[x]),
            )
        )
    ]
    for load in loads:
        load.start()

    plus, minus, across = t.along_x(1), t.along_x(-1), t.along_x(2)
    peers = (t.at(1, 0), t.at(-1, 0), t.at(0, 1), t.at(0, -1), t.twin(), plus, minus, across)
    barrier = pltpu.get_barrier_semaphore()
    for peer in peers:
        pl.semaphore_signal(barrier, inc=1, device_id=peer, device_id_type=MESH)

    slab_rows = kv.shape[1]
    pieces = Gather(t, kv, [(0, slab_rows // 2), (slab_rows // 2, slab_rows // 2)], kv_send.at[0], kv_recv, kv_twin, lambda k, part: k)
    halves = Gather(t, weights, [(0, 2 * depth), (2 * depth, depth)], w_send.at[0], w_recv, w_twin, lambda k, part: 2 * part + k // EARLY)

    class Ring:
        def __init__(self, buf, send_sem, first_sem):
            self.buf, self.send_sem, self.first_sem, self.half = buf, send_sem, first_sem, buf.shape[1] // 2

        def copy(self, d, which, sem, to):
            ref = self.buf.at[lax.rem(x + d + 4, 4), pl.ds(which * self.half, self.half)]
            n = self.first_sem + sem
            return remote(ref, ref, self.send_sem, ring_recv.at[n], to)

        def first(self):
            return [
                self.copy(0, 0, 0, plus),
                self.copy(0, 1, 1, minus),
                self.copy(0, 1, 2, plus),
                self.copy(0, 0, 3, minus),
            ]

        def second(self, which):
            return self.copy(1, 1, 5, minus) if which else self.copy(-1, 0, 4, plus)

        def forward(self):
            for d, which in ((-1, 0), (1, 1)):
                self.copy(d, which, which, plus).wait_recv()
                self.second(which).start()

        def near_arrived(self):
            self.copy(-1, 1, 2, plus).wait_recv()
            self.copy(1, 0, 3, plus).wait_recv()

        def far_arrived(self):
            self.copy(2, 0, 4, plus).wait_recv()
            self.copy(2, 1, 5, plus).wait_recv()

    stream_ring = Ring(stream_all, ring_send.at[0], 0)
    heads_ring = Ring(heads_all, ring_send.at[1], 6)

    share = proj.shape[1] // 2

    def proj_part(d, which):
        slot = lax.rem(x + d + 4, 4)
        size = share if which is None else share // 2
        first = t.c * share + (0 if which is None else which * size)
        return proj.at[slot, pl.ds(pl.multiple_of(first, size), size)]

    def proj_copy(d, which, sem, recv, to):
        ref = proj_part(d, which)
        return remote(ref, ref, proj_send.at[0], proj_recv.at[recv], to)

    proj_first = [proj_copy(0, None, 0, 0, plus), proj_copy(0, None, 1, 1, minus)]
    proj_second = [
        proj_copy(-1, 0, 2, 2, plus),
        proj_copy(1, 1, 3, 3, minus),
        proj_copy(-1, None, 4, 4, t.twin()),
        proj_copy(1, None, 5, 5, t.twin()),
    ]
    proj_third = [proj_copy(2, None, 6, 6, t.twin())]

    def twin_proj(d, recv):
        slot = lax.rem(x + d + 4, 4)
        first = (1 - t.c) * share
        ref = proj.at[slot, pl.ds(pl.multiple_of(first, share), share)]
        return remote(ref, ref, proj_send.at[0], proj_recv.at[recv], t.twin())

    for load in loads[:6]:
        load.wait()
    wide = latent_v[...].astype(F32)
    factor = lax.rsqrt(jnp.mean(wide * wide, axis=-1, keepdims=True) + norm_floor)
    normed = (wide * factor * latent_gain_ref[...]).astype(BF16)
    slab = kv.at[me]
    keys = jnp.dot(normed, key_up_v[...], preferred_element_type=F32).astype(BF16)
    values = jnp.dot(normed, value_up_v[...], preferred_element_type=F32)
    for h in range(2):
        slab[h * rows : (h + 1) * rows, :] = keys[:, 128 * h : 128 * (h + 1)]
        turned = values[:, 128 * h : 128 * (h + 1)].T.astype(BF16)
        for i in range(rows // 128):
            at = 2 * rows + h * rows + 128 * i
            slab[at : at + 128, :] = turned[:, 128 * i : 128 * (i + 1)]
    outer_cos, outer_sin = outer_v[0, :, 0:1], outer_v[1, :, 0:1]
    inner_cos, inner_sin = inner_v[0], inner_v[1]
    cosine = outer_cos * inner_cos - outer_sin * inner_sin
    sine = outer_sin * inner_cos + outer_cos * inner_sin
    mid = rows // 2
    key_turned = turn(rope_key_v[...].astype(F32), cosine, sine).T
    slab[4 * rows : 4 * rows + mid, :] = jnp.concatenate([key_turned[:mid], key_turned[mid:]], axis=1).astype(BF16)

    pl.semaphore_wait(barrier, len(peers))
    for part in range(2):
        pieces.send(0, part)
    loads[6].wait()
    for copy in proj_first:
        copy.start()

    for load in loads[7:]:
        load.wait()
    for copy in stream_ring.first():
        copy.start()
    zeros = jnp.zeros((64, rows), BF16)
    for h in range(2):
        nope = qn_v[:, h, :].astype(F32).T.astype(BF16)
        rotary = turn(qr_v[64 * h : 64 * (h + 1), :].astype(F32), cosine, sine).astype(BF16)
        for odd in range(2):
            q_ref[2 * h + odd, 0:128, :] = nope
            q_ref[2 * h + odd, 128:192, :] = zeros if odd else rotary
            q_ref[2 * h + odd, 192:256, :] = rotary if odd else zeros

    m_ref[...] = jnp.full_like(m_ref, big_negative)
    l_ref[...] = jnp.zeros_like(l_ref)
    acc_ref[...] = jnp.zeros_like(acc_ref)
    attend([kv.at[me]], q_ref, m_ref, l_ref, acc_ref, rows, const, diag=True)

    last = len(ITEMS)

    def step(i, carry):
        for group in range(0, last, 4):

            @pl.when(i // 4 == group // 4)
            def _():
                for k in range(max(group, 1), group + 4):

                    @pl.when(i == k)
                    def _():
                        for begin, end in GROUPS:
                            if k == begin:
                                for other in range(begin, end):
                                    pieces.pass_on(other, 0)
                        pieces.pass_on(k, 1)
                        if k == PROJ_SECOND:
                            proj_copy(-1, None, 0, 0, minus).wait_recv()
                            proj_copy(1, None, 0, 1, minus).wait_recv()
                            for copy in proj_second:
                                copy.start()
                        if k == PROJ_THIRD:
                            proj_copy(2, 0, 0, 2, minus).wait_recv()
                            proj_copy(2, 1, 0, 3, minus).wait_recv()
                            for copy in proj_third:
                                copy.start()
                            stream_ring.forward()
                        if k == WEIGHTS_FIRST:
                            for part in range(2):
                                halves.send(0, part)

        da, db, ea, eb = (jnp.int32(0) for _ in range(4))
        for k, (ka, kb) in enumerate(ITEMS):
            da = jnp.where(i == k, ka, da)
            db = jnp.where(i == k, kb, db)
            ea = jnp.where(i == k + 1, ka, ea)
            eb = jnp.where(i == k + 1, kb, eb)
        own_slot = t.index(da, db)
        twin_slot = t.twin_index(ea, eb)
        pieces.twin_arrived(i - 1, twin_slot, 1)
        own_here = jnp.logical_and(own_slot < me, i < last)
        twin_here = twin_slot < me

        @pl.when(jnp.logical_and(own_here, twin_here))
        def _():
            attend([kv.at[own_slot], kv.at[twin_slot]], q_ref, m_ref, l_ref, acc_ref, rows, const)

        @pl.when(own_here != twin_here)
        def _():
            slot = jnp.where(own_here, own_slot, twin_slot)
            attend([kv.at[slot]], q_ref, m_ref, l_ref, acc_ref, rows, const)

        return carry

    lax.fori_loop(1, last + 1, step, 0)

    own = rows // 4
    for h in range(2):
        heads_all[x, :, 128 * h : 128 * (h + 1)] = (acc_ref[h] / l_ref[h]).T.astype(BF16)
    for copy in heads_ring.first():
        copy.start()

    def pass_weights(first, last, part):
        for k in range(first, last):
            halves.pass_on(k, part)

    pass_weights(1, 5, 0)
    stream_ring.near_arrived()
    stream_ring.far_arrived()
    for d, sem in ((1, 4), (-1, 5), (2, 6)):
        twin_proj(d, sem).wait_recv()
    heads_ring.forward()
    pass_weights(5, 8, 0)
    heads_ring.near_arrived()

    def slots(ref, offsets, axis):
        return jnp.concatenate([ref[lax.rem(x + d + 4, 4)] for d in offsets], axis=axis)

    near = (0, 1, -1)
    sums[...] = jnp.dot(slots(heads_all, near, 1), slots(proj, near, 0), preferred_element_type=F32)
    pass_weights(8, 10, 0)
    heads_ring.far_arrived()
    sums[...] += jnp.dot(slots(heads_all, (2,), 1), slots(proj, (2,), 0), preferred_element_type=F32)

    def norm_rows(n, carry):
        total = sums[pl.ds(pl.multiple_of(n * own, own), own), :]
        mixed[n] = layer_norm(residual_weight * stream_all[n].astype(F32) + total, mix_gain_ref[...]).astype(BF16)
        return carry

    lax.fori_loop(0, 4, norm_rows, 0)
    count, units = weights.shape[0], weights.shape[2]
    pass_weights(10, 11, 0)
    pass_weights(1, 5, 1)
    pass_weights(11, 13, 0)
    halves.twin_arrived(0, 0, EARLY, 0)

    def weight_rows(chips, begin):
        blocks = [weights[pl.ds(chip * 2, 2), begin : begin + depth, :].reshape(2 * depth, units) for chip in chips]
        return jnp.concatenate(blocks, axis=0)

    def expand(chips, into):
        return [jnp.dot(into, weight_rows(chips, begin), preferred_element_type=F32) for begin in (0, depth)]

    def columns(ref, chips):
        n = ref.shape[0] if len(ref.shape) == 2 else ref.shape[0] * ref.shape[1]
        cols = [ref.at[..., pl.ds(pl.multiple_of(chip * 2 * depth, 2 * depth), 2 * depth)] for chip in chips]
        return jnp.concatenate([c[...].reshape(n, 2 * depth) for c in cols], axis=1)

    chips = [t.index(*item) // 2 for item in ITEMS]
    gate_sum[...], up_sum[...] = expand(chips[:EARLY], columns(mixed, chips[:EARLY]))
    pass_weights(13, 15, 0)
    pass_weights(5, 10, 1)
    pass_weights(15, 16, 0)
    halves.twin_arrived(1, 0, 16 - EARLY, 0)

    def rows_at(d):
        return pl.ds(pl.multiple_of(lax.rem(x + d + 4, 4) * own, own), own)

    def activate(first, second):
        into = [columns(mixed.at[lax.rem(x + d + 4, 4)], chips[EARLY:]) for d in (first, second)]
        gate, up = expand(chips[EARLY:], jnp.concatenate(into, axis=0))
        for n, d in enumerate((first, second)):
            g = gate_sum[rows_at(d), :] + gate[n * own : (n + 1) * own]
            u = up_sum[rows_at(d), :] + up[n * own : (n + 1) * own]
            hidden[rows_at(d), :] = (g / (1.0 + jnp.exp(-g)) * u).astype(BF16)

    activate(2, 1)
    activate(-1, 0)
    pass_weights(10, 13, 1)
    halves.twin_arrived(2, 0, EARLY, 1)

    half = own // 2
    top, low = pl.ds(0, half), pl.ds(half, half)
    split = EARLY * 2 * depth
    column_sets = [(chips[:EARLY], pl.ds(0, split)), (chips[EARLY:], pl.ds(split, sums.shape[1] - split))]

    def lower(first, second, late):
        lhs = jnp.concatenate([hidden[rows_at(first), :], hidden[rows_at(second), :]], axis=0)
        rhs = weight_rows(column_sets[late][0], 2 * depth)
        out = lax.dot_general(lhs, rhs, (((1,), (1,)), ((), ())), preferred_element_type=F32)
        return out[:own], out[own:]

    def back(n, late):
        cols = column_sets[late][1]
        src, src_rows, dst, dst_rows, recv, to = (
            (far_out, top, far_minus, pl.ds(0, half), 2 * late, plus),
            (far_out, low, far_plus, pl.ds(0, half), 2 * late + 1, minus),
            (plus_out, low, from_minus, low, 4, plus),
            (minus_out, top, from_plus, top, 5, minus),
            (plus_out, top, from_minus, top, 4, plus),
            (minus_out, low, from_plus, low, 5, minus),
        )[n]
        return remote(src.at[src_rows, cols], dst.at[dst_rows, cols], x_send.at[0], x_recv.at[recv], to)

    def lower_far(late):
        cols = column_sets[late][1]
        far, near = lower(2, 1, late)
        far_out[:, cols] = far.astype(BF16)
        plus_out[:, cols] = near.astype(BF16)
        back(0, late).start()
        back(1, late).start()

    def lower_near(late):
        cols = column_sets[late][1]
        near, here = lower(-1, 0, late)
        minus_out[:, cols] = near.astype(BF16)
        sums[0:own, cols] = here
        back(2, late).start()
        back(3, late).start()

    def add_far(late):
        cols = column_sets[late][1]
        back(0, late).wait_recv()
        plus_out[top, cols] = (plus_out[top, cols].astype(F32) + far_minus[:, cols].astype(F32)).astype(BF16)
        back(4, late).start()
        back(1, late).wait_recv()
        minus_out[low, cols] = (minus_out[low, cols].astype(F32) + far_plus[:, cols].astype(F32)).astype(BF16)
        back(5, late).start()

    lower_far(0)
    lower_near(0)
    for k in range(13, 16):
        halves.pass_on(k, 1)
    halves.twin_arrived(3, 0, 16 - EARLY, 1)
    lower_far(1)
    add_far(0)
    lower_near(1)
    add_far(1)
    for n, ref in ((4, from_minus), (5, from_plus)):
        remote(ref, ref, x_send.at[0], x_recv.at[n], plus).wait_recv()
    lowered = sums[0:own, :] + from_plus[...].astype(F32) + from_minus[...].astype(F32)
    result = layer_norm(
        residual_weight * columns(mixed.at[x], chips).astype(F32) + 0.5 * lowered, columns(mlp_gain_ref, chips)
    ).astype(BF16)
    for n, chip in enumerate(chips):
        out_ref[:, pl.ds(pl.multiple_of(chip * 2 * depth, 2 * depth), 2 * depth)] = result[:, n * 2 * depth : (n + 1) * 2 * depth]

    pieces.sent()
    halves.sent()
    for ref, sem in (
        (proj.at[pl.ds(0, 3)], proj_send.at[0]),
        (stream_all.at[pl.ds(0, 3)], ring_send.at[0]),
        (heads_all.at[pl.ds(0, 3)], ring_send.at[1]),
        (mixed.at[pl.ds(0, 3)], x_send.at[0]),
    ):
        remote(ref, ref, sem, x_recv.at[0], t.twin()).wait_send()


GROUPS = ((1, 5), (5, 11), (11, 15), (15, 16))
EARLY = 11
PROJ_SECOND = 5
PROJ_THIRD = 9
WEIGHTS_FIRST = 12


def per_device(
    queries_nope,
    queries_rope,
    latent,
    rope_key,
    latent_gain,
    key_up,
    value_up,
    out_proj,
    stream,
    mix_gain,
    w_gate,
    w_up,
    w_down,
    mlp_gain,
):
    rows, heads, head_dim = queries_nope.shape
    rope_dim = queries_rope.shape[2]
    count = lax.axis_size("sp")
    tp = lax.axis_size("tp")
    own, width = stream.shape
    units = w_gate.shape[1]
    const = (head_dim + rope_dim) ** (-0.5) * math.log2(math.e)
    lanes = heads * rope_dim
    inner, outer = turn_tables(rows, count, rope_dim)
    slab = 4 * rows + rows // 2
    vmem = pl.BlockSpec(memory_space=pltpu.VMEM)
    hbm = pl.BlockSpec(memory_space=pl.ANY)
    dma = pltpu.SemaphoreType.DMA
    return pl.pallas_call(
        functools.partial(whole_kernel, rows, const),
        out_shape=jax.ShapeDtypeStruct((own, width), BF16),
        in_specs=[hbm] * 13 + [vmem] * 3,
        out_specs=vmem,
        scratch_shapes=[
            pltpu.VMEM(latent.shape, BF16),
            pltpu.VMEM((rope_dim, rows), BF16),
            pltpu.VMEM(key_up.shape, BF16),
            pltpu.VMEM(value_up.shape, BF16),
            pltpu.VMEM(inner.shape, F32),
            pltpu.VMEM(outer.shape[1:], F32),
            pltpu.VMEM(queries_nope.shape, BF16),
            pltpu.VMEM((lanes, rows), BF16),
            pltpu.VMEM((2 * heads, 2 * head_dim, rows), BF16),
            pltpu.VMEM((count, slab, 128), BF16),
            pltpu.VMEM((count, 3 * w_gate.shape[0], units), BF16),
            pltpu.VMEM((tp, *out_proj.shape), BF16),
            pltpu.VMEM((2, 1, rows), F32),
            pltpu.VMEM((2, 1, rows), F32),
            pltpu.VMEM((2, 128, rows), F32),
            pltpu.VMEM((tp, rows, heads * head_dim), BF16),
            pltpu.VMEM((tp, own, width), BF16),
            pltpu.VMEM((rows, width), F32),
            pltpu.VMEM((tp, own, width), BF16),
            pltpu.VMEM((rows, units), BF16),
            pltpu.VMEM((rows, units), F32),
            pltpu.VMEM((rows, units), F32),
            pltpu.VMEM((own, width), BF16),
            pltpu.VMEM((own, width), BF16),
            pltpu.VMEM((own, width), BF16),
            pltpu.VMEM((own // 2, width), BF16),
            pltpu.VMEM((own // 2, width), BF16),
            pltpu.VMEM((own, width), BF16),
            pltpu.VMEM((own, width), BF16),
            dma((13,)),
            dma((1,)),
            dma((16, 2)),
            dma((16,)),
            dma((1,)),
            dma((16, 2)),
            dma((4,)),
            dma((1,)),
            dma((7,)),
            dma((2,)),
            dma((12,)),
            dma((1,)),
            dma((6,)),
        ],
        compiler_params=pltpu.CompilerParams(
            collective_id=0, has_side_effects=True, vmem_limit_bytes=60 * 1024 * 1024
        ),
        name="layer",
    )(
        latent,
        rope_key.T,
        key_up,
        value_up,
        inner,
        queries_nope,
        jnp.transpose(queries_rope, (1, 2, 0)).reshape(lanes, rows),
        out_proj,
        w_gate,
        w_up,
        w_down.T,
        stream,
        outer,
        latent_gain.reshape(1, -1),
        mix_gain.reshape(1, -1),
        mlp_gain.reshape(1, -1),
    )


def solution(mesh):
    return jax.shard_map(
        per_device,
        mesh=mesh,
        in_specs=(
            P("sp", "tp", None),
            P("sp", "tp", None),
            P("sp", None),
            P("sp", None),
            P(),
            P(None, "tp"),
            P(None, "tp"),
            P("tp", None),
            P(("sp", "tp"), None),
            P(),
            P("sp", "tp"),
            P("sp", "tp"),
            P("tp", "sp"),
            P(),
        ),
        out_specs=P(("sp", "tp"), None),
        check_vma=False,
    )
```

```python
import functools
import math

import jax
import jax.numpy as jnp
import numpy as np
from jax import lax
from jax.experimental import pallas as pl
from jax.experimental.pallas import tpu as pltpu
from jax.sharding import PartitionSpec as P

theta_base = 10000.0
residual_weight = 8.0**0.25
norm_floor = 1.0
big_negative = -1e30
F32 = jnp.float32
BF16 = jnp.bfloat16


def turn_tables(rows, count, rope_dim):
    rates = theta_base ** (-2.0 * np.arange(rope_dim // 2) / rope_dim)[:, None]
    inner = rates * np.arange(rows)
    outer = (rates * (np.arange(count) * rows)).T[:, :, None] + np.zeros((1, 1, 128))
    pair = lambda angle: jnp.asarray(np.stack([np.cos(angle), np.sin(angle)]), F32)
    return pair(inner), jnp.moveaxis(pair(outer), 0, 1)


def turn(v, cosine, sine):
    half = v.shape[0] // 2
    a, b = v[:half], v[half:]
    return jnp.concatenate([a * cosine - b * sine, a * sine + b * cosine], axis=0)


def layer_norm(values, gain):
    centre = jnp.mean(values, axis=-1, keepdims=True)
    centred = values - centre
    spread = jnp.mean(centred * centred, axis=-1, keepdims=True)
    return centred * lax.rsqrt(spread + norm_floor) * gain


def scores(kv, h, q_ref, rows, const):
    half = rows // 2
    r = kv[4 * rows : 4 * rows + half, :]
    top = jnp.concatenate([kv[h * rows : h * rows + half, :], r], axis=1)
    low = jnp.concatenate([kv[h * rows + half : (h + 1) * rows, :], r], axis=1)
    both = [
        jnp.dot(top, q_ref[2 * h], preferred_element_type=F32),
        jnp.dot(low, q_ref[2 * h + 1], preferred_element_type=F32),
    ]
    return jnp.concatenate(both, axis=0) * const


def values_of(kv, h, rows):
    at = 2 * rows + h * rows
    return [kv[at + 128 * i : at + 128 * (i + 1), :] for i in range(rows // 128)]


def attend(pieces, q_ref, m_ref, l_ref, acc_ref, rows, const, diag=False):
    for h in range(2):
        s = jnp.concatenate([scores(kv, h, q_ref, rows, const) for kv in pieces], axis=0)
        if diag:
            key = lax.broadcasted_iota(jnp.int32, s.shape, 0)
            query = lax.broadcasted_iota(jnp.int32, s.shape, 1)
            s = jnp.where(key <= query, s, big_negative)
        m_old = m_ref[h]
        m_new = jnp.maximum(m_old, jnp.max(s, axis=0, keepdims=True))
        p = jnp.exp2(s - m_new)
        alpha = jnp.exp2(m_old - m_new)
        l_ref[h] = l_ref[h] * alpha + jnp.sum(p, axis=0, keepdims=True)
        m_ref[h] = m_new
        vt = jnp.concatenate([block for kv in pieces for block in values_of(kv, h, rows)], axis=1)
        acc_ref[h] = acc_ref[h] * alpha + jnp.dot(vt, p.astype(BF16), preferred_element_type=F32)


MESH = pl.DeviceIdType.MESH
ITEMS = (
    (0, 0), (-1, 0), (1, 0), (0, -1), (0, 1), (2, 0), (-1, -1), (-1, 1),
    (1, -1), (1, 1), (0, 2), (2, -1), (2, 1), (-1, 2), (1, 2), (2, 2),
)
PLACE = {item: k for k, item in enumerate(ITEMS)}


def remote(src, dst, send_sem, recv_sem, device):
    return pltpu.make_async_remote_copy(
        src_ref=src, dst_ref=dst, send_sem=send_sem, recv_sem=recv_sem, device_id=device, device_id_type=MESH
    )


class Torus:
    def __init__(self):
        self.me = lax.axis_index("sp")
        self.x = lax.axis_index("tp")
        self.c = lax.rem(self.me, 2)
        chip = self.me // 2
        z, y = chip // 4, lax.rem(chip, 4)
        self.a = z + self.c * (y - z)
        self.b = y + self.c * (z - y)
        self.step_a = 8 - 6 * self.c
        self.step_b = 2 + 6 * self.c

    def index(self, da, db):
        at_a = lax.rem(self.a + da + 4, 4)
        at_b = lax.rem(self.b + db + 4, 4)
        return at_a * self.step_a + at_b * self.step_b + self.c

    def twin_index(self, da, db):
        at_b = lax.rem(self.b + da + 4, 4)
        at_a = lax.rem(self.a + db + 4, 4)
        return at_a * self.step_a + at_b * self.step_b + 1 - self.c

    def at(self, da, db):
        return (self.index(da, db), self.x)

    def twin(self):
        return (self.me + 1 - 2 * self.c, self.x)

    def along_x(self, d):
        return (self.me, lax.rem(self.x + d + 4, 4))


class Gather:
    def __init__(self, torus, buf, parts, send_sem, recv_sems, twin_sems, twin_of):
        self.torus, self.buf, self.parts = torus, buf, parts
        self.send_sem, self.recv_sems, self.twin_sems, self.twin_of = send_sem, recv_sems, twin_sems, twin_of

    def ref(self, slot, part, which=None):
        begin, size = self.parts[part]
        if which is not None:
            size //= 2
            begin += which * size
        return self.buf.at[slot, pl.ds(begin, size)]

    def copies(self, k, part):
        t = self.torus
        da, db = ITEMS[k]
        slot = t.index(da, db)
        plan = []
        if db == 0:
            if da == 0:
                plan += [((1, 0), (-1, 0), None), ((-1, 0), (1, 0), None)]
            plan += [((0, 1), (da, -1), None), ((0, -1), (da, 1), None)]
            if da == -1:
                plan += [((1, 0), (2, 0), 0)]
            if da == 1:
                plan += [((-1, 0), (2, 0), 1)]
        if db == -1:
            plan += [((0, 1), (da, 2), 0)]
        if db == 1:
            plan += [((0, -1), (da, 2), 1)]
        out = []
        for to, name, which in plan:
            ref = self.ref(slot, part, which)
            out.append(remote(ref, ref, self.send_sem, self.recv_sems.at[PLACE[name], part], t.at(*to)))
        ref = self.ref(slot, part)
        out.append(remote(ref, ref, self.send_sem, self.twin_sems.at[self.twin_of(k, part)], t.twin()))
        return out

    def send(self, k, part):
        for copy in self.copies(k, part):
            copy.start()

    def sent(self):
        ref = self.buf.at[pl.ds(0, 31)]
        remote(ref, ref, self.send_sem, self.recv_sems.at[0, 0], self.torus.twin()).wait_send()

    def arrived(self, k, part):
        ref = self.ref(self.torus.index(*ITEMS[k]), part)
        remote(ref, ref, self.send_sem, self.recv_sems.at[k, part], self.torus.twin()).wait_recv()

    def pass_on(self, k, part):
        self.arrived(k, part)
        self.send(k, part)

    def twin_arrived(self, sem, first, count, part=None):
        ref = self.buf.at[pl.ds(first, count)]
        if part is not None:
            ref = self.buf.at[pl.ds(first, count), pl.ds(*self.parts[part])]
        remote(ref, ref, self.send_sem, self.twin_sems.at[sem], self.torus.twin()).wait_recv()


def whole_kernel(
    rows,
    const,
    latent_hbm,
    rope_key_hbm,
    key_up_hbm,
    value_up_hbm,
    inner_hbm,
    qn_hbm,
    qr_hbm,
    proj_hbm,
    gate_hbm,
    up_hbm,
    down_hbm,
    stream_hbm,
    outer_hbm,
    latent_gain_ref,
    mix_gain_ref,
    mlp_gain_ref,
    out_ref,
    latent_v,
    rope_key_v,
    key_up_v,
    value_up_v,
    inner_v,
    outer_v,
    qn_v,
    qr_v,
    q_ref,
    kv,
    weights,
    proj,
    m_ref,
    l_ref,
    acc_ref,
    heads_all,
    stream_all,
    sums,
    mixed,
    hidden,
    gate_sum,
    up_sum,
    far_out,
    plus_out,
    minus_out,
    far_plus,
    far_minus,
    from_plus,
    from_minus,
    load_sems,
    kv_send,
    kv_recv,
    kv_twin,
    w_send,
    w_recv,
    w_twin,
    proj_send,
    proj_recv,
    ring_send,
    ring_recv,
    x_send,
    x_recv,
):
    t = Torus()
    me, x = t.me, t.x
    depth = weights.shape[1] // 3
    loads = [
        pltpu.make_async_copy(src, dst, load_sems.at[n])
        for n, (src, dst) in enumerate(
            (
                (latent_hbm, latent_v),
                (key_up_hbm, key_up_v),
                (value_up_hbm, value_up_v),
                (rope_key_hbm, rope_key_v),
                (inner_hbm, inner_v),
                (outer_hbm.at[me], outer_v),
                (proj_hbm, proj.at[x]),
                (qn_hbm, qn_v),
                (qr_hbm, qr_v),
                (down_hbm, weights.at[me, pl.ds(2 * depth, depth)]),
                (gate_hbm, weights.at[me, pl.ds(0, depth)]),
                (up_hbm, weights.at[me, pl.ds(depth, depth)]),
                (stream_hbm, stream_all.at[x]),
            )
        )
    ]
    for load in loads[:2]:
        load.start()

    plus, minus, across = t.along_x(1), t.along_x(-1), t.along_x(2)
    peers = (t.at(1, 0), t.at(-1, 0), t.at(0, 1), t.at(0, -1), t.twin(), plus, minus, across)
    barrier = pltpu.get_barrier_semaphore()
    for peer in peers:
        pl.semaphore_signal(barrier, inc=1, device_id=peer, device_id_type=MESH)
    for load in loads[2:]:
        load.start()

    slab_rows = kv.shape[1]
    pieces = Gather(t, kv, [(0, 2 * rows), (2 * rows, slab_rows - 2 * rows)], kv_send.at[0], kv_recv, kv_twin, lambda k, part: k)
    halves = Gather(t, weights, [(0, 2 * depth), (2 * depth, depth)], w_send.at[0], w_recv, w_twin, lambda k, part: k // EARLY if part == 0 else 2 + [first <= k < last for first, last in COLUMN_SETS].index(True))

    class Ring:
        def __init__(self, buf, send_sem, first_sem):
            self.buf, self.send_sem, self.first_sem, self.half = buf, send_sem, first_sem, buf.shape[1] // 2

        def copy(self, d, which, sem, to):
            ref = self.buf.at[lax.rem(x + d + 4, 4), pl.ds(which * self.half, self.half)]
            n = self.first_sem + sem
            return remote(ref, ref, self.send_sem, ring_recv.at[n], to)

        def first(self):
            return [
                self.copy(0, 0, 0, plus),
                self.copy(0, 1, 1, minus),
                self.copy(0, 1, 2, plus),
                self.copy(0, 0, 3, minus),
            ]

        def second(self, which):
            return self.copy(1, 1, 5, minus) if which else self.copy(-1, 0, 4, plus)

        def forward(self):
            for d, which in ((-1, 0), (1, 1)):
                self.copy(d, which, which, plus).wait_recv()
                self.second(which).start()

        def near_arrived(self):
            self.copy(-1, 1, 2, plus).wait_recv()
            self.copy(1, 0, 3, plus).wait_recv()

        def far_arrived(self):
            self.copy(2, 0, 4, plus).wait_recv()
            self.copy(2, 1, 5, plus).wait_recv()

    stream_ring = Ring(stream_all, ring_send.at[0], 0)
    heads_ring = Ring(heads_all, ring_send.at[1], 6)

    share = proj.shape[1] // 2

    def proj_part(d, which):
        slot = lax.rem(x + d + 4, 4)
        size = share if which is None else share // 2
        first = t.c * share + (0 if which is None else which * size)
        return proj.at[slot, pl.ds(pl.multiple_of(first, size), size)]

    def proj_copy(d, which, sem, recv, to):
        ref = proj_part(d, which)
        return remote(ref, ref, proj_send.at[0], proj_recv.at[recv], to)

    proj_first = [proj_copy(0, None, 0, 0, plus), proj_copy(0, None, 1, 1, minus)]
    proj_second = [
        proj_copy(-1, 0, 2, 2, plus),
        proj_copy(1, 1, 3, 3, minus),
        proj_copy(-1, None, 4, 4, t.twin()),
        proj_copy(1, None, 5, 5, t.twin()),
    ]
    proj_third = [proj_copy(2, None, 6, 6, t.twin())]

    def twin_proj(d, recv):
        slot = lax.rem(x + d + 4, 4)
        first = (1 - t.c) * share
        ref = proj.at[slot, pl.ds(pl.multiple_of(first, share), share)]
        return remote(ref, ref, proj_send.at[0], proj_recv.at[recv], t.twin())

    loads[0].wait()
    loads[1].wait()
    wide = latent_v[...].astype(F32)
    factor = lax.rsqrt(jnp.mean(wide * wide, axis=-1, keepdims=True) + norm_floor)
    normed = (wide * factor * latent_gain_ref[...]).astype(BF16)
    slab = kv.at[me]
    keys = jnp.dot(normed, key_up_v[...], preferred_element_type=F32).astype(BF16)
    for h in range(2):
        slab[h * rows : (h + 1) * rows, :] = keys[:, 128 * h : 128 * (h + 1)]
    pl.semaphore_wait(barrier, len(peers))
    pieces.send(0, 0)
    for load in loads[2:6]:
        load.wait()
    values = jnp.dot(normed, value_up_v[...], preferred_element_type=F32)
    for h in range(2):
        turned = values[:, 128 * h : 128 * (h + 1)].T.astype(BF16)
        for i in range(rows // 128):
            at = 2 * rows + h * rows + 128 * i
            slab[at : at + 128, :] = turned[:, 128 * i : 128 * (i + 1)]
    outer_cos, outer_sin = outer_v[0, :, 0:1], outer_v[1, :, 0:1]
    inner_cos, inner_sin = inner_v[0], inner_v[1]
    cosine = outer_cos * inner_cos - outer_sin * inner_sin
    sine = outer_sin * inner_cos + outer_cos * inner_sin
    mid = rows // 2
    key_turned = turn(rope_key_v[...].astype(F32), cosine, sine).T
    slab[4 * rows : 4 * rows + mid, :] = jnp.concatenate([key_turned[:mid], key_turned[mid:]], axis=1).astype(BF16)

    pieces.send(0, 1)
    loads[6].wait()
    for copy in proj_first:
        copy.start()

    for load in loads[7:]:
        load.wait()
    for copy in stream_ring.first():
        copy.start()
    zeros = jnp.zeros((64, rows), BF16)
    for h in range(2):
        nope = qn_v[:, h, :].astype(F32).T.astype(BF16)
        rotary = turn(qr_v[64 * h : 64 * (h + 1), :].astype(F32), cosine, sine).astype(BF16)
        for odd in range(2):
            q_ref[2 * h + odd, 0:128, :] = nope
            q_ref[2 * h + odd, 128:192, :] = zeros if odd else rotary
            q_ref[2 * h + odd, 192:256, :] = rotary if odd else zeros

    m_ref[...] = jnp.full_like(m_ref, big_negative)
    l_ref[...] = jnp.zeros_like(l_ref)
    acc_ref[...] = jnp.zeros_like(acc_ref)
    attend([kv.at[me]], q_ref, m_ref, l_ref, acc_ref, rows, const, diag=True)

    last = len(ITEMS)

    def step(i, carry):
        for group in range(0, last, 4):

            @pl.when(i // 4 == group // 4)
            def _():
                for k in range(max(group, 1), group + 4):

                    @pl.when(i == k)
                    def _():
                        for begin, end in GROUPS:
                            if k == begin:
                                for other in range(begin, end):
                                    pieces.pass_on(other, 0)
                        pieces.pass_on(k, 1)
                        if k == PROJ_SECOND:
                            proj_copy(-1, None, 0, 0, minus).wait_recv()
                            proj_copy(1, None, 0, 1, minus).wait_recv()
                            for copy in proj_second:
                                copy.start()
                        if k == PROJ_THIRD:
                            proj_copy(2, 0, 0, 2, minus).wait_recv()
                            proj_copy(2, 1, 0, 3, minus).wait_recv()
                            for copy in proj_third:
                                copy.start()
                            stream_ring.forward()
                        if k == WEIGHTS_FIRST:
                            for part in range(2):
                                halves.send(0, part)

        da, db, ea, eb = (jnp.int32(0) for _ in range(4))
        for k, (ka, kb) in enumerate(ITEMS):
            da = jnp.where(i == k, ka, da)
            db = jnp.where(i == k, kb, db)
            ea = jnp.where(i == k + 1, ka, ea)
            eb = jnp.where(i == k + 1, kb, eb)
        own_slot = t.index(da, db)
        twin_slot = t.twin_index(ea, eb)
        pieces.twin_arrived(i - 1, twin_slot, 1)
        own_here = jnp.logical_and(own_slot < me, i < last)
        twin_here = twin_slot < me

        @pl.when(jnp.logical_and(own_here, twin_here))
        def _():
            attend([kv.at[own_slot], kv.at[twin_slot]], q_ref, m_ref, l_ref, acc_ref, rows, const)

        @pl.when(own_here != twin_here)
        def _():
            slot = jnp.where(own_here, own_slot, twin_slot)
            attend([kv.at[slot]], q_ref, m_ref, l_ref, acc_ref, rows, const)

        return carry

    lax.fori_loop(1, last + 1, step, 0)

    own = rows // 4
    for h in range(2):
        heads_all[x, :, 128 * h : 128 * (h + 1)] = (acc_ref[h] / l_ref[h]).T.astype(BF16)
    for copy in heads_ring.first():
        copy.start()

    def pass_weights(first, last, part):
        for k in range(first, last):
            halves.pass_on(k, part)

    pass_weights(1, 5, 0)
    stream_ring.near_arrived()
    stream_ring.far_arrived()
    for d, sem in ((1, 4), (-1, 5), (2, 6)):
        twin_proj(d, sem).wait_recv()
    heads_ring.forward()
    pass_weights(5, 8, 0)
    heads_ring.near_arrived()

    def slots(ref, offsets, axis):
        return jnp.concatenate([ref[lax.rem(x + d + 4, 4)] for d in offsets], axis=axis)

    near = (0, 1, -1)
    sums[...] = jnp.dot(slots(heads_all, near, 1), slots(proj, near, 0), preferred_element_type=F32)
    pass_weights(8, 10, 0)
    heads_ring.far_arrived()
    sums[...] += jnp.dot(slots(heads_all, (2,), 1), slots(proj, (2,), 0), preferred_element_type=F32)

    def norm_rows(n, carry):
        total = sums[pl.ds(pl.multiple_of(n * own, own), own), :]
        mixed[n] = layer_norm(residual_weight * stream_all[n].astype(F32) + total, mix_gain_ref[...]).astype(BF16)
        return carry

    lax.fori_loop(0, 4, norm_rows, 0)
    count, units = weights.shape[0], weights.shape[2]
    pass_weights(10, 11, 0)
    pass_weights(1, 5, 1)
    pass_weights(11, 13, 0)
    halves.twin_arrived(0, 0, EARLY, 0)

    def weight_rows(chips, begin):
        blocks = [weights[pl.ds(chip * 2, 2), begin : begin + depth, :].reshape(2 * depth, units) for chip in chips]
        return jnp.concatenate(blocks, axis=0)

    def expand(chips, into):
        return [jnp.dot(into, weight_rows(chips, begin), preferred_element_type=F32) for begin in (0, depth)]

    def columns(ref, chips):
        n = ref.shape[0] if len(ref.shape) == 2 else ref.shape[0] * ref.shape[1]
        cols = [ref.at[..., pl.ds(pl.multiple_of(chip * 2 * depth, 2 * depth), 2 * depth)] for chip in chips]
        return jnp.concatenate([c[...].reshape(n, 2 * depth) for c in cols], axis=1)

    chips = [t.index(*item) // 2 for item in ITEMS]
    gate_sum[...], up_sum[...] = expand(chips[:EARLY], columns(mixed, chips[:EARLY]))
    pass_weights(13, 15, 0)
    pass_weights(5, 10, 1)
    pass_weights(15, 16, 0)
    halves.twin_arrived(1, 0, 16 - EARLY, 0)

    def rows_at(d):
        return pl.ds(pl.multiple_of(lax.rem(x + d + 4, 4) * own, own), own)

    def activate(first, second):
        into = [columns(mixed.at[lax.rem(x + d + 4, 4)], chips[EARLY:]) for d in (first, second)]
        gate, up = expand(chips[EARLY:], jnp.concatenate(into, axis=0))
        for n, d in enumerate((first, second)):
            g = gate_sum[rows_at(d), :] + gate[n * own : (n + 1) * own]
            u = up_sum[rows_at(d), :] + up[n * own : (n + 1) * own]
            hidden[rows_at(d), :] = (g / (1.0 + jnp.exp(-g)) * u).astype(BF16)

    half = own // 2
    top, low = pl.ds(0, half), pl.ds(half, half)
    column_sets = [
        (chips[first:last], pl.ds(first * 2 * depth, (last - first) * 2 * depth)) for first, last in COLUMN_SETS
    ]
    sets = len(column_sets)

    def lower(first, second, late):
        lhs = jnp.concatenate([hidden[rows_at(first), :], hidden[rows_at(second), :]], axis=0)
        rhs = weight_rows(column_sets[late][0], 2 * depth)
        out = lax.dot_general(lhs, rhs, (((1,), (1,)), ((), ())), preferred_element_type=F32)
        return out[:own], out[own:]

    def back(n, late):
        cols = column_sets[late][1]
        src, src_rows, dst, dst_rows, recv, to = (
            (far_out, top, far_minus, pl.ds(0, half), 2 * late, plus),
            (far_out, low, far_plus, pl.ds(0, half), 2 * late + 1, minus),
            (plus_out, low, from_minus, low, 2 * sets, plus),
            (minus_out, top, from_plus, top, 2 * sets + 1, minus),
            (plus_out, top, from_minus, top, 2 * sets, plus),
            (minus_out, low, from_plus, low, 2 * sets + 1, minus),
        )[n]
        return remote(src.at[src_rows, cols], dst.at[dst_rows, cols], x_send.at[0], x_recv.at[recv], to)

    def lower_far(late):
        cols = column_sets[late][1]
        far, near = lower(2, 1, late)
        far_out[:, cols] = far.astype(BF16)
        plus_out[:, cols] = near.astype(BF16)
        back(0, late).start()
        back(1, late).start()

    def lower_near(late):
        cols = column_sets[late][1]
        near, here = lower(-1, 0, late)
        minus_out[:, cols] = near.astype(BF16)
        sums[0:own, cols] = here
        back(2, late).start()
        back(3, late).start()

    def add_far(late):
        cols = column_sets[late][1]
        back(0, late).wait_recv()
        plus_out[top, cols] = (plus_out[top, cols].astype(F32) + far_minus[:, cols].astype(F32)).astype(BF16)
        back(4, late).start()
        back(1, late).wait_recv()
        minus_out[low, cols] = (minus_out[low, cols].astype(F32) + far_plus[:, cols].astype(F32)).astype(BF16)
        back(5, late).start()

    def down_arrived(n):
        first, last = COLUMN_SETS[n]
        halves.twin_arrived(2 + n, 0, last - first, 1)

    activate(2, 1)
    down_arrived(0)
    lower_far(0)
    activate(-1, 0)
    lower_near(0)
    pass_weights(10, 13, 1)
    down_arrived(1)
    lower_far(1)
    lower_near(1)
    add_far(0)
    pass_weights(13, 16, 1)
    down_arrived(2)
    lower_far(2)
    lower_near(2)
    add_far(1)
    add_far(2)
    for n, ref in ((2 * sets, from_minus), (2 * sets + 1, from_plus)):
        remote(ref, ref, x_send.at[0], x_recv.at[n], plus).wait_recv()
    lowered = sums[0:own, :] + from_plus[...].astype(F32) + from_minus[...].astype(F32)
    result = layer_norm(
        residual_weight * columns(mixed.at[x], chips).astype(F32) + 0.5 * lowered, columns(mlp_gain_ref, chips)
    ).astype(BF16)
    for n, chip in enumerate(chips):
        out_ref[:, pl.ds(pl.multiple_of(chip * 2 * depth, 2 * depth), 2 * depth)] = result[:, n * 2 * depth : (n + 1) * 2 * depth]

    pieces.sent()
    halves.sent()
    for ref, sem in (
        (proj.at[pl.ds(0, 3)], proj_send.at[0]),
        (stream_all.at[pl.ds(0, 3)], ring_send.at[0]),
        (heads_all.at[pl.ds(0, 3)], ring_send.at[1]),
        (mixed.at[pl.ds(0, 3)], x_send.at[0]),
    ):
        remote(ref, ref, sem, x_recv.at[0], t.twin()).wait_send()


GROUPS = ((1, 5), (5, 11), (11, 15), (15, 16))
EARLY = 11
COLUMN_SETS = ((0, 5), (5, 11), (11, 16))
PROJ_SECOND = 5
PROJ_THIRD = 9
WEIGHTS_FIRST = 12


def per_device(
    queries_nope,
    queries_rope,
    latent,
    rope_key,
    latent_gain,
    key_up,
    value_up,
    out_proj,
    stream,
    mix_gain,
    w_gate,
    w_up,
    w_down,
    mlp_gain,
):
    rows, heads, head_dim = queries_nope.shape
    rope_dim = queries_rope.shape[2]
    count = lax.axis_size("sp")
    tp = lax.axis_size("tp")
    own, width = stream.shape
    units = w_gate.shape[1]
    const = (head_dim + rope_dim) ** (-0.5) * math.log2(math.e)
    lanes = heads * rope_dim
    inner, outer = turn_tables(rows, count, rope_dim)
    slab = 4 * rows + rows // 2
    vmem = pl.BlockSpec(memory_space=pltpu.VMEM)
    hbm = pl.BlockSpec(memory_space=pl.ANY)
    dma = pltpu.SemaphoreType.DMA
    return pl.pallas_call(
        functools.partial(whole_kernel, rows, const),
        out_shape=jax.ShapeDtypeStruct((own, width), BF16),
        in_specs=[hbm] * 13 + [vmem] * 3,
        out_specs=vmem,
        scratch_shapes=[
            pltpu.VMEM(latent.shape, BF16),
            pltpu.VMEM((rope_dim, rows), BF16),
            pltpu.VMEM(key_up.shape, BF16),
            pltpu.VMEM(value_up.shape, BF16),
            pltpu.VMEM(inner.shape, F32),
            pltpu.VMEM(outer.shape[1:], F32),
            pltpu.VMEM(queries_nope.shape, BF16),
            pltpu.VMEM((lanes, rows), BF16),
            pltpu.VMEM((2 * heads, 2 * head_dim, rows), BF16),
            pltpu.VMEM((count, slab, 128), BF16),
            pltpu.VMEM((count, 3 * w_gate.shape[0], units), BF16),
            pltpu.VMEM((tp, *out_proj.shape), BF16),
            pltpu.VMEM((2, 1, rows), F32),
            pltpu.VMEM((2, 1, rows), F32),
            pltpu.VMEM((2, 128, rows), F32),
            pltpu.VMEM((tp, rows, heads * head_dim), BF16),
            pltpu.VMEM((tp, own, width), BF16),
            pltpu.VMEM((rows, width), F32),
            pltpu.VMEM((tp, own, width), BF16),
            pltpu.VMEM((rows, units), BF16),
            pltpu.VMEM((rows, units), F32),
            pltpu.VMEM((rows, units), F32),
            pltpu.VMEM((own, width), BF16),
            pltpu.VMEM((own, width), BF16),
            pltpu.VMEM((own, width), BF16),
            pltpu.VMEM((own // 2, width), BF16),
            pltpu.VMEM((own // 2, width), BF16),
            pltpu.VMEM((own, width), BF16),
            pltpu.VMEM((own, width), BF16),
            dma((13,)),
            dma((1,)),
            dma((16, 2)),
            dma((16,)),
            dma((1,)),
            dma((16, 2)),
            dma((2 + len(COLUMN_SETS),)),
            dma((1,)),
            dma((7,)),
            dma((2,)),
            dma((12,)),
            dma((1,)),
            dma((2 * len(COLUMN_SETS) + 2,)),
        ],
        compiler_params=pltpu.CompilerParams(
            collective_id=0, has_side_effects=True, vmem_limit_bytes=60 * 1024 * 1024
        ),
        name="layer",
    )(
        latent,
        rope_key.T,
        key_up,
        value_up,
        inner,
        queries_nope,
        jnp.transpose(queries_rope, (1, 2, 0)).reshape(lanes, rows),
        out_proj,
        w_gate,
        w_up,
        w_down.T,
        stream,
        outer,
        latent_gain.reshape(1, -1),
        mix_gain.reshape(1, -1),
        mlp_gain.reshape(1, -1),
    )


def solution(mesh):
    return jax.shard_map(
        per_device,
        mesh=mesh,
        in_specs=(
            P("sp", "tp", None),
            P("sp", "tp", None),
            P("sp", None),
            P("sp", None),
            P(),
            P(None, "tp"),
            P(None, "tp"),
            P("tp", None),
            P(("sp", "tp"), None),
            P(),
            P("sp", "tp"),
            P("sp", "tp"),
            P("tp", "sp"),
            P(),
        ),
        out_specs=P(("sp", "tp"), None),
        check_vma=False,
    )
```

```python
import functools
import math

import jax
import jax.numpy as jnp
import numpy as np
from jax import lax
from jax.experimental import pallas as pl
from jax.experimental.pallas import tpu as pltpu
from jax.sharding import PartitionSpec as P

theta_base = 10000.0
residual_weight = 8.0**0.25
norm_floor = 1.0
big_negative = -1e30
F32 = jnp.float32
BF16 = jnp.bfloat16


def turn_tables(rows, count, rope_dim):
    rates = theta_base ** (-2.0 * np.arange(rope_dim // 2) / rope_dim)[:, None]
    inner = rates * np.arange(rows)
    outer = (rates * (np.arange(count) * rows)).T[:, :, None] + np.zeros((1, 1, 128))
    pair = lambda angle: jnp.asarray(np.stack([np.cos(angle), np.sin(angle)]), F32)
    return pair(inner), jnp.moveaxis(pair(outer), 0, 1)


def turn(v, cosine, sine):
    half = v.shape[0] // 2
    a, b = v[:half], v[half:]
    return jnp.concatenate([a * cosine - b * sine, a * sine + b * cosine], axis=0)


def layer_norm(values, gain):
    centre = jnp.mean(values, axis=-1, keepdims=True)
    centred = values - centre
    spread = jnp.mean(centred * centred, axis=-1, keepdims=True)
    return centred * lax.rsqrt(spread + norm_floor) * gain


def scores(kv, h, q_ref, rows, const):
    half = rows // 2
    r = kv[4 * rows : 4 * rows + half, :]
    top = jnp.concatenate([kv[h * rows : h * rows + half, :], r], axis=1)
    low = jnp.concatenate([kv[h * rows + half : (h + 1) * rows, :], r], axis=1)
    both = [
        jnp.dot(top, q_ref[2 * h], preferred_element_type=F32),
        jnp.dot(low, q_ref[2 * h + 1], preferred_element_type=F32),
    ]
    return jnp.concatenate(both, axis=0) * const


def values_of(kv, h, rows):
    at = 2 * rows + h * rows
    return [kv[at + 128 * i : at + 128 * (i + 1), :] for i in range(rows // 128)]


def attend(pieces, q_ref, m_ref, l_ref, acc_ref, rows, const, diag=False):
    for h in range(2):
        s = jnp.concatenate([scores(kv, h, q_ref, rows, const) for kv in pieces], axis=0)
        if diag:
            key = lax.broadcasted_iota(jnp.int32, s.shape, 0)
            query = lax.broadcasted_iota(jnp.int32, s.shape, 1)
            s = jnp.where(key <= query, s, big_negative)
        m_old = m_ref[h]
        m_new = jnp.maximum(m_old, jnp.max(s, axis=0, keepdims=True))
        p = jnp.exp2(s - m_new)
        alpha = jnp.exp2(m_old - m_new)
        l_ref[h] = l_ref[h] * alpha + jnp.sum(p, axis=0, keepdims=True)
        m_ref[h] = m_new
        vt = jnp.concatenate([block for kv in pieces for block in values_of(kv, h, rows)], axis=1)
        acc_ref[h] = acc_ref[h] * alpha + jnp.dot(vt, p.astype(BF16), preferred_element_type=F32)


MESH = pl.DeviceIdType.MESH
ITEMS = (
    (0, 0), (-1, 0), (1, 0), (0, -1), (0, 1), (2, 0), (-1, -1), (-1, 1),
    (1, -1), (1, 1), (0, 2), (2, -1), (2, 1), (-1, 2), (1, 2), (2, 2),
)
PLACE = {item: k for k, item in enumerate(ITEMS)}


def remote(src, dst, send_sem, recv_sem, device):
    return pltpu.make_async_remote_copy(
        src_ref=src, dst_ref=dst, send_sem=send_sem, recv_sem=recv_sem, device_id=device, device_id_type=MESH
    )


class Torus:
    def __init__(self):
        self.me = lax.axis_index("sp")
        self.x = lax.axis_index("tp")
        self.c = lax.rem(self.me, 2)
        chip = self.me // 2
        z, y = chip // 4, lax.rem(chip, 4)
        self.a = z + self.c * (y - z)
        self.b = y + self.c * (z - y)
        self.step_a = 8 - 6 * self.c
        self.step_b = 2 + 6 * self.c

    def index(self, da, db):
        at_a = lax.rem(self.a + da + 4, 4)
        at_b = lax.rem(self.b + db + 4, 4)
        return at_a * self.step_a + at_b * self.step_b + self.c

    def twin_index(self, da, db):
        at_b = lax.rem(self.b + da + 4, 4)
        at_a = lax.rem(self.a + db + 4, 4)
        return at_a * self.step_a + at_b * self.step_b + 1 - self.c

    def at(self, da, db):
        return (self.index(da, db), self.x)

    def twin(self):
        return (self.me + 1 - 2 * self.c, self.x)

    def along_x(self, d):
        return (self.me, lax.rem(self.x + d + 4, 4))


class Gather:
    def __init__(self, torus, buf, parts, send_sem, recv_sems, twin_sems, twin_of):
        self.torus, self.buf, self.parts = torus, buf, parts
        self.send_sem, self.recv_sems, self.twin_sems, self.twin_of = send_sem, recv_sems, twin_sems, twin_of

    def ref(self, slot, part, which=None):
        begin, size = self.parts[part]
        if which is not None:
            size //= 2
            begin += which * size
        return self.buf.at[slot, pl.ds(begin, size)]

    def copies(self, k, part):
        t = self.torus
        da, db = ITEMS[k]
        slot = t.index(da, db)
        plan = []
        if db == 0:
            if da == 0:
                plan += [((1, 0), (-1, 0), None), ((-1, 0), (1, 0), None)]
            plan += [((0, 1), (da, -1), None), ((0, -1), (da, 1), None)]
            if da == -1:
                plan += [((1, 0), (2, 0), 0)]
            if da == 1:
                plan += [((-1, 0), (2, 0), 1)]
        if db == -1:
            plan += [((0, 1), (da, 2), 0)]
        if db == 1:
            plan += [((0, -1), (da, 2), 1)]
        out = []
        for to, name, which in plan:
            ref = self.ref(slot, part, which)
            out.append(remote(ref, ref, self.send_sem, self.recv_sems.at[PLACE[name] - 1, part], t.at(*to)))
        ref = self.ref(slot, part)
        out.append(remote(ref, ref, self.send_sem, self.twin_sems.at[self.twin_of(k, part)], t.twin()))
        return out

    def send(self, k, part):
        for copy in self.copies(k, part):
            copy.start()

    def sent(self):
        ref = self.buf.at[pl.ds(0, 31)]
        remote(ref, ref, self.send_sem, self.recv_sems.at[0, 0], self.torus.twin()).wait_send()

    def arrived(self, k, part):
        ref = self.ref(self.torus.index(*ITEMS[k]), part)
        remote(ref, ref, self.send_sem, self.recv_sems.at[k - 1, part], self.torus.twin()).wait_recv()

    def pass_on(self, k, part):
        self.arrived(k, part)
        self.send(k, part)

    def twin_arrived(self, sem, first, count, part=None):
        ref = self.buf.at[pl.ds(first, count)]
        if part is not None:
            ref = self.buf.at[pl.ds(first, count), pl.ds(*self.parts[part])]
        remote(ref, ref, self.send_sem, self.twin_sems.at[sem], self.torus.twin()).wait_recv()


def whole_kernel(
    rows,
    const,
    latent_hbm,
    rope_key_hbm,
    key_up_hbm,
    value_up_hbm,
    inner_hbm,
    qn_hbm,
    qr_hbm,
    proj_hbm,
    gate_hbm,
    up_hbm,
    down_hbm,
    stream_hbm,
    outer_hbm,
    latent_gain_ref,
    mix_gain_ref,
    mlp_gain_ref,
    out_ref,
    latent_v,
    rope_key_v,
    key_up_v,
    value_up_v,
    inner_v,
    outer_v,
    qn_v,
    qr_v,
    q_ref,
    kv,
    weights,
    proj,
    m_ref,
    l_ref,
    acc_ref,
    heads_all,
    stream_all,
    sums,
    mixed,
    hidden,
    gate_sum,
    up_sum,
    far_out,
    plus_out,
    minus_out,
    far_plus,
    far_minus,
    from_plus,
    from_minus,
    load_sems,
    kv_send,
    kv_recv,
    kv_twin,
    w_send,
    w_recv,
    w_twin,
    proj_send,
    proj_recv,
    ring_send,
    ring_recv,
    x_send,
    x_recv,
):
    t = Torus()
    me, x = t.me, t.x
    depth = weights.shape[1] // 3
    loads = [
        pltpu.make_async_copy(src, dst, load_sems.at[min(n, LOADS - 1)])
        for n, (src, dst) in enumerate(
            (
                (latent_hbm, latent_v),
                (key_up_hbm, key_up_v),
                (value_up_hbm, value_up_v),
                (rope_key_hbm, rope_key_v),
                (inner_hbm, inner_v),
                (outer_hbm.at[me], outer_v),
                (proj_hbm, proj.at[x]),
                (qn_hbm, qn_v),
                (qr_hbm, qr_v),
                (stream_hbm, stream_all.at[x]),
                (gate_hbm, weights.at[me, pl.ds(0, depth)]),
                (up_hbm, weights.at[me, pl.ds(depth, depth)]),
                (down_hbm, weights.at[me, pl.ds(2 * depth, depth)]),
            )
        )
    ]
    for load in loads[:2]:
        load.start()

    plus, minus, across = t.along_x(1), t.along_x(-1), t.along_x(2)
    peers = (t.at(1, 0), t.at(-1, 0), t.at(0, 1), t.at(0, -1), t.twin(), plus, minus, across)
    barrier = pltpu.get_barrier_semaphore()
    for peer in peers:
        pl.semaphore_signal(barrier, inc=1, device_id=peer, device_id_type=MESH)
    for load in loads[2:]:
        load.start()

    slab_rows = kv.shape[1]
    pieces = Gather(t, kv, [(0, 2 * rows), (2 * rows, slab_rows - 2 * rows)], kv_send.at[0], kv_recv, kv_twin, lambda k, part: k)
    halves = Gather(t, weights, [(0, 2 * depth), (2 * depth, depth)], w_send.at[0], w_recv, w_twin, lambda k, part: k // EARLY if part == 0 else 2 + [first <= k < last for first, last in COLUMN_SETS].index(True))

    class Ring:
        def __init__(self, buf, send_sem, first_sem):
            self.buf, self.send_sem, self.first_sem, self.half = buf, send_sem, first_sem, buf.shape[1] // 2

        def copy(self, d, which, sem, to):
            ref = self.buf.at[lax.rem(x + d + 4, 4), pl.ds(which * self.half, self.half)]
            n = self.first_sem + sem
            return remote(ref, ref, self.send_sem, ring_recv.at[n], to)

        def first(self):
            return [
                self.copy(0, 0, 0, plus),
                self.copy(0, 1, 1, minus),
                self.copy(0, 1, 2, plus),
                self.copy(0, 0, 2, minus),
            ]

        def second(self, which):
            return self.copy(1, 1, 3, minus) if which else self.copy(-1, 0, 3, plus)

        def forward(self):
            for d, which in ((-1, 0), (1, 1)):
                self.copy(d, which, which, plus).wait_recv()
                self.second(which).start()

        def both_halves(self, sem):
            ref = self.buf.at[0]
            remote(ref, ref, self.send_sem, ring_recv.at[self.first_sem + sem], plus).wait_recv()

        def near_arrived(self):
            self.both_halves(2)

        def far_arrived(self):
            self.both_halves(3)

    stream_ring = Ring(stream_all, ring_send.at[0], 0)
    heads_ring = Ring(heads_all, ring_send.at[1], 4)

    share = proj.shape[1] // 2

    def proj_part(d, which):
        slot = lax.rem(x + d + 4, 4)
        size = share if which is None else share // 2
        first = t.c * share + (0 if which is None else which * size)
        return proj.at[slot, pl.ds(pl.multiple_of(first, size), size)]

    def proj_copy(d, which, sem, recv, to):
        ref = proj_part(d, which)
        return remote(ref, ref, proj_send.at[0], proj_recv.at[recv], to)

    proj_first = [proj_copy(0, None, 0, 0, plus), proj_copy(0, None, 1, 1, minus)]
    proj_second = [
        proj_copy(-1, 0, 2, 2, plus),
        proj_copy(1, 1, 3, 2, minus),
        proj_copy(-1, None, 4, 3, t.twin()),
        proj_copy(1, None, 5, 3, t.twin()),
    ]
    proj_third = [proj_copy(2, None, 6, 3, t.twin())]

    loads[0].wait()
    loads[1].wait()
    wide = latent_v[...].astype(F32)
    factor = lax.rsqrt(jnp.mean(wide * wide, axis=-1, keepdims=True) + norm_floor)
    normed = (wide * factor * latent_gain_ref[...]).astype(BF16)
    slab = kv.at[me]
    keys = jnp.dot(normed, key_up_v[...], preferred_element_type=F32).astype(BF16)
    for h in range(2):
        slab[h * rows : (h + 1) * rows, :] = keys[:, 128 * h : 128 * (h + 1)]
    pl.semaphore_wait(barrier, len(peers))
    pieces.send(0, 0)
    for load in loads[2:6]:
        load.wait()
    values = jnp.dot(normed, value_up_v[...], preferred_element_type=F32)
    for h in range(2):
        turned = values[:, 128 * h : 128 * (h + 1)].T.astype(BF16)
        for i in range(rows // 128):
            at = 2 * rows + h * rows + 128 * i
            slab[at : at + 128, :] = turned[:, 128 * i : 128 * (i + 1)]
    outer_cos, outer_sin = outer_v[0, :, 0:1], outer_v[1, :, 0:1]
    inner_cos, inner_sin = inner_v[0], inner_v[1]
    cosine = outer_cos * inner_cos - outer_sin * inner_sin
    sine = outer_sin * inner_cos + outer_cos * inner_sin
    mid = rows // 2
    key_turned = turn(rope_key_v[...].astype(F32), cosine, sine).T
    slab[4 * rows : 4 * rows + mid, :] = jnp.concatenate([key_turned[:mid], key_turned[mid:]], axis=1).astype(BF16)

    pieces.send(0, 1)
    loads[6].wait()
    for copy in proj_first:
        copy.start()

    for load in loads[7 : LOADS - 1]:
        load.wait()
    for copy in stream_ring.first():
        copy.start()
    zeros = jnp.zeros((64, rows), BF16)
    for h in range(2):
        nope = qn_v[:, h, :].astype(F32).T.astype(BF16)
        rotary = turn(qr_v[64 * h : 64 * (h + 1), :].astype(F32), cosine, sine).astype(BF16)
        for odd in range(2):
            q_ref[2 * h + odd, 0:128, :] = nope
            q_ref[2 * h + odd, 128:192, :] = zeros if odd else rotary
            q_ref[2 * h + odd, 192:256, :] = rotary if odd else zeros

    m_ref[...] = jnp.full_like(m_ref, big_negative)
    l_ref[...] = jnp.zeros_like(l_ref)
    acc_ref[...] = jnp.zeros_like(acc_ref)
    attend([kv.at[me]], q_ref, m_ref, l_ref, acc_ref, rows, const, diag=True)

    pltpu.make_async_copy(weights.at[me], weights.at[me], load_sems.at[LOADS - 1]).wait()
    last = len(ITEMS)

    def step(i, carry):
        for group in range(0, last, 4):

            @pl.when(i // 4 == group // 4)
            def _():
                for k in range(max(group, 1), group + 4):

                    @pl.when(i == k)
                    def _():
                        for begin, end in GROUPS:
                            if k == begin:
                                for other in range(begin, end):
                                    pieces.pass_on(other, 0)
                        pieces.pass_on(k, 1)
                        if k == PROJ_SECOND:
                            proj_copy(-1, None, 0, 0, minus).wait_recv()
                            proj_copy(1, None, 0, 1, minus).wait_recv()
                            for copy in proj_second:
                                copy.start()
                        if k == PROJ_THIRD:
                            proj_copy(2, None, 0, 2, minus).wait_recv()
                            for copy in proj_third:
                                copy.start()
                            stream_ring.forward()
                        if k == WEIGHTS_FIRST:
                            for part in range(2):
                                halves.send(0, part)

        da, db, ea, eb = (jnp.int32(0) for _ in range(4))
        for k, (ka, kb) in enumerate(ITEMS):
            da = jnp.where(i == k, ka, da)
            db = jnp.where(i == k, kb, db)
            ea = jnp.where(i == k + 1, ka, ea)
            eb = jnp.where(i == k + 1, kb, eb)
        own_slot = t.index(da, db)
        twin_slot = t.twin_index(ea, eb)
        pieces.twin_arrived(i - 1, twin_slot, 1)
        own_here = jnp.logical_and(own_slot < me, i < last)
        twin_here = twin_slot < me

        @pl.when(jnp.logical_and(own_here, twin_here))
        def _():
            attend([kv.at[own_slot], kv.at[twin_slot]], q_ref, m_ref, l_ref, acc_ref, rows, const)

        @pl.when(own_here != twin_here)
        def _():
            slot = jnp.where(own_here, own_slot, twin_slot)
            attend([kv.at[slot]], q_ref, m_ref, l_ref, acc_ref, rows, const)

        return carry

    lax.fori_loop(1, last + 1, step, 0)

    own = rows // 4
    for h in range(2):
        heads_all[x, :, 128 * h : 128 * (h + 1)] = (acc_ref[h] / l_ref[h]).T.astype(BF16)
    for copy in heads_ring.first():
        copy.start()

    def pass_weights(first, last, part):
        for k in range(first, last):
            halves.pass_on(k, part)

    pass_weights(1, 5, 0)
    stream_ring.near_arrived()
    stream_ring.far_arrived()
    twin_proj = proj.at[pl.ds(0, 3), pl.ds(0, share)]
    remote(twin_proj, twin_proj, proj_send.at[0], proj_recv.at[3], t.twin()).wait_recv()
    heads_ring.forward()
    pass_weights(5, 8, 0)
    heads_ring.near_arrived()

    def slots(ref, offsets, axis):
        return jnp.concatenate([ref[lax.rem(x + d + 4, 4)] for d in offsets], axis=axis)

    near = (0, 1, -1)
    sums[...] = jnp.dot(slots(heads_all, near, 1), slots(proj, near, 0), preferred_element_type=F32)
    pass_weights(8, 10, 0)
    heads_ring.far_arrived()
    sums[...] += jnp.dot(slots(heads_all, (2,), 1), slots(proj, (2,), 0), preferred_element_type=F32)

    def norm_rows(n, carry):
        total = sums[pl.ds(pl.multiple_of(n * own, own), own), :]
        mixed[n] = layer_norm(residual_weight * stream_all[n].astype(F32) + total, mix_gain_ref[...]).astype(BF16)
        return carry

    lax.fori_loop(0, 4, norm_rows, 0)
    count, units = weights.shape[0], weights.shape[2]
    pass_weights(10, 11, 0)
    pass_weights(1, 5, 1)
    pass_weights(11, 13, 0)
    halves.twin_arrived(0, 0, EARLY, 0)

    def weight_rows(chips, begin):
        blocks = [weights[pl.ds(chip * 2, 2), begin : begin + depth, :].reshape(2 * depth, units) for chip in chips]
        return jnp.concatenate(blocks, axis=0)

    def expand(chips, into):
        return [jnp.dot(into, weight_rows(chips, begin), preferred_element_type=F32) for begin in (0, depth)]

    def columns(ref, chips):
        n = ref.shape[0] if len(ref.shape) == 2 else ref.shape[0] * ref.shape[1]
        cols = [ref.at[..., pl.ds(pl.multiple_of(chip * 2 * depth, 2 * depth), 2 * depth)] for chip in chips]
        return jnp.concatenate([c[...].reshape(n, 2 * depth) for c in cols], axis=1)

    chips = [t.index(*item) // 2 for item in ITEMS]
    gate_sum[...], up_sum[...] = expand(chips[:EARLY], columns(mixed, chips[:EARLY]))
    pass_weights(13, 15, 0)
    pass_weights(5, 10, 1)
    pass_weights(15, 16, 0)
    halves.twin_arrived(1, 0, 16 - EARLY, 0)

    def rows_at(d):
        return pl.ds(pl.multiple_of(lax.rem(x + d + 4, 4) * own, own), own)

    def activate(first, second):
        into = [columns(mixed.at[lax.rem(x + d + 4, 4)], chips[EARLY:]) for d in (first, second)]
        gate, up = expand(chips[EARLY:], jnp.concatenate(into, axis=0))
        for n, d in enumerate((first, second)):
            g = gate_sum[rows_at(d), :] + gate[n * own : (n + 1) * own]
            u = up_sum[rows_at(d), :] + up[n * own : (n + 1) * own]
            hidden[rows_at(d), :] = (g / (1.0 + jnp.exp(-g)) * u).astype(BF16)

    half = own // 2
    top, low = pl.ds(0, half), pl.ds(half, half)
    column_sets = [
        (chips[first:last], pl.ds(first * 2 * depth, (last - first) * 2 * depth)) for first, last in COLUMN_SETS
    ]
    sets = len(column_sets)

    def lower(first, second, late):
        lhs = jnp.concatenate([hidden[rows_at(first), :], hidden[rows_at(second), :]], axis=0)
        rhs = weight_rows(column_sets[late][0], 2 * depth)
        out = lax.dot_general(lhs, rhs, (((1,), (1,)), ((), ())), preferred_element_type=F32)
        return out[:own], out[own:]

    def back(n, late):
        cols = column_sets[late][1]
        src, src_rows, dst, dst_rows, recv, to = (
            (far_out, top, far_minus, pl.ds(0, half), 2 * late, plus),
            (far_out, low, far_plus, pl.ds(0, half), 2 * late + 1, minus),
            (plus_out, low, from_minus, low, 2 * sets, plus),
            (minus_out, top, from_plus, top, 2 * sets + 1, minus),
            (plus_out, top, from_minus, top, 2 * sets, plus),
            (minus_out, low, from_plus, low, 2 * sets + 1, minus),
        )[n]
        return remote(src.at[src_rows, cols], dst.at[dst_rows, cols], x_send.at[0], x_recv.at[recv], to)

    def lower_far(late):
        cols = column_sets[late][1]
        far, near = lower(2, 1, late)
        far_out[:, cols] = far.astype(BF16)
        plus_out[:, cols] = near.astype(BF16)
        back(0, late).start()
        back(1, late).start()

    def lower_near(late):
        cols = column_sets[late][1]
        near, here = lower(-1, 0, late)
        minus_out[:, cols] = near.astype(BF16)
        sums[0:own, cols] = here
        back(2, late).start()
        back(3, late).start()

    def add_far(late):
        cols = column_sets[late][1]
        back(0, late).wait_recv()
        plus_out[top, cols] = (plus_out[top, cols].astype(F32) + far_minus[:, cols].astype(F32)).astype(BF16)
        back(4, late).start()
        back(1, late).wait_recv()
        minus_out[low, cols] = (minus_out[low, cols].astype(F32) + far_plus[:, cols].astype(F32)).astype(BF16)
        back(5, late).start()

    def down_arrived(n):
        first, last = COLUMN_SETS[n]
        halves.twin_arrived(2 + n, 0, last - first, 1)

    activate(2, 1)
    down_arrived(0)
    lower_far(0)
    activate(-1, 0)
    lower_near(0)
    pass_weights(10, 13, 1)
    down_arrived(1)
    lower_far(1)
    lower_near(1)
    add_far(0)
    pass_weights(13, 16, 1)
    down_arrived(2)
    lower_far(2)
    lower_near(2)
    add_far(1)
    add_far(2)
    for n, ref in ((2 * sets, from_minus), (2 * sets + 1, from_plus)):
        remote(ref, ref, x_send.at[0], x_recv.at[n], plus).wait_recv()
    lowered = sums[0:own, :] + from_plus[...].astype(F32) + from_minus[...].astype(F32)
    result = layer_norm(
        residual_weight * columns(mixed.at[x], chips).astype(F32) + 0.5 * lowered, columns(mlp_gain_ref, chips)
    ).astype(BF16)
    for n, chip in enumerate(chips):
        out_ref[:, pl.ds(pl.multiple_of(chip * 2 * depth, 2 * depth), 2 * depth)] = result[:, n * 2 * depth : (n + 1) * 2 * depth]

    pieces.sent()
    halves.sent()
    for ref, sem in (
        (proj.at[pl.ds(0, 3)], proj_send.at[0]),
        (stream_all.at[pl.ds(0, 3)], ring_send.at[0]),
        (heads_all.at[pl.ds(0, 3)], ring_send.at[1]),
        (mixed.at[pl.ds(0, 3)], x_send.at[0]),
    ):
        remote(ref, ref, sem, x_recv.at[0], t.twin()).wait_send()


GROUPS = ((1, 5), (5, 11), (11, 15), (15, 16))
LOADS = 11
EARLY = 11
COLUMN_SETS = ((0, 5), (5, 11), (11, 16))
PROJ_SECOND = 5
PROJ_THIRD = 9
WEIGHTS_FIRST = 13


def per_device(
    queries_nope,
    queries_rope,
    latent,
    rope_key,
    latent_gain,
    key_up,
    value_up,
    out_proj,
    stream,
    mix_gain,
    w_gate,
    w_up,
    w_down,
    mlp_gain,
):
    rows, heads, head_dim = queries_nope.shape
    rope_dim = queries_rope.shape[2]
    count = lax.axis_size("sp")
    tp = lax.axis_size("tp")
    own, width = stream.shape
    units = w_gate.shape[1]
    const = (head_dim + rope_dim) ** (-0.5) * math.log2(math.e)
    lanes = heads * rope_dim
    inner, outer = turn_tables(rows, count, rope_dim)
    slab = 4 * rows + rows // 2
    vmem = pl.BlockSpec(memory_space=pltpu.VMEM)
    hbm = pl.BlockSpec(memory_space=pl.ANY)
    dma = pltpu.SemaphoreType.DMA
    return pl.pallas_call(
        functools.partial(whole_kernel, rows, const),
        out_shape=jax.ShapeDtypeStruct((own, width), BF16),
        in_specs=[hbm] * 13 + [vmem] * 3,
        out_specs=vmem,
        scratch_shapes=[
            pltpu.VMEM(latent.shape, BF16),
            pltpu.VMEM((rope_dim, rows), BF16),
            pltpu.VMEM(key_up.shape, BF16),
            pltpu.VMEM(value_up.shape, BF16),
            pltpu.VMEM(inner.shape, F32),
            pltpu.VMEM(outer.shape[1:], F32),
            pltpu.VMEM(queries_nope.shape, BF16),
            pltpu.VMEM((lanes, rows), BF16),
            pltpu.VMEM((2 * heads, 2 * head_dim, rows), BF16),
            pltpu.VMEM((count, slab, 128), BF16),
            pltpu.VMEM((count, 3 * w_gate.shape[0], units), BF16),
            pltpu.VMEM((tp, *out_proj.shape), BF16),
            pltpu.VMEM((2, 1, rows), F32),
            pltpu.VMEM((2, 1, rows), F32),
            pltpu.VMEM((2, 128, rows), F32),
            pltpu.VMEM((tp, rows, heads * head_dim), BF16),
            pltpu.VMEM((tp, own, width), BF16),
            pltpu.VMEM((rows, width), F32),
            pltpu.VMEM((tp, own, width), BF16),
            pltpu.VMEM((rows, units), BF16),
            pltpu.VMEM((rows, units), F32),
            pltpu.VMEM((rows, units), F32),
            pltpu.VMEM((own, width), BF16),
            pltpu.VMEM((own, width), BF16),
            pltpu.VMEM((own, width), BF16),
            pltpu.VMEM((own // 2, width), BF16),
            pltpu.VMEM((own // 2, width), BF16),
            pltpu.VMEM((own, width), BF16),
            pltpu.VMEM((own, width), BF16),
            dma((LOADS,)),
            dma((1,)),
            dma((15, 2)),
            dma((16,)),
            dma((1,)),
            dma((15, 2)),
            dma((2 + len(COLUMN_SETS),)),
            dma((1,)),
            dma((4,)),
            dma((2,)),
            dma((8,)),
            dma((1,)),
            dma((2 * len(COLUMN_SETS) + 2,)),
        ],
        compiler_params=pltpu.CompilerParams(
            collective_id=0, has_side_effects=True, vmem_limit_bytes=60 * 1024 * 1024
        ),
        name="layer",
    )(
        latent,
        rope_key.T,
        key_up,
        value_up,
        inner,
        queries_nope,
        jnp.transpose(queries_rope, (1, 2, 0)).reshape(lanes, rows),
        out_proj,
        w_gate,
        w_up,
        w_down.T,
        stream,
        outer,
        latent_gain.reshape(1, -1),
        mix_gain.reshape(1, -1),
        mlp_gain.reshape(1, -1),
    )


def solution(mesh):
    return jax.shard_map(
        per_device,
        mesh=mesh,
        in_specs=(
            P("sp", "tp", None),
            P("sp", "tp", None),
            P("sp", None),
            P("sp", None),
            P(),
            P(None, "tp"),
            P(None, "tp"),
            P("tp", None),
            P(("sp", "tp"), None),
            P(),
            P("sp", "tp"),
            P("sp", "tp"),
            P("tp", "sp"),
            P(),
        ),
        out_specs=P(("sp", "tp"), None),
        check_vma=False,
    )
```

```python
import functools
import math

import jax
import jax.numpy as jnp
import numpy as np
from jax import lax
from jax.experimental import pallas as pl
from jax.experimental.pallas import tpu as pltpu
from jax.sharding import PartitionSpec as P

theta_base = 10000.0
residual_weight = 8.0**0.25
norm_floor = 1.0
big_negative = -1e30
F32 = jnp.float32
BF16 = jnp.bfloat16


def turn_tables(rows, count, rope_dim):
    rates = theta_base ** (-2.0 * np.arange(rope_dim // 2) / rope_dim)[:, None]
    inner = rates * np.arange(rows)
    outer = (rates * (np.arange(count) * rows)).T[:, :, None] + np.zeros((1, 1, 128))
    pair = lambda angle: jnp.asarray(np.stack([np.cos(angle), np.sin(angle)]), F32)
    return pair(inner), jnp.moveaxis(pair(outer), 0, 1)


def turn(v, cosine, sine):
    half = v.shape[0] // 2
    a, b = v[:half], v[half:]
    return jnp.concatenate([a * cosine - b * sine, a * sine + b * cosine], axis=0)


def layer_norm(values, gain):
    centre = jnp.mean(values, axis=-1, keepdims=True)
    centred = values - centre
    spread = jnp.mean(centred * centred, axis=-1, keepdims=True)
    return centred * lax.rsqrt(spread + norm_floor) * gain


def scores(kv, h, q_ref, rows, const):
    half = rows // 2
    r = kv[4 * rows : 4 * rows + half, :]
    top = jnp.concatenate([kv[h * rows : h * rows + half, :], r], axis=1)
    low = jnp.concatenate([kv[h * rows + half : (h + 1) * rows, :], r], axis=1)
    both = [
        jnp.dot(top, q_ref[2 * h], preferred_element_type=F32),
        jnp.dot(low, q_ref[2 * h + 1], preferred_element_type=F32),
    ]
    return jnp.concatenate(both, axis=0) * const


def values_of(kv, h, rows):
    at = 2 * rows + h * rows
    return [kv[at + 128 * i : at + 128 * (i + 1), :] for i in range(rows // 128)]


def attend(pieces, q_ref, m_ref, l_ref, acc_ref, rows, const, diag=False):
    for h in range(2):
        s = jnp.concatenate([scores(kv, h, q_ref, rows, const) for kv in pieces], axis=0)
        if diag:
            key = lax.broadcasted_iota(jnp.int32, s.shape, 0)
            query = lax.broadcasted_iota(jnp.int32, s.shape, 1)
            s = jnp.where(key <= query, s, big_negative)
        m_old = m_ref[h]
        m_new = jnp.maximum(m_old, jnp.max(s, axis=0, keepdims=True))
        p = jnp.exp2(s - m_new)
        alpha = jnp.exp2(m_old - m_new)
        l_ref[h] = l_ref[h] * alpha + jnp.sum(p, axis=0, keepdims=True)
        m_ref[h] = m_new
        vt = jnp.concatenate([block for kv in pieces for block in values_of(kv, h, rows)], axis=1)
        acc_ref[h] = acc_ref[h] * alpha + jnp.dot(vt, p.astype(BF16), preferred_element_type=F32)


MESH = pl.DeviceIdType.MESH
ITEMS = (
    (0, 0), (-1, 0), (1, 0), (0, -1), (0, 1), (2, 0), (-1, -1), (-1, 1),
    (1, -1), (1, 1), (0, 2), (2, -1), (2, 1), (-1, 2), (1, 2), (2, 2),
)
PLACE = {item: k for k, item in enumerate(ITEMS)}


def remote(src, dst, send_sem, recv_sem, device):
    return pltpu.make_async_remote_copy(
        src_ref=src, dst_ref=dst, send_sem=send_sem, recv_sem=recv_sem, device_id=device, device_id_type=MESH
    )


class Torus:
    def __init__(self):
        self.me = lax.axis_index("sp")
        self.x = lax.axis_index("tp")
        self.c = lax.rem(self.me, 2)
        chip = self.me // 2
        z, y = chip // 4, lax.rem(chip, 4)
        self.a = z + self.c * (y - z)
        self.b = y + self.c * (z - y)
        self.step_a = 8 - 6 * self.c
        self.step_b = 2 + 6 * self.c

    def index(self, da, db):
        at_a = lax.rem(self.a + da + 4, 4)
        at_b = lax.rem(self.b + db + 4, 4)
        return at_a * self.step_a + at_b * self.step_b + self.c

    def twin_index(self, da, db):
        at_b = lax.rem(self.b + da + 4, 4)
        at_a = lax.rem(self.a + db + 4, 4)
        return at_a * self.step_a + at_b * self.step_b + 1 - self.c

    def at(self, da, db):
        return (self.index(da, db), self.x)

    def twin(self):
        return (self.me + 1 - 2 * self.c, self.x)

    def along_x(self, d):
        return (self.me, lax.rem(self.x + d + 4, 4))


class Gather:
    def __init__(self, torus, buf, parts, send_sem, recv_sems, twin_sems, twin_of):
        self.torus, self.buf, self.parts = torus, buf, parts
        self.send_sem, self.recv_sems, self.twin_sems, self.twin_of = send_sem, recv_sems, twin_sems, twin_of

    def ref(self, slot, part, which=None):
        begin, size = self.parts[part]
        if which is not None:
            size //= 2
            begin += which * size
        return self.buf.at[slot, pl.ds(begin, size)]

    def copies(self, k, part):
        t = self.torus
        da, db = ITEMS[k]
        slot = t.index(da, db)
        plan = []
        if db == 0:
            if da == 0:
                plan += [((1, 0), (-1, 0), None), ((-1, 0), (1, 0), None)]
            plan += [((0, 1), (da, -1), None), ((0, -1), (da, 1), None)]
            if da == -1:
                plan += [((1, 0), (2, 0), 0)]
            if da == 1:
                plan += [((-1, 0), (2, 0), 1)]
        if db == -1:
            plan += [((0, 1), (da, 2), 0)]
        if db == 1:
            plan += [((0, -1), (da, 2), 1)]
        out = []
        for to, name, which in plan:
            ref = self.ref(slot, part, which)
            out.append(remote(ref, ref, self.send_sem, self.recv_sems.at[PLACE[name] - 1, part], t.at(*to)))
        ref = self.ref(slot, part)
        out.append(remote(ref, ref, self.send_sem, self.twin_sems.at[self.twin_of(k, part)], t.twin()))
        return out

    def send(self, k, part):
        for copy in self.copies(k, part):
            copy.start()

    def sent(self):
        ref = self.buf.at[pl.ds(0, 31)]
        remote(ref, ref, self.send_sem, self.recv_sems.at[0, 0], self.torus.twin()).wait_send()

    def arrived(self, k, part):
        ref = self.ref(self.torus.index(*ITEMS[k]), part)
        remote(ref, ref, self.send_sem, self.recv_sems.at[k - 1, part], self.torus.twin()).wait_recv()

    def pass_on(self, k, part):
        self.arrived(k, part)
        self.send(k, part)

    def twin_arrived(self, sem, first, count, part=None):
        ref = self.buf.at[pl.ds(first, count)]
        if part is not None:
            ref = self.buf.at[pl.ds(first, count), pl.ds(*self.parts[part])]
        remote(ref, ref, self.send_sem, self.twin_sems.at[sem], self.torus.twin()).wait_recv()


def whole_kernel(
    rows,
    const,
    latent_hbm,
    rope_key_hbm,
    key_up_hbm,
    value_up_hbm,
    inner_hbm,
    qn_hbm,
    qr_hbm,
    proj_hbm,
    gate_hbm,
    up_hbm,
    down_hbm,
    stream_hbm,
    outer_hbm,
    latent_gain_ref,
    mix_gain_ref,
    mlp_gain_ref,
    out_ref,
    latent_v,
    rope_key_v,
    key_up_v,
    value_up_v,
    inner_v,
    outer_v,
    qn_v,
    qr_v,
    q_ref,
    kv,
    weights,
    proj,
    m_ref,
    l_ref,
    acc_ref,
    heads_all,
    stream_all,
    sums,
    mixed,
    hidden,
    gate_sum,
    up_sum,
    far_out,
    plus_out,
    minus_out,
    far_plus,
    far_minus,
    from_plus,
    from_minus,
    load_sems,
    kv_send,
    kv_recv,
    kv_twin,
    w_send,
    w_recv,
    w_twin,
    proj_send,
    proj_recv,
    ring_send,
    ring_recv,
    x_send,
    x_recv,
):
    t = Torus()
    me, x = t.me, t.x
    depth = weights.shape[1] // 3
    loads = [
        pltpu.make_async_copy(src, dst, load_sems.at[min(n, LOADS - 1)])
        for n, (src, dst) in enumerate(
            (
                (latent_hbm, latent_v),
                (key_up_hbm, key_up_v),
                (value_up_hbm, value_up_v),
                (rope_key_hbm, rope_key_v),
                (inner_hbm, inner_v),
                (outer_hbm.at[me], outer_v),
                (proj_hbm, proj.at[x]),
                (qn_hbm, qn_v),
                (qr_hbm, qr_v),
                (stream_hbm, stream_all.at[x]),
                (gate_hbm, weights.at[me, pl.ds(0, depth)]),
                (up_hbm, weights.at[me, pl.ds(depth, depth)]),
                (down_hbm, weights.at[me, pl.ds(2 * depth, depth)]),
            )
        )
    ]
    for load in loads[:2]:
        load.start()

    plus, minus, across = t.along_x(1), t.along_x(-1), t.along_x(2)
    peers = (t.at(1, 0), t.at(-1, 0), t.at(0, 1), t.at(0, -1), t.twin(), plus, minus, across)
    barrier = pltpu.get_barrier_semaphore()
    for peer in peers:
        pl.semaphore_signal(barrier, inc=1, device_id=peer, device_id_type=MESH)
    for load in loads[2:]:
        load.start()

    slab_rows = kv.shape[1]
    pieces = Gather(t, kv, [(0, 2 * rows), (2 * rows, slab_rows - 2 * rows)], kv_send.at[0], kv_recv, kv_twin, lambda k, part: k)
    halves = Gather(t, weights, [(0, 2 * depth), (2 * depth, depth)], w_send.at[0], w_recv, w_twin, lambda k, part: k // EARLY if part == 0 else 2 + [first <= k < last for first, last in COLUMN_SETS].index(True))

    class Ring:
        def __init__(self, buf, send_sem, first_sem):
            self.buf, self.send_sem, self.first_sem, self.half = buf, send_sem, first_sem, buf.shape[1] // 2

        def copy(self, d, which, sem, to):
            ref = self.buf.at[lax.rem(x + d + 4, 4), pl.ds(which * self.half, self.half)]
            n = self.first_sem + sem
            return remote(ref, ref, self.send_sem, ring_recv.at[n], to)

        def first(self, begin=0, end=4):
            plan = ((0, 0, plus), (1, 1, minus), (1, 2, plus), (0, 2, minus))
            return [self.copy(0, *one) for one in plan[begin:end]]

        def second(self, which):
            return self.copy(1, 1, 3, minus) if which else self.copy(-1, 0, 3, plus)

        def forward(self):
            for d, which in ((-1, 0), (1, 1)):
                self.copy(d, which, which, plus).wait_recv()
                self.second(which).start()

        def both_halves(self, sem):
            ref = self.buf.at[0]
            remote(ref, ref, self.send_sem, ring_recv.at[self.first_sem + sem], plus).wait_recv()

        def near_arrived(self):
            self.both_halves(2)

        def far_arrived(self):
            self.both_halves(3)

    stream_ring = Ring(stream_all, ring_send.at[0], 0)
    heads_ring = Ring(heads_all, ring_send.at[1], 4)

    share = proj.shape[1] // 2

    def proj_part(d, which):
        slot = lax.rem(x + d + 4, 4)
        size = share if which is None else share // 2
        first = t.c * share + (0 if which is None else which * size)
        return proj.at[slot, pl.ds(pl.multiple_of(first, size), size)]

    def proj_copy(d, which, sem, recv, to):
        ref = proj_part(d, which)
        return remote(ref, ref, proj_send.at[0], proj_recv.at[recv], to)

    proj_first = [proj_copy(0, None, 0, 0, plus), proj_copy(0, None, 1, 1, minus)]
    proj_second = [
        proj_copy(-1, 0, 2, 2, plus),
        proj_copy(1, 1, 3, 2, minus),
        proj_copy(-1, None, 4, 3, t.twin()),
        proj_copy(1, None, 5, 3, t.twin()),
    ]
    proj_third = [proj_copy(2, None, 6, 3, t.twin())]

    loads[0].wait()
    loads[1].wait()
    wide = latent_v[...].astype(F32)
    factor = lax.rsqrt(jnp.mean(wide * wide, axis=-1, keepdims=True) + norm_floor)
    normed = (wide * factor * latent_gain_ref[...]).astype(BF16)
    slab = kv.at[me]
    keys = jnp.dot(normed, key_up_v[...], preferred_element_type=F32).astype(BF16)
    for h in range(2):
        slab[h * rows : (h + 1) * rows, :] = keys[:, 128 * h : 128 * (h + 1)]
    pl.semaphore_wait(barrier, len(peers))
    pieces.send(0, 0)
    for load in loads[2:6]:
        load.wait()
    values = jnp.dot(normed, value_up_v[...], preferred_element_type=F32)
    for h in range(2):
        turned = values[:, 128 * h : 128 * (h + 1)].T.astype(BF16)
        for i in range(rows // 128):
            at = 2 * rows + h * rows + 128 * i
            slab[at : at + 128, :] = turned[:, 128 * i : 128 * (i + 1)]
    outer_cos, outer_sin = outer_v[0, :, 0:1], outer_v[1, :, 0:1]
    inner_cos, inner_sin = inner_v[0], inner_v[1]
    cosine = outer_cos * inner_cos - outer_sin * inner_sin
    sine = outer_sin * inner_cos + outer_cos * inner_sin
    mid = rows // 2
    key_turned = turn(rope_key_v[...].astype(F32), cosine, sine).T
    slab[4 * rows : 4 * rows + mid, :] = jnp.concatenate([key_turned[:mid], key_turned[mid:]], axis=1).astype(BF16)

    pieces.send(0, 1)
    loads[6].wait()
    for copy in proj_first:
        copy.start()

    for load in loads[7 : LOADS - 1]:
        load.wait()
    for copy in stream_ring.first():
        copy.start()
    zeros = jnp.zeros((64, rows), BF16)
    for h in range(2):
        nope = qn_v[:, h, :].astype(F32).T.astype(BF16)
        rotary = turn(qr_v[64 * h : 64 * (h + 1), :].astype(F32), cosine, sine).astype(BF16)
        for odd in range(2):
            q_ref[2 * h + odd, 0:128, :] = nope
            q_ref[2 * h + odd, 128:192, :] = zeros if odd else rotary
            q_ref[2 * h + odd, 192:256, :] = rotary if odd else zeros

    m_ref[...] = jnp.full_like(m_ref, big_negative)
    l_ref[...] = jnp.zeros_like(l_ref)
    acc_ref[...] = jnp.zeros_like(acc_ref)
    attend([kv.at[me]], q_ref, m_ref, l_ref, acc_ref, rows, const, diag=True)

    pltpu.make_async_copy(weights.at[me], weights.at[me], load_sems.at[LOADS - 1]).wait()
    last = len(ITEMS)

    def step(i, carry):
        for group in range(0, last, 4):

            @pl.when(i // 4 == group // 4)
            def _():
                for k in range(max(group, 1), group + 4):

                    @pl.when(i == k)
                    def _():
                        for begin, end in GROUPS:
                            if k == begin:
                                for other in range(begin, end):
                                    pieces.pass_on(other, 0)
                        pieces.pass_on(k, 1)
                        if k == PROJ_SECOND:
                            proj_copy(-1, None, 0, 0, minus).wait_recv()
                            proj_copy(1, None, 0, 1, minus).wait_recv()
                            for copy in proj_second:
                                copy.start()
                        if k == PROJ_THIRD:
                            proj_copy(2, None, 0, 2, minus).wait_recv()
                            for copy in proj_third:
                                copy.start()
                            stream_ring.forward()
                        if k == WEIGHTS_FIRST:
                            for part in range(2):
                                halves.send(0, part)

        da, db, ea, eb = (jnp.int32(0) for _ in range(4))
        for k, (ka, kb) in enumerate(ITEMS):
            da = jnp.where(i == k, ka, da)
            db = jnp.where(i == k, kb, db)
            ea = jnp.where(i == k + 1, ka, ea)
            eb = jnp.where(i == k + 1, kb, eb)
        own_slot = t.index(da, db)
        twin_slot = t.twin_index(ea, eb)
        pieces.twin_arrived(i - 1, twin_slot, 1)
        own_here = jnp.logical_and(own_slot < me, i < last)
        twin_here = twin_slot < me

        @pl.when(jnp.logical_and(own_here, twin_here))
        def _():
            attend([kv.at[own_slot], kv.at[twin_slot]], q_ref, m_ref, l_ref, acc_ref, rows, const)

        @pl.when(own_here != twin_here)
        def _():
            slot = jnp.where(own_here, own_slot, twin_slot)
            attend([kv.at[slot]], q_ref, m_ref, l_ref, acc_ref, rows, const)

        return carry

    lax.fori_loop(1, last + 1, step, 0)

    own = rows // 4
    for h in range(2):
        heads_all[x, :, 128 * h : 128 * (h + 1)] = (acc_ref[h] / l_ref[h]).T.astype(BF16)
    for copy in heads_ring.first(0, 2):
        copy.start()

    def pass_weights(first, last, part):
        for k in range(first, last):
            halves.pass_on(k, part)

    pass_weights(1, 5, 0)
    stream_ring.near_arrived()
    stream_ring.far_arrived()
    twin_proj = proj.at[pl.ds(0, 3), pl.ds(0, share)]
    remote(twin_proj, twin_proj, proj_send.at[0], proj_recv.at[3], t.twin()).wait_recv()
    for copy in heads_ring.first(2, 4):
        copy.start()
    heads_ring.forward()
    pass_weights(5, 8, 0)
    heads_ring.near_arrived()

    def slots(ref, offsets, axis):
        return jnp.concatenate([ref[lax.rem(x + d + 4, 4)] for d in offsets], axis=axis)

    near = (0, 1, -1)
    sums[...] = jnp.dot(slots(heads_all, near, 1), slots(proj, near, 0), preferred_element_type=F32)
    pass_weights(8, 10, 0)
    heads_ring.far_arrived()
    sums[...] += jnp.dot(slots(heads_all, (2,), 1), slots(proj, (2,), 0), preferred_element_type=F32)

    def norm_rows(n, carry):
        total = sums[pl.ds(pl.multiple_of(n * own, own), own), :]
        mixed[n] = layer_norm(residual_weight * stream_all[n].astype(F32) + total, mix_gain_ref[...]).astype(BF16)
        return carry

    lax.fori_loop(0, 4, norm_rows, 0)
    count, units = weights.shape[0], weights.shape[2]
    pass_weights(10, 11, 0)
    pass_weights(1, 5, 1)
    pass_weights(11, 13, 0)
    halves.twin_arrived(0, 0, EARLY, 0)

    def weight_rows(chips, begin):
        blocks = [weights[pl.ds(chip * 2, 2), begin : begin + depth, :].reshape(2 * depth, units) for chip in chips]
        return jnp.concatenate(blocks, axis=0)

    def expand(chips, into):
        return [jnp.dot(into, weight_rows(chips, begin), preferred_element_type=F32) for begin in (0, depth)]

    def columns(ref, chips):
        n = ref.shape[0] if len(ref.shape) == 2 else ref.shape[0] * ref.shape[1]
        cols = [ref.at[..., pl.ds(pl.multiple_of(chip * 2 * depth, 2 * depth), 2 * depth)] for chip in chips]
        return jnp.concatenate([c[...].reshape(n, 2 * depth) for c in cols], axis=1)

    chips = [t.index(*item) // 2 for item in ITEMS]
    gate_sum[...], up_sum[...] = expand(chips[:EARLY], columns(mixed, chips[:EARLY]))
    pass_weights(13, 15, 0)
    pass_weights(5, 10, 1)
    pass_weights(15, 16, 0)
    halves.twin_arrived(1, 0, 16 - EARLY, 0)

    def rows_at(d):
        return pl.ds(pl.multiple_of(lax.rem(x + d + 4, 4) * own, own), own)

    def activate(first, second):
        into = [columns(mixed.at[lax.rem(x + d + 4, 4)], chips[EARLY:]) for d in (first, second)]
        gate, up = expand(chips[EARLY:], jnp.concatenate(into, axis=0))
        for n, d in enumerate((first, second)):
            g = gate_sum[rows_at(d), :] + gate[n * own : (n + 1) * own]
            u = up_sum[rows_at(d), :] + up[n * own : (n + 1) * own]
            hidden[rows_at(d), :] = (g / (1.0 + jnp.exp(-g)) * u).astype(BF16)

    half = own // 2
    top, low = pl.ds(0, half), pl.ds(half, half)
    column_sets = [
        (chips[first:last], pl.ds(first * 2 * depth, (last - first) * 2 * depth)) for first, last in COLUMN_SETS
    ]
    sets = len(column_sets)

    def lower(first, second, late):
        lhs = jnp.concatenate([hidden[rows_at(first), :], hidden[rows_at(second), :]], axis=0)
        rhs = weight_rows(column_sets[late][0], 2 * depth)
        out = lax.dot_general(lhs, rhs, (((1,), (1,)), ((), ())), preferred_element_type=F32)
        return out[:own], out[own:]

    def back(n, late):
        cols = column_sets[late][1]
        src, src_rows, dst, dst_rows, recv, to = (
            (far_out, top, far_minus, pl.ds(0, half), 2 * late, plus),
            (far_out, low, far_plus, pl.ds(0, half), 2 * late + 1, minus),
            (plus_out, low, from_minus, low, 2 * sets, plus),
            (minus_out, top, from_plus, top, 2 * sets + 1, minus),
            (plus_out, top, from_minus, top, 2 * sets, plus),
            (minus_out, low, from_plus, low, 2 * sets + 1, minus),
        )[n]
        return remote(src.at[src_rows, cols], dst.at[dst_rows, cols], x_send.at[0], x_recv.at[recv], to)

    def lower_far(late):
        cols = column_sets[late][1]
        far, near = lower(2, 1, late)
        far_out[:, cols] = far.astype(BF16)
        plus_out[:, cols] = near.astype(BF16)
        back(0, late).start()
        back(1, late).start()

    def lower_near(late):
        cols = column_sets[late][1]
        near, here = lower(-1, 0, late)
        minus_out[:, cols] = near.astype(BF16)
        sums[0:own, cols] = here
        back(2, late).start()
        back(3, late).start()

    def add_far(late):
        cols = column_sets[late][1]
        back(0, late).wait_recv()
        plus_out[top, cols] = (plus_out[top, cols].astype(F32) + far_minus[:, cols].astype(F32)).astype(BF16)
        back(4, late).start()
        back(1, late).wait_recv()
        minus_out[low, cols] = (minus_out[low, cols].astype(F32) + far_plus[:, cols].astype(F32)).astype(BF16)
        back(5, late).start()

    def down_arrived(n):
        first, last = COLUMN_SETS[n]
        halves.twin_arrived(2 + n, 0, last - first, 1)

    activate(2, 1)
    down_arrived(0)
    lower_far(0)
    activate(-1, 0)
    lower_near(0)
    pass_weights(10, 13, 1)
    down_arrived(1)
    lower_far(1)
    lower_near(1)
    add_far(0)
    pass_weights(13, 16, 1)
    down_arrived(2)
    lower_far(2)
    lower_near(2)
    add_far(1)
    add_far(2)
    for n, ref in ((2 * sets, from_minus), (2 * sets + 1, from_plus)):
        remote(ref, ref, x_send.at[0], x_recv.at[n], plus).wait_recv()
    lowered = sums[0:own, :] + from_plus[...].astype(F32) + from_minus[...].astype(F32)
    result = layer_norm(
        residual_weight * columns(mixed.at[x], chips).astype(F32) + 0.5 * lowered, columns(mlp_gain_ref, chips)
    ).astype(BF16)
    for n, chip in enumerate(chips):
        out_ref[:, pl.ds(pl.multiple_of(chip * 2 * depth, 2 * depth), 2 * depth)] = result[:, n * 2 * depth : (n + 1) * 2 * depth]

    pieces.sent()
    halves.sent()
    for ref, sem in (
        (proj.at[pl.ds(0, 3)], proj_send.at[0]),
        (stream_all.at[pl.ds(0, 3)], ring_send.at[0]),
        (heads_all.at[pl.ds(0, 3)], ring_send.at[1]),
        (mixed.at[pl.ds(0, 3)], x_send.at[0]),
    ):
        remote(ref, ref, sem, x_recv.at[0], t.twin()).wait_send()


GROUPS = ((1, 5), (5, 11), (11, 15), (15, 16))
LOADS = 11
EARLY = 11
COLUMN_SETS = ((0, 5), (5, 11), (11, 16))
PROJ_SECOND = 5
PROJ_THIRD = 9
WEIGHTS_FIRST = 13


def per_device(
    queries_nope,
    queries_rope,
    latent,
    rope_key,
    latent_gain,
    key_up,
    value_up,
    out_proj,
    stream,
    mix_gain,
    w_gate,
    w_up,
    w_down,
    mlp_gain,
):
    rows, heads, head_dim = queries_nope.shape
    rope_dim = queries_rope.shape[2]
    count = lax.axis_size("sp")
    tp = lax.axis_size("tp")
    own, width = stream.shape
    units = w_gate.shape[1]
    const = (head_dim + rope_dim) ** (-0.5) * math.log2(math.e)
    lanes = heads * rope_dim
    inner, outer = turn_tables(rows, count, rope_dim)
    slab = 4 * rows + rows // 2
    vmem = pl.BlockSpec(memory_space=pltpu.VMEM)
    hbm = pl.BlockSpec(memory_space=pl.ANY)
    dma = pltpu.SemaphoreType.DMA
    return pl.pallas_call(
        functools.partial(whole_kernel, rows, const),
        out_shape=jax.ShapeDtypeStruct((own, width), BF16),
        in_specs=[hbm] * 13 + [vmem] * 3,
        out_specs=vmem,
        scratch_shapes=[
            pltpu.VMEM(latent.shape, BF16),
            pltpu.VMEM((rope_dim, rows), BF16),
            pltpu.VMEM(key_up.shape, BF16),
            pltpu.VMEM(value_up.shape, BF16),
            pltpu.VMEM(inner.shape, F32),
            pltpu.VMEM(outer.shape[1:], F32),
            pltpu.VMEM(queries_nope.shape, BF16),
            pltpu.VMEM((lanes, rows), BF16),
            pltpu.VMEM((2 * heads, 2 * head_dim, rows), BF16),
            pltpu.VMEM((count, slab, 128), BF16),
            pltpu.VMEM((count, 3 * w_gate.shape[0], units), BF16),
            pltpu.VMEM((tp, *out_proj.shape), BF16),
            pltpu.VMEM((2, 1, rows), F32),
            pltpu.VMEM((2, 1, rows), F32),
            pltpu.VMEM((2, 128, rows), F32),
            pltpu.VMEM((tp, rows, heads * head_dim), BF16),
            pltpu.VMEM((tp, own, width), BF16),
            pltpu.VMEM((rows, width), F32),
            pltpu.VMEM((tp, own, width), BF16),
            pltpu.VMEM((rows, units), BF16),
            pltpu.VMEM((rows, units), F32),
            pltpu.VMEM((rows, units), F32),
            pltpu.VMEM((own, width), BF16),
            pltpu.VMEM((own, width), BF16),
            pltpu.VMEM((own, width), BF16),
            pltpu.VMEM((own // 2, width), BF16),
            pltpu.VMEM((own // 2, width), BF16),
            pltpu.VMEM((own, width), BF16),
            pltpu.VMEM((own, width), BF16),
            dma((LOADS,)),
            dma((1,)),
            dma((15, 2)),
            dma((16,)),
            dma((1,)),
            dma((15, 2)),
            dma((2 + len(COLUMN_SETS),)),
            dma((1,)),
            dma((4,)),
            dma((2,)),
            dma((8,)),
            dma((1,)),
            dma((2 * len(COLUMN_SETS) + 2,)),
        ],
        compiler_params=pltpu.CompilerParams(
            collective_id=0, has_side_effects=True, vmem_limit_bytes=60 * 1024 * 1024
        ),
        name="layer",
    )(
        latent,
        rope_key.T,
        key_up,
        value_up,
        inner,
        queries_nope,
        jnp.transpose(queries_rope, (1, 2, 0)).reshape(lanes, rows),
        out_proj,
        w_gate,
        w_up,
        w_down.T,
        stream,
        outer,
        latent_gain.reshape(1, -1),
        mix_gain.reshape(1, -1),
        mlp_gain.reshape(1, -1),
    )


def solution(mesh):
    return jax.shard_map(
        per_device,
        mesh=mesh,
        in_specs=(
            P("sp", "tp", None),
            P("sp", "tp", None),
            P("sp", None),
            P("sp", None),
            P(),
            P(None, "tp"),
            P(None, "tp"),
            P("tp", None),
            P(("sp", "tp"), None),
            P(),
            P("sp", "tp"),
            P("sp", "tp"),
            P("tp", "sp"),
            P(),
        ),
        out_specs=P(("sp", "tp"), None),
        check_vma=False,
    )
```
